32 devices in a mesh: rep: 2 (over x), fs: 8 (over z, y), tp: 2 (over core).
Axes of the slice: x: 2, y: 2, z: 4, core: 2. Of those that a mesh axis runs over, the one named last changes fastest.
Arguments:
- tokens: bfloat16 [6144, 2048], P(('rep', 'fs')), may hold values from -6 to 6
- first_gain: float32 [2048], replicated, may hold values from 0.1 to 1.9
- mixer_gate: bfloat16 [2048, 2048], P('fs', 'tp'), may hold values from -0.125 to 0.125
- mixer_value: bfloat16 [2048, 2048], P('fs', 'tp'), may hold values from -1 to 1
- value_gain: float32 [2048], replicated, may hold values from 0.1 to 1.9
- value_shift: float32 [2048], replicated, may hold values from -3 to 3
- spatial_weight: bfloat16 [16, 128, 128], replicated, may hold values from -0.75 to 0.75
- spatial_bias: float32 [16, 128], replicated, may hold values from 0.1 to 1.9
- mixer_out: bfloat16 [2048, 2048], P('tp', 'fs'), may hold values from -0.125 to 0.125
- second_gain: float32 [2048], replicated, may hold values from 0.1 to 1.9
- up_gate: bfloat16 [2048, 4096], P('fs', 'tp'), may hold values from -0.125 to 0.125
- up_value: bfloat16 [2048, 4096], P('fs', 'tp'), may hold values from -0.125 to 0.125
- taps_gate: float32 [3, 4096], replicated, may hold values from -3.5 to 3.5
- taps_value: float32 [3, 4096], replicated, may hold values from -3.5 to 3.5
- down_proj: bfloat16 [4096, 2048], P('tp', 'fs'), may hold values from -0.09375 to 0.09375
Outputs:
- layer_out: bfloat16 [6144, 2048], P(('rep', 'fs'))
The draws below stay inside these ranges and needn't reach their ends.
All inputs are finite; a program needn't handle non-finite values.
Results may differ from the reference program's by a relative error of at most 0.015.
Values may be sent and summed in bfloat16 or wider, within the bound.
A program may use at most 64 MiB of HBM per device.

```python
import math
import jax
import jax.numpy as jnp
from jax import lax

D = 2048
FF = 4096
GDIM = 128
BLK = 128
LEN = 128
TOK_DEV = 384
GROUPS = 16
TOKENS = 6144
N_TP = 2


def draw_mixer_value(key, part):
    first_key, second_key = jax.random.split(jax.random.fold_in(key, 17))
    base = jax.random.truncated_normal(first_key, -6.0, 6.0, (D, D), jnp.float32) * D ** (-0.5)
    scales = jnp.exp(jax.random.uniform(second_key, (D // GDIM,), jnp.float32, math.log(0.25), math.log(4.0)))
    return jnp.clip(base * jnp.repeat(scales, GDIM)[None, :], -1.0, 1.0).astype(jnp.bfloat16)


def level_of(rng, dims, cuts, least, largest):
    loudness = 1.0
    for axis_at, shards_of in cuts:
        heights = jax.random.uniform(jax.random.fold_in(jax.random.fold_in(rng, 6), axis_at), (shards_of,), jnp.float32, least / len(cuts), largest / len(cuts))
        loudness = loudness * jnp.repeat(jnp.exp(heights), dims[axis_at] // shards_of).reshape((-1,) + (1,) * (len(dims) - 1 - axis_at))
    return loudness


def normal_values(key, shape, deviation, bound, shards=(), dtype=jnp.bfloat16):
    loudness = level_of(key, shape, shards, -0.22, 0.18) if shards else 1.0
    array = jax.random.normal(key, shape, jnp.float32) * deviation * loudness
    return jnp.minimum(jnp.maximum(array, -bound), bound).astype(dtype)


def setup_inputs(seed: int = 0) -> dict:
    key_list = jax.random.split(jax.random.key(seed), 16)
    tokens = normal_values(key_list[0], (TOKENS, D), 1.0, 6.0, ((0, 16),))
    first_gain = jnp.clip(1.0 + 0.18 * jax.random.normal(key_list[1], (D,), jnp.float32), 0.1, 1.9)
    mixer_gate = normal_values(key_list[2], (D, D), D ** -0.5, 0.125, ((0, 8), (1, 2)))
    mixer_value = draw_mixer_value(jax.random.fold_in(key_list[15], 71), 0)
    value_gain = jnp.clip(1.0 + 0.18 * jax.random.normal(key_list[4], (D,), jnp.float32), 0.1, 1.9)
    value_shift = normal_values(key_list[5], (D,), 0.5, 3.0, (), jnp.float32)
    spatial_weight = normal_values(key_list[6], (GROUPS, BLK, BLK), (BLK // 2) ** -0.5, 0.75)
    spatial_bias = jnp.clip(1.0 + 0.18 * jax.random.normal(key_list[7], (GROUPS, BLK), jnp.float32), 0.1, 1.9)
    mixer_out = normal_values(key_list[8], (D, D), D ** -0.5, 0.125, ((0, 2), (1, 8)))
    second_gain = jnp.clip(1.0 + 0.18 * jax.random.normal(key_list[9], (D,), jnp.float32), 0.1, 1.9)
    up_gate = normal_values(key_list[10], (D, FF), D ** -0.5, 0.125, ((0, 8), (1, 2)))
    up_value = normal_values(key_list[11], (D, FF), D ** -0.5, 0.125, ((0, 8), (1, 2)))
    taps_gate = normal_values(key_list[12], (3, FF), 3 ** -0.5, 3.5, (), jnp.float32)
    taps_value = normal_values(key_list[13], (3, FF), 3 ** -0.5, 3.5, (), jnp.float32)
    down_proj = normal_values(key_list[14], (FF, D), FF ** -0.5, 0.09375, ((0, 2), (1, 8)))
    return dict(tokens=tokens, first_gain=first_gain, mixer_gate=mixer_gate, mixer_value=mixer_value, value_gain=value_gain, value_shift=value_shift, spatial_weight=spatial_weight, spatial_bias=spatial_bias, mixer_out=mixer_out, second_gain=second_gain, up_gate=up_gate, up_value=up_value, taps_gate=taps_gate, taps_value=taps_value, down_proj=down_proj)


def normalize(matrix, scale_gain):
    values = matrix.astype(jnp.float32)
    factor = lax.rsqrt(lax.optimization_barrier(jnp.mean(values * values, axis=-1, keepdims=True)) + 1e-06)
    return (values * factor * scale_gain).astype(jnp.bfloat16)

def causal_conv(values, tap_weights):
    by_sequence = values.reshape(-1, LEN, values.shape[-1])
    padded = jnp.pad(by_sequence, ((0, 0), (2, 0), (0, 0)))
    summed = tap_weights[0] * padded[:, 0:LEN] + tap_weights[1] * padded[:, 1:LEN + 1] + tap_weights[2] * padded[:, 2:LEN + 2]
    return summed.reshape(values.shape)

def rounded_sum(operand, weight):
    block_width = operand.shape[1] // N_TP
    summed = jnp.zeros((operand.shape[0], weight.shape[1]), jnp.float32)
    for segment in range(N_TP):
        partial_value = jnp.dot(operand[:, segment * block_width:(segment + 1) * block_width], weight[segment * block_width:(segment + 1) * block_width], preferred_element_type=jnp.float32).astype(jnp.bfloat16)
        partial_value = lax.optimization_barrier(partial_value)
        summed = summed + partial_value.astype(jnp.float32)
    return summed

def reference(tokens, first_gain, mixer_gate, mixer_value, value_gain, value_shift, spatial_weight, spatial_bias, mixer_out, second_gain, up_gate, up_value, taps_gate, taps_value, down_proj):

    def one_group(group_rows):
        first = normalize(group_rows, first_gain)
        gate_act = jax.nn.gelu(jnp.dot(first, mixer_gate, preferred_element_type=jnp.float32))
        value_act = jax.nn.gelu(jnp.dot(first, mixer_value, preferred_element_type=jnp.float32))
        row_mean = lax.optimization_barrier(jnp.sum(value_act, axis=1)) / D
        variance = lax.optimization_barrier(jnp.sum(value_act * value_act, axis=1)) / D - row_mean * row_mean
        centred = ((value_act - row_mean[:, None]) * lax.rsqrt(variance[:, None] + 1e-05) * value_gain + value_shift).astype(jnp.bfloat16)
        lower = jnp.tril(jnp.ones((BLK, BLK), jnp.float32))
        masked = spatial_weight.astype(jnp.float32) * lower
        blocks = centred.reshape(TOK_DEV // BLK, BLK, D // GDIM, GDIM).astype(jnp.float32)
        mixed_rows = jnp.einsum('gts,bsgc->btgc', masked, blocks) + spatial_bias.T[None, :, :, None]
        gated_rows = (gate_act * mixed_rows.reshape(TOK_DEV, D)).astype(jnp.bfloat16)
        mixer_sum = rounded_sum(gated_rows, mixer_out)
        residual = (group_rows.astype(jnp.float32) + mixer_sum).astype(jnp.bfloat16)
        second = normalize(residual, second_gain)
        gate_up = jnp.dot(second, up_gate, preferred_element_type=jnp.float32)
        value_up = jnp.dot(second, up_value, preferred_element_type=jnp.float32)
        hidden = (jax.nn.silu(causal_conv(gate_up, taps_gate)) * causal_conv(value_up, taps_value)).astype(jnp.bfloat16)
        ffn_sum = rounded_sum(hidden, down_proj)
        return (residual.astype(jnp.float32) + ffn_sum).astype(jnp.bfloat16)
    grouped = tokens.reshape(-1, TOK_DEV, D)
    result = lax.map(one_group, grouped)
    return result.reshape(-1, D)
```

```python
import functools

import jax
import jax.numpy as jnp
from jax import lax
from jax.experimental import pallas as pl
from jax.experimental.pallas import tpu as pltpu
from jax.sharding import PartitionSpec as P

D = 2048
GDIM = 128
BLK = 128
LEN = 128


def normalize(matrix, scale_gain):
    values = matrix.astype(jnp.float32)
    factor = lax.rsqrt(jnp.mean(values * values, axis=-1, keepdims=True) + 1e-06)
    return (values * factor * scale_gain).astype(jnp.bfloat16)


def causal_conv(values, tap_weights):
    by_sequence = values.reshape(-1, LEN, values.shape[-1])
    padded = jnp.pad(by_sequence, ((0, 0), (2, 0), (0, 0)))
    summed = (
        tap_weights[0] * padded[:, 0:LEN]
        + tap_weights[1] * padded[:, 1 : LEN + 1]
        + tap_weights[2] * padded[:, 2 : LEN + 2]
    )
    return summed.reshape(values.shape)


def local(
    tokens,
    first_gain,
    mixer_gate,
    mixer_value,
    value_gain,
    value_shift,
    spatial_weight,
    spatial_bias,
    mixer_out,
    second_gain,
    up_gate,
    up_value,
    taps_gate,
    taps_value,
    down_proj,
):
    n_rep, n_tp = lax.axis_size("rep"), lax.axis_size("tp")
    rep_index, tp_index = lax.axis_index("rep"), lax.axis_index("tp")
    team = ("rep", "tp")

    def part(array, axis):
        width = array.shape[axis] // n_rep
        return lax.dynamic_slice_in_dim(array, rep_index * width, width, axis)

    def own(array, width, axis):
        at = (tp_index * n_rep + rep_index) * width
        return lax.dynamic_slice_in_dim(array, at, width, axis)

    w_gate = lax.all_gather(part(mixer_gate, 1), "fs", axis=0, tiled=True)
    w_value = lax.all_gather(part(mixer_value, 1), "fs", axis=0, tiled=True)
    w_out = lax.all_gather(part(mixer_out, 0), "fs", axis=1, tiled=True)
    u_gate = lax.all_gather(part(up_gate, 1), "fs", axis=0, tiled=True)
    u_value = lax.all_gather(part(up_value, 1), "fs", axis=0, tiled=True)
    w_down = lax.all_gather(part(down_proj, 0), "fs", axis=1, tiled=True)

    row_share = tokens.shape[0] // n_tp
    kept_tokens = lax.dynamic_slice_in_dim(tokens, tp_index * row_share, row_share, 0)
    first = lax.all_gather(normalize(kept_tokens, first_gain), team, axis=0, tiled=True)
    row_count = first.shape[0]
    cols = w_gate.shape[1]
    gate_act = jax.nn.gelu(jnp.dot(first, w_gate, preferred_element_type=jnp.float32))
    value_act = jax.nn.gelu(jnp.dot(first, w_value, preferred_element_type=jnp.float32))
    value_sum, value_squares = lax.psum(
        (jnp.sum(value_act, axis=1), jnp.sum(value_act * value_act, axis=1)), team
    )
    row_mean = value_sum / D
    variance = value_squares / D - row_mean * row_mean
    centred = (
        (value_act - row_mean[:, None])
        * lax.rsqrt(variance[:, None] + 1e-05)
        * own(value_gain, cols, 0)
        + own(value_shift, cols, 0)
    ).astype(jnp.bfloat16)
    groups = cols // GDIM
    masked = own(spatial_weight, groups, 0) * jnp.tril(jnp.ones((BLK, BLK), jnp.bfloat16))
    blocks = centred.reshape(row_count // BLK, BLK, groups, GDIM)
    mixed_rows = (
        jnp.einsum("gts,bsgc->btgc", masked, blocks, preferred_element_type=jnp.float32)
        + own(spatial_bias, groups, 0).T[None, :, :, None]
    )
    gated_rows = (gate_act * mixed_rows.reshape(row_count, cols)).astype(jnp.bfloat16)
    summed = lax.psum_scatter(
        jnp.dot(gated_rows, w_out, preferred_element_type=jnp.float32).astype(jnp.bfloat16),
        team,
        scatter_dimension=0,
        tiled=True,
    ).astype(jnp.float32)
    residual = (kept_tokens.astype(jnp.float32) + summed).astype(jnp.bfloat16)
    second = lax.all_gather(normalize(residual, second_gain), team, axis=0, tiled=True)
    hidden_cols = u_gate.shape[1]
    gate_up = jnp.dot(second, u_gate, preferred_element_type=jnp.float32)
    value_up = jnp.dot(second, u_value, preferred_element_type=jnp.float32)
    hidden = (
        jax.nn.silu(causal_conv(gate_up, own(taps_gate, hidden_cols, 1)))
        * causal_conv(value_up, own(taps_value, hidden_cols, 1))
    ).astype(jnp.bfloat16)
    ffn_total = lax.psum_scatter(
        jnp.dot(hidden, w_down, preferred_element_type=jnp.float32).astype(jnp.bfloat16),
        team,
        scatter_dimension=0,
        tiled=True,
    ).astype(jnp.float32)
    final_rows = (residual.astype(jnp.float32) + ffn_total).astype(jnp.bfloat16)
    return lax.all_gather(final_rows, "tp", axis=0, tiled=True)


PLANE = 2
ARRAYS = 6
FAR = 3
MESH = pl.DeviceIdType.MESH


def team_kernel(
    dims,
    tokens,
    first_gain,
    mixer_gate,
    mixer_value,
    value_gain,
    value_shift,
    spatial_weight,
    spatial_bias,
    mixer_out,
    second_gain,
    up_gate,
    up_value,
    taps_gate,
    taps_value,
    down_proj,
    out,
    w_gate,
    w_value,
    w_out,
    w_ug,
    w_uv,
    w_down,
    tok,
    rows_in,
    gate_act,
    value_act,
    gated,
    gate_half,
    hidden,
    part,
    from_partner,
    from_team,
    residual,
    stats,
    own_sem,
    side_send,
    up_send,
    down_send,
    weight_recv,
    team_send,
    team_recv,
    pass_send,
    pass_recv,
    stat_send,
    stat_recv,
    pair_send,
    pair_recv,
    sum_send,
    sum_recv,
    cross_send,
    cross_recv,
    last_sem,
):
    n_rep, n_fs, n_tp = dims
    n_side, n_line = PLANE, n_fs // PLANE
    n_chip = n_rep * n_side
    x, c = lax.axis_index("rep"), lax.axis_index("tp")
    f_own = lax.axis_index("fs")
    z, y = f_own // n_side, f_own % n_side
    other = (c + 1) % n_tp
    q_own = x * n_side + y
    rows = tokens.shape[0]
    half = rows // n_tp
    width = tokens.shape[1]
    sources = (mixer_value, mixer_gate, mixer_out, up_gate, up_value, down_proj)
    held = (w_value, w_gate, w_out, w_ug, w_uv, w_down)
    offsets = [(dx, dy) for dx in range(n_rep) for dy in range(n_side)]
    partner = (x, f_own, other)

    def chip_to(k, core):
        dx, dy = offsets[k]
        return ((x + dx) % n_rep, z * n_side + (y + dy) % n_side, core)

    def chip_q(k, sign):
        dx, dy = offsets[k]
        return ((x + sign * dx + n_rep) % n_rep) * n_side + (y + sign * dy + n_side) % n_side

    def remote(src, dst, send, recv, device):
        return pltpu.make_async_remote_copy(
            src_ref=src, dst_ref=dst, send_sem=send, recv_sem=recv, device_id=device, device_id_type=MESH
        )

    def block(a, f):
        if len(held[a].shape) == 3:
            return held[a].at[f]
        height = sources[a].shape[0]
        return held[a].at[pl.ds(pl.multiple_of(f * height, height), height)]

    def piece(a, q):
        if len(held[a].shape) == 3:
            height = sources[a].shape[0] // n_chip
            return sources[a].at[pl.ds(pl.multiple_of(q * height, height), height)]
        cols = sources[a].shape[1] // n_chip
        return sources[a].at[:, pl.ds(pl.multiple_of(q * cols, cols), cols)]

    def own_copy(a):
        return pltpu.make_async_copy(piece(a, q_own), block(a, f_own), own_sem.at[a])

    def side(a, dy):
        to_y = (y + dy) % n_side
        return remote(
            piece(a, x * n_side + to_y),
            block(a, f_own),
            side_send.at[a, dy],
            weight_recv.at[a, f_own],
            (x, z * n_side + to_y, c),
        )

    def along(a, f, step, src):
        sem = up_send if step == 1 else down_send
        return remote(
            src, block(a, f), sem.at[a, f], weight_recv.at[a, f], (x, f_own + step * n_side, c)
        )

    def landed(a, f):
        remote(block(a, f), block(a, f), side_send.at[a, 0], weight_recv.at[a, f], partner).wait_recv()

    has_up, has_down = z + 1 < n_line, z >= 1

    def send_line(a, f, src, up=True, down=True):
        if up:
            pl.when(has_up)(lambda: along(a, f, 1, src).start())
        if down:
            pl.when(has_down)(lambda: along(a, f, -1, src).start())

    def start_side(a):
        own_copy(a).start()
        for dy in range(1, n_side):
            side(a, dy).start()

    def start_line(a):
        send_line(a, f_own, piece(a, q_own))

    def relay(a, d):
        if d == 0:
            for dy in range(1, n_side):
                f = z * n_side + (y + dy) % n_side
                landed(a, f)
                send_line(a, f, block(a, f))
            own_copy(a).wait()
            return
        for j in range(n_side):

            @pl.when((z - d >= 0) & has_up)
            def _():
                f = (z - d) * n_side + j
                landed(a, f)
                send_line(a, f, block(a, f), down=False)

            @pl.when((z + d < n_line) & has_down)
            def _():
                f = (z + d) * n_side + j
                landed(a, f)
                send_line(a, f, block(a, f), up=False)

    def arrived(a, d):
        for j in range(n_side):
            pl.when((z - d >= 0) & (z == n_line - 1))(lambda: landed(a, (z - d) * n_side + j))
            pl.when((z + d < n_line) & (z == 0))(lambda: landed(a, (z + d) * n_side + j))

    def arrived_all(a):
        for d in range(1, n_line):
            arrived(a, d)

    def chip_rows(q, core):
        return pl.ds(pl.multiple_of(q * rows + core * half, half), half)

    def share(g, k, buffer, src):
        place = buffer.at[chip_rows(q_own, c)]
        return remote(src, place, team_send.at[g, k], team_recv.at[g, k], chip_to(k, c))

    def share_landed(g, k, buffer):
        place = buffer.at[chip_rows(chip_q(k, -1), c)]
        remote(place, place, team_send.at[g, k], team_recv.at[g, k], partner).wait_recv()

    def across_place(buffer, q, k):
        quarter = half // 2
        first = q * rows + c * half + (quarter if k == 1 else 0)
        return buffer.at[pl.ds(pl.multiple_of(first, quarter), quarter)]

    def across(g, k, buffer):
        place = across_place(buffer, chip_q(k, -1), k)
        return remote(
            place, place, cross_send.at[g, k], cross_recv.at[g, k], chip_to(FAR - k, c)
        )

    def across_landed(g, k, buffer):
        place = across_place(buffer, chip_q(FAR, -1), k)
        remote(place, place, cross_send.at[g, k], cross_recv.at[g, k], partner).wait_recv()

    def hand_on(g, k, buffer):
        place = buffer.at[chip_rows(chip_q(k, -1), c)]
        return remote(place, place, pass_send.at[g, k], pass_recv.at[g, k], partner)

    def hand_landed(g, k, buffer):
        place = buffer.at[chip_rows(chip_q(k, -1), other)]
        remote(place, place, pass_send.at[g, k], pass_recv.at[g, k], partner).wait_recv()

    def norm_rows(values, gain):
        factor = lax.rsqrt(jnp.mean(values * values, axis=-1, keepdims=True) + 1e-06)
        return (values * factor * gain).astype(jnp.bfloat16)

    step_rows = 64

    def norm_chip(q):
        def body(i, carry):
            at = pl.ds(pl.multiple_of(q * rows + i * step_rows, step_rows), step_rows)
            rows_in[at, :] = norm_rows(tok[at, :].astype(jnp.float32), first_gain[...])
            return carry

        lax.fori_loop(0, rows // step_rows, body, 0)

    barrier = pltpu.get_barrier_semaphore()
    for k in range(n_chip):
        for core in (c, other):
            if k or core is other:
                pl.semaphore_signal(barrier, inc=1, device_id=chip_to(k, core), device_id_type=MESH)
    for flag, step in ((has_up, 1), (has_down, -1)):

        @pl.when(flag)
        def _():
            pl.semaphore_signal(
                barrier, inc=1, device_id=(x, f_own + step * n_side, c), device_id_type=MESH
            )

    neighbours = has_up.astype(jnp.int32) + has_down.astype(jnp.int32)
    pl.semaphore_wait(barrier, n_chip * n_tp - 1 + neighbours)

    my_tokens = tokens.at[pl.ds(pl.multiple_of(c * half, half), half)]
    start_side(0)
    start_side(1)
    start_line(0)
    start_line(1)
    for k in (1, 2):
        share(0, k, tok, my_tokens).start()
    tok_copy = pltpu.make_async_copy(
        tokens, tok.at[pl.ds(pl.multiple_of(q_own * rows, rows), rows)], own_sem.at[ARRAYS]
    )
    tok_copy.start()
    start_side(2)
    relay(0, 0)
    relay(1, 0)
    relay(0, 1)
    relay(1, 1)
    start_line(2)
    for d in range(2, n_line - 1):
        relay(0, d)
    tok_copy.wait()
    norm_chip(q_own)
    for k in (1, 2):
        share_landed(0, k, tok)
        across(0, k, tok).start()
        hand_on(0, k, tok).start()
    relay(2, 0)
    start_side(3)
    for d in range(2, n_line - 1):
        relay(1, d)
    relay(2, 1)
    start_line(3)
    for d in range(2, n_line - 1):
        relay(2, d)
    for k in (1, 2):
        across_landed(0, k, tok)
    hand_on(0, FAR, tok).start()
    start_side(4)
    start_side(5)
    relay(3, 0)
    for k in range(1, n_chip):
        hand_landed(0, k, tok)
        norm_chip(chip_q(k, -1))
    arrived_all(0)

    def project(weight, target):
        tile = half

        def body(i, carry):
            at = pl.ds(pl.multiple_of(i * tile, tile), tile)
            product = jnp.dot(rows_in[at, :], weight[...], preferred_element_type=jnp.float32)
            target[at, :] = jax.nn.gelu(product)
            return carry

        lax.fori_loop(0, n_chip * n_tp, body, 0)

    cols = w_gate.shape[1]
    slot = c * n_chip + q_own
    blocks = n_chip * rows // BLK
    lane = lax.broadcasted_iota(jnp.int32, (BLK, BLK), 1)
    sub = lax.broadcasted_iota(jnp.int32, (BLK, BLK), 0)
    project(w_value, value_act)

    def stat_body(i, carry):
        at = pl.ds(pl.multiple_of(i * BLK, BLK), BLK)
        values = value_act[at, :]
        total = jnp.sum(values, axis=1, keepdims=True)
        squares = jnp.sum(values * values, axis=1, keepdims=True)
        both = jnp.where(lane == 0, total, squares).T
        stats[0, :, at] = both[0:2, :]
        return carry

    lax.fori_loop(0, blocks, stat_body, 0)
    mates = [(k, j) for k in range(n_chip) for j in range(n_tp) if k or j]

    def tell(i):
        k, j = mates[i]
        return remote(
            stats.at[0],
            stats.at[i + 1],
            stat_send.at[i],
            stat_recv.at[i],
            chip_to(k, (c + j) % n_tp),
        )

    for i in range(len(mates)):
        tell(i).start()
    relay(3, 1)
    start_line(4)
    arrived_all(1)
    project(w_gate, gate_act)
    for d in range(2, n_line - 1):
        relay(3, d)
    relay(4, 0)
    for i in range(len(mates)):
        tell(i).wait_recv()
    at_cols = pl.ds(pl.multiple_of(slot * cols, cols), cols)
    groups = cols // GDIM

    def mix_body(i, carry):
        at = pl.ds(pl.multiple_of(i * BLK, BLK), BLK)
        total = stats[0, :, at]
        for s in range(1, len(mates) + 1):
            total = total + stats[s, :, at]
        row_mean = jnp.broadcast_to(total[0:1, :] / width, (BLK, BLK)).T[:, 0:1]
        row_square = jnp.broadcast_to(total[1:2, :] / width, (BLK, BLK)).T[:, 0:1]
        variance = row_square - row_mean * row_mean
        centred = (
            (value_act[at, :] - row_mean) * lax.rsqrt(variance + 1e-05) * value_gain[:, at_cols]
            + value_shift[:, at_cols]
        ).astype(jnp.bfloat16)
        for g in range(groups):
            group = slot * groups + g
            matrix = spatial_weight[group]
            matrix = jnp.where(sub >= lane, matrix, jnp.zeros_like(matrix))
            bias = jnp.broadcast_to(spatial_bias[pl.ds(group, 1), :], (BLK, BLK)).T
            mixed = (
                jnp.dot(
                    matrix, centred[:, g * GDIM : (g + 1) * GDIM], preferred_element_type=jnp.float32
                )
                + bias
            )
            channels = slice(g * GDIM, (g + 1) * GDIM)
            gated[at, channels] = (gate_act[at, channels] * mixed).astype(jnp.bfloat16)
        return carry

    lax.fori_loop(0, blocks, mix_body, 0)

    out_width = w_out.shape[2] * n_side

    def plane_cols(p):
        return pl.ds(pl.multiple_of(p * out_width, out_width), out_width)

    def pair(s, p, q):
        place = plane_cols(p)
        return remote(
            part.at[chip_rows(q, other), place],
            from_partner.at[pl.ds(pl.multiple_of(q * half, half), half), place],
            pair_send.at[s, p, q],
            pair_recv.at[s, p, q],
            partner,
        )

    def piece_cols(p, j):
        cut = w_out.shape[2]
        return pl.ds(pl.multiple_of((p * n_side + j) * cut, cut), cut)

    def to_team(s, p, j, t):
        near = 2 if j == 0 else 1
        place = piece_cols(p, j)
        k_rows = (near, FAR, FAR - near)[t]
        k_chip = (near, near, FAR - near)[t]
        return remote(
            part.at[chip_rows(chip_q(k_rows, 1), c), place],
            from_team.at[t, :, place],
            sum_send.at[s, p, j * FAR + t],
            sum_recv.at[s, p, j * FAR + t],
            chip_to(k_chip, c),
        )

    def out_plane(s, p, acts, weight):
        def multiply(q, carry):
            at = pl.ds(pl.multiple_of(q * rows, rows), rows)
            for j in range(n_side):
                part[at, piece_cols(p, j)] = jnp.dot(
                    acts[at, :], weight[p * n_side + j], preferred_element_type=jnp.float32
                ).astype(jnp.bfloat16)
            pair(s, p, q).start()
            return carry

        lax.fori_loop(0, n_chip, multiply, 0)
        place = plane_cols(p)
        for k in (3, 2, 1, 0):
            q = chip_q(k, 1)
            pair(s, p, q).wait_recv()
            at = chip_rows(q, c)
            part[at, place] = (
                part[at, place].astype(jnp.float32)
                + from_partner[pl.ds(pl.multiple_of(q * half, half), half), place].astype(
                    jnp.float32
                )
            ).astype(jnp.bfloat16)
            for j in range(n_side):
                if k == FAR:
                    to_team(s, p, j, 1).start()
                elif k == 2 - j:
                    to_team(s, p, j, 0).start()

    def pass_plane(s, p):
        for j in range(n_side):
            to_team(s, p, j, 1).wait_recv()
            at, place = chip_rows(chip_q(1 if j == 0 else 2, 1), c), piece_cols(p, j)
            part[at, place] = (
                part[at, place].astype(jnp.float32) + from_team[1, :, place].astype(jnp.float32)
            ).astype(jnp.bfloat16)
            to_team(s, p, j, 2).start()

    def finish_plane(s, p, carry):
        for j in range(n_side):
            to_team(s, p, j, 0).wait_recv()
            to_team(s, p, j, 2).wait_recv()
        return carry

    def drain_plane(s, p, carry):
        for j in range(n_side):
            for t in range(FAR):
                to_team(s, p, j, t).wait_send()
        for q in range(n_chip):
            pair(s, p, q).wait_send()
        return carry

    def summed(i):
        at = pl.ds(pl.multiple_of(i * step_rows, step_rows), step_rows)
        mine = pl.ds(pl.multiple_of(q_own * rows + c * half + i * step_rows, step_rows), step_rows)
        total = part[mine, :].astype(jnp.float32)
        for t in (0, 2):
            total = total + from_team[t, at, :].astype(jnp.float32)
        return at, mine, total

    def out_body(p, carry):
        out_plane(0, p, gated, w_out)
        return carry

    def pass_body(p, carry):
        pass_plane(0, p)
        return carry

    arrived_all(2)
    lax.fori_loop(0, n_line, out_body, 0)
    relay(4, 1)
    start_line(5)
    lax.fori_loop(0, n_line, pass_body, 0)
    for d in range(2, n_line - 1):
        relay(4, d)
    relay(5, 0)
    lax.fori_loop(0, n_line, functools.partial(finish_plane, 0), 0)

    def residual_body(i, carry):
        at, mine, total = summed(i)
        kept = (tok[mine, :].astype(jnp.float32) + total).astype(jnp.bfloat16)
        residual[at, :] = kept
        rows_in[mine, :] = norm_rows(kept.astype(jnp.float32), second_gain[...])
        return carry

    lax.fori_loop(0, half // step_rows, residual_body, 0)
    mine = rows_in.at[chip_rows(q_own, c)]
    for k in (1, 2):
        share(1, k, rows_in, mine).start()
    hand_on(1, 0, rows_in).start()
    lax.fori_loop(0, n_line, functools.partial(drain_plane, 0), 0)
    relay(5, 1)
    for k in (1, 2):
        share_landed(1, k, rows_in)
        across(1, k, rows_in).start()
        hand_on(1, k, rows_in).start()
    for d in range(2, n_line - 1):
        relay(5, d)
    for k in (1, 2):
        across_landed(1, k, rows_in)
    hand_on(1, FAR, rows_in).start()
    for k in range(n_chip):
        hand_landed(1, k, rows_in)

    hidden_cols = w_ug.shape[1]
    at_hidden = pl.ds(pl.multiple_of(slot * hidden_cols, hidden_cols), hidden_cols)
    position = lax.broadcasted_iota(jnp.int32, (LEN, hidden_cols), 0)

    def conv(values, taps):
        back1 = jnp.where(position >= 1, pltpu.roll(values, 1, 0), 0.0)
        back2 = jnp.where(position >= 2, pltpu.roll(values, 2, 0), 0.0)
        weights = taps[:, at_hidden]
        return weights[0:1] * back2 + weights[1:2] * back1 + weights[2:3] * values

    def raise_body(weight, taps, last, i, carry):
        at = pl.ds(pl.multiple_of(i * rows, rows), rows)
        product = jnp.dot(rows_in[at, :], weight[...], preferred_element_type=jnp.float32)
        for s in range(rows // LEN):
            here = pl.ds(pl.multiple_of(i * rows + s * LEN, LEN), LEN)
            done = conv(product[s * LEN : (s + 1) * LEN], taps)
            if last:
                hidden[here, :] = (gate_half[here, :] * done).astype(jnp.bfloat16)
            else:
                gate_half[here, :] = jax.nn.silu(done)
        return carry

    arrived_all(3)
    lax.fori_loop(0, n_chip, functools.partial(raise_body, w_ug, taps_gate, False), 0)
    arrived_all(4)
    lax.fori_loop(0, n_chip, functools.partial(raise_body, w_uv, taps_value, True), 0)

    def at_distance(d, act):
        pl.when(z - d >= 0)(lambda: act(z - d))
        if d:
            pl.when(z + d < n_line)(lambda: act(z + d))

    for d in range(n_line):
        if d:
            arrived(5, d)
        at_distance(d, lambda p: out_plane(1, p, hidden, w_down))
        if d:
            at_distance(d - 1, lambda p: pass_plane(1, p))
    at_distance(n_line - 1, lambda p: pass_plane(1, p))
    lax.fori_loop(0, n_line, functools.partial(finish_plane, 1), 0)

    def last_body(i, carry):
        at, mine, total = summed(i)
        here = pl.ds(pl.multiple_of(c * half + i * step_rows, step_rows), step_rows)
        out[here, :] = (residual[at, :].astype(jnp.float32) + total).astype(jnp.bfloat16)
        return carry

    lax.fori_loop(0, half // step_rows, last_body, 0)
    my_half = out.at[pl.ds(pl.multiple_of(c * half, half), half)]
    last = remote(my_half, my_half, last_sem.at[0], last_sem.at[1], partner)
    last.start()
    lax.fori_loop(0, n_line, functools.partial(drain_plane, 1), 0)
    for i in range(len(mates)):
        tell(i).wait_send()
    for k in (1, 2):
        share(0, k, tok, my_tokens).wait_send()
        share(1, k, rows_in, mine).wait_send()
        across(0, k, tok).wait_send()
        across(1, k, rows_in).wait_send()
    for k in range(1, n_chip):
        hand_on(0, k, tok).wait_send()
    for k in range(n_chip):
        hand_on(1, k, rows_in).wait_send()
    for a in range(ARRAYS):
        for dy in range(1, n_side):
            side(a, dy).wait_send()

        def settle(f, carry, a=a):
            @pl.when(has_up & (f // n_side <= z))
            def _():
                along(a, f, 1, block(a, f)).wait_send()

            @pl.when(has_down & (f // n_side >= z))
            def _():
                along(a, f, -1, block(a, f)).wait_send()

            return carry

        lax.fori_loop(0, n_fs, settle, 0)
    last.wait_send()
    last.wait_recv()


def team_layer(
    dims,
    tokens,
    first_gain,
    mixer_gate,
    mixer_value,
    value_gain,
    value_shift,
    spatial_weight,
    spatial_bias,
    mixer_out,
    second_gain,
    up_gate,
    up_value,
    taps_gate,
    taps_value,
    down_proj,
):
    n_rep, n_fs, n_tp = dims
    n_chip, n_line = n_rep * PLANE, n_fs // PLANE
    rows, width = tokens.shape
    half, team_rows = rows // n_tp, rows * n_chip
    cols, hidden_cols = mixer_gate.shape[1] // n_chip, up_gate.shape[1] // n_chip
    vmem, anywhere = pl.BlockSpec(memory_space=pltpu.VMEM), pl.BlockSpec(memory_space=pl.ANY)
    bf16, f32, dma = jnp.bfloat16, jnp.float32, pltpu.SemaphoreType.DMA
    in_specs = [anywhere, vmem, anywhere, anywhere] + [vmem] * 4 + [anywhere, vmem]
    in_specs += [anywhere, anywhere, vmem, vmem, anywhere]
    scratch = [
        pltpu.VMEM((width, cols), bf16),
        pltpu.VMEM((width, cols), bf16),
        pltpu.VMEM((n_fs, mixer_out.shape[0] // n_chip, mixer_out.shape[1]), bf16),
        pltpu.VMEM((width, hidden_cols), bf16),
        pltpu.VMEM((width, hidden_cols), bf16),
        pltpu.VMEM((n_fs, down_proj.shape[0] // n_chip, down_proj.shape[1]), bf16),
        pltpu.VMEM((team_rows, width), bf16),
        pltpu.VMEM((team_rows, width), bf16),
        pltpu.VMEM((team_rows, cols), f32),
        pltpu.VMEM((team_rows, cols), f32),
        pltpu.VMEM((team_rows, cols), bf16),
        pltpu.VMEM((team_rows, hidden_cols), f32),
        pltpu.VMEM((team_rows, hidden_cols), bf16),
        pltpu.VMEM((team_rows, width), bf16),
        pltpu.VMEM((n_chip * half, width), bf16),
        pltpu.VMEM((n_chip - 1, half, width), bf16),
        pltpu.VMEM((half, width), bf16),
        pltpu.VMEM((n_chip * n_tp, 2, team_rows), f32),
        dma((ARRAYS + 1,)),
        dma((ARRAYS, PLANE)),
        dma((ARRAYS, n_fs)),
        dma((ARRAYS, n_fs)),
        dma((ARRAYS, n_fs)),
        dma((2, n_chip)),
        dma((2, n_chip)),
        dma((2, n_chip)),
        dma((2, n_chip)),
        dma((n_chip * n_tp,)),
        dma((n_chip * n_tp,)),
        dma((2, n_line, n_chip)),
        dma((2, n_line, n_chip)),
        dma((2, n_line, 2 * FAR)),
        dma((2, n_line, 2 * FAR)),
        dma((2, n_chip)),
        dma((2, n_chip)),
        dma((2,)),
    ]
    return pl.pallas_call(
        functools.partial(team_kernel, dims),
        out_shape=jax.ShapeDtypeStruct((rows, width), bf16),
        in_specs=in_specs,
        out_specs=vmem,
        scratch_shapes=scratch,
        compiler_params=pltpu.CompilerParams(
            collective_id=0, has_side_effects=True, vmem_limit_bytes=63 * 1024 * 1024
        ),
    )(
        tokens,
        first_gain.reshape(1, -1),
        mixer_gate,
        mixer_value,
        value_gain.reshape(1, -1),
        value_shift.reshape(1, -1),
        spatial_weight,
        spatial_bias,
        mixer_out,
        second_gain.reshape(1, -1),
        up_gate,
        up_value,
        taps_gate,
        taps_value,
        down_proj,
    )


def team_fits(mesh):
    n_rep, n_fs, n_tp = (mesh.shape[name] for name in ("rep", "fs", "tp"))
    if n_tp != 2 or n_rep * PLANE != FAR + 1 or n_fs % PLANE:
        return False
    return D % (n_fs * GDIM) == 0 and D % (n_tp * n_rep * PLANE * GDIM) == 0


def solution(mesh):
    in_specs = (
        P(("rep", "fs"), None),
        P(),
        P("fs", "tp"),
        P("fs", "tp"),
        P(),
        P(),
        P(),
        P(),
        P("tp", "fs"),
        P(),
        P("fs", "tp"),
        P("fs", "tp"),
        P(),
        P(),
        P("tp", "fs"),
    )
    out_specs = P(("rep", "fs"), None)
    body = local
    if team_fits(mesh):
        dims = tuple(mesh.shape[name] for name in ("rep", "fs", "tp"))
        body = functools.partial(team_layer, dims)
    return jax.shard_map(body, mesh=mesh, in_specs=in_specs, out_specs=out_specs, check_vma=False)
```

```python
import functools

import jax
import jax.numpy as jnp
from jax import lax
from jax.experimental import pallas as pl
from jax.experimental.pallas import tpu as pltpu
from jax.sharding import PartitionSpec as P

D = 2048
GDIM = 128
BLK = 128
LEN = 128


def normalize(matrix, scale_gain):
    values = matrix.astype(jnp.float32)
    factor = lax.rsqrt(jnp.mean(values * values, axis=-1, keepdims=True) + 1e-06)
    return (values * factor * scale_gain).astype(jnp.bfloat16)


def causal_conv(values, tap_weights):
    by_sequence = values.reshape(-1, LEN, values.shape[-1])
    padded = jnp.pad(by_sequence, ((0, 0), (2, 0), (0, 0)))
    summed = (
        tap_weights[0] * padded[:, 0:LEN]
        + tap_weights[1] * padded[:, 1 : LEN + 1]
        + tap_weights[2] * padded[:, 2 : LEN + 2]
    )
    return summed.reshape(values.shape)


def local(
    tokens,
    first_gain,
    mixer_gate,
    mixer_value,
    value_gain,
    value_shift,
    spatial_weight,
    spatial_bias,
    mixer_out,
    second_gain,
    up_gate,
    up_value,
    taps_gate,
    taps_value,
    down_proj,
):
    n_rep, n_tp = lax.axis_size("rep"), lax.axis_size("tp")
    rep_index, tp_index = lax.axis_index("rep"), lax.axis_index("tp")
    team = ("rep", "tp")

    def part(array, axis):
        width = array.shape[axis] // n_rep
        return lax.dynamic_slice_in_dim(array, rep_index * width, width, axis)

    def own(array, width, axis):
        at = (tp_index * n_rep + rep_index) * width
        return lax.dynamic_slice_in_dim(array, at, width, axis)

    w_gate = lax.all_gather(part(mixer_gate, 1), "fs", axis=0, tiled=True)
    w_value = lax.all_gather(part(mixer_value, 1), "fs", axis=0, tiled=True)
    w_out = lax.all_gather(part(mixer_out, 0), "fs", axis=1, tiled=True)
    u_gate = lax.all_gather(part(up_gate, 1), "fs", axis=0, tiled=True)
    u_value = lax.all_gather(part(up_value, 1), "fs", axis=0, tiled=True)
    w_down = lax.all_gather(part(down_proj, 0), "fs", axis=1, tiled=True)

    row_share = tokens.shape[0] // n_tp
    kept_tokens = lax.dynamic_slice_in_dim(tokens, tp_index * row_share, row_share, 0)
    first = lax.all_gather(normalize(kept_tokens, first_gain), team, axis=0, tiled=True)
    row_count = first.shape[0]
    cols = w_gate.shape[1]
    gate_act = jax.nn.gelu(jnp.dot(first, w_gate, preferred_element_type=jnp.float32))
    value_act = jax.nn.gelu(jnp.dot(first, w_value, preferred_element_type=jnp.float32))
    value_sum, value_squares = lax.psum(
        (jnp.sum(value_act, axis=1), jnp.sum(value_act * value_act, axis=1)), team
    )
    row_mean = value_sum / D
    variance = value_squares / D - row_mean * row_mean
    centred = (
        (value_act - row_mean[:, None])
        * lax.rsqrt(variance[:, None] + 1e-05)
        * own(value_gain, cols, 0)
        + own(value_shift, cols, 0)
    ).astype(jnp.bfloat16)
    groups = cols // GDIM
    masked = own(spatial_weight, groups, 0) * jnp.tril(jnp.ones((BLK, BLK), jnp.bfloat16))
    blocks = centred.reshape(row_count // BLK, BLK, groups, GDIM)
    mixed_rows = (
        jnp.einsum("gts,bsgc->btgc", masked, blocks, preferred_element_type=jnp.float32)
        + own(spatial_bias, groups, 0).T[None, :, :, None]
    )
    gated_rows = (gate_act * mixed_rows.reshape(row_count, cols)).astype(jnp.bfloat16)
    summed = lax.psum_scatter(
        jnp.dot(gated_rows, w_out, preferred_element_type=jnp.float32).astype(jnp.bfloat16),
        team,
        scatter_dimension=0,
        tiled=True,
    ).astype(jnp.float32)
    residual = (kept_tokens.astype(jnp.float32) + summed).astype(jnp.bfloat16)
    second = lax.all_gather(normalize(residual, second_gain), team, axis=0, tiled=True)
    hidden_cols = u_gate.shape[1]
    gate_up = jnp.dot(second, u_gate, preferred_element_type=jnp.float32)
    value_up = jnp.dot(second, u_value, preferred_element_type=jnp.float32)
    hidden = (
        jax.nn.silu(causal_conv(gate_up, own(taps_gate, hidden_cols, 1)))
        * causal_conv(value_up, own(taps_value, hidden_cols, 1))
    ).astype(jnp.bfloat16)
    ffn_total = lax.psum_scatter(
        jnp.dot(hidden, w_down, preferred_element_type=jnp.float32).astype(jnp.bfloat16),
        team,
        scatter_dimension=0,
        tiled=True,
    ).astype(jnp.float32)
    final_rows = (residual.astype(jnp.float32) + ffn_total).astype(jnp.bfloat16)
    return lax.all_gather(final_rows, "tp", axis=0, tiled=True)


PLANE = 2
ARRAYS = 6
FAR = 3
MESH = pl.DeviceIdType.MESH


def team_kernel(
    dims,
    tokens,
    first_gain,
    mixer_gate,
    mixer_value,
    value_gain,
    value_shift,
    spatial_weight,
    spatial_bias,
    mixer_out,
    second_gain,
    up_gate,
    up_value,
    taps_gate,
    taps_value,
    down_proj,
    out,
    w_gate,
    w_value,
    w_out,
    w_ug,
    w_uv,
    w_down,
    tok,
    rows_in,
    gate_act,
    value_act,
    gated,
    gate_half,
    hidden,
    part,
    from_partner,
    from_team,
    residual,
    stats,
    mixing,
    taps,
    own_sem,
    side_send,
    up_send,
    down_send,
    weight_recv,
    team_send,
    team_recv,
    pass_send,
    pass_recv,
    stat_sem,
    pair_send,
    pair_recv,
    sum_send,
    sum_recv,
    cross_send,
    cross_recv,
    last_sem,
    local_sem,
):
    n_rep, n_fs, n_tp = dims
    n_side, n_line = PLANE, n_fs // PLANE
    n_chip = n_rep * n_side
    x, c = lax.axis_index("rep"), lax.axis_index("tp")
    f_own = lax.axis_index("fs")
    z, y = f_own // n_side, f_own % n_side
    other = (c + 1) % n_tp
    q_own = x * n_side + y
    rows = tokens.shape[0]
    half = rows // n_tp
    width = tokens.shape[1]
    sources = (mixer_value, mixer_gate, mixer_out, up_gate, up_value, down_proj)
    held = (w_value, w_gate, w_out, w_ug, w_uv, w_down)
    partner = (x, f_own, other)
    has_up, has_down = z + 1 < n_line, z >= 1
    at_end = (z == 0) | (z == n_line - 1)

    def chip_to(k, core):
        dx, dy = k // n_side, k % n_side
        return ((x + dx) % n_rep, z * n_side + (y + dy) % n_side, core)

    def chip_q(k, sign):
        dx, dy = k // n_side, k % n_side
        return ((x + sign * dx + n_rep) % n_rep) * n_side + (y + sign * dy + n_side) % n_side

    def remote(src, dst, send, recv, device):
        return pltpu.make_async_remote_copy(
            src_ref=src, dst_ref=dst, send_sem=send, recv_sem=recv, device_id=device, device_id_type=MESH
        )

    def all_sent(ref, sem):
        remote(ref, ref, sem, sem, partner).wait_send()

    def blocks_of(a, f, count):
        if len(held[a].shape) == 3:
            return held[a].at[pl.ds(f, count)]
        height = sources[a].shape[0]
        return held[a].at[pl.ds(pl.multiple_of(f * height, height), count * height)]

    def block(a, f):
        return held[a].at[f] if len(held[a].shape) == 3 else blocks_of(a, f, 1)

    def piece(a, q):
        if len(held[a].shape) == 3:
            height = sources[a].shape[0] // n_chip
            return sources[a].at[pl.ds(pl.multiple_of(q * height, height), height)]
        cols = sources[a].shape[1] // n_chip
        return sources[a].at[:, pl.ds(pl.multiple_of(q * cols, cols), cols)]

    def own_copy(a):
        return pltpu.make_async_copy(piece(a, q_own), block(a, f_own), own_sem.at[a])

    def side(a):
        to_y = (y + 1) % n_side
        return remote(
            piece(a, x * n_side + to_y),
            block(a, f_own),
            side_send.at[a],
            weight_recv.at[a, f_own],
            (x, z * n_side + to_y, c),
        )

    def along(a, f, step, src):
        sem = up_send if step == 1 else down_send
        return remote(
            src, block(a, f), sem.at[a], weight_recv.at[a, f], (x, f_own + step * n_side, c)
        )

    def landed(a, f):
        remote(block(a, f), block(a, f), side_send.at[a], weight_recv.at[a, f], partner).wait_recv()

    def send_line(a, f, src, up=True, down=True):
        if up:
            pl.when(has_up)(lambda: along(a, f, 1, src).start())
        if down:
            pl.when(has_down)(lambda: along(a, f, -1, src).start())

    def start_side(a):
        own_copy(a).start()
        side(a).start()

    def start_line(a):
        send_line(a, f_own, piece(a, q_own))

    def relay(a, *distances):
        for d in distances:
            if d == 0:
                f = z * n_side + (y + 1) % n_side
                landed(a, f)
                send_line(a, f, block(a, f))
                own_copy(a).wait()
                continue
            for j in range(n_side):

                @pl.when((z - d >= 0) & has_up)
                def _():
                    f = (z - d) * n_side + j
                    landed(a, f)
                    send_line(a, f, block(a, f), down=False)

                @pl.when((z + d < n_line) & has_down)
                def _():
                    f = (z + d) * n_side + j
                    landed(a, f)
                    send_line(a, f, block(a, f), up=False)

    beyond = tuple(range(2, n_line - 1))

    def arrived(a, f):
        pl.when(at_end & (f // n_side != z))(lambda: landed(a, f))

    def arrived_all(a):
        def body(f, carry):
            arrived(a, f)
            return carry

        lax.fori_loop(0, n_fs, body, 0)

    def chip_rows(q, core):
        return pl.ds(pl.multiple_of(q * rows + core * half, half), half)

    cuts = (half * 2 // 3 // 16 * 16, half // 2 // 16 * 16)

    def strip(g, k, forwarded):
        low = (k == 1) == forwarded
        return (0, cuts[g]) if low else (cuts[g], half - cuts[g])

    def strip_rows(buffer, g, k, forwarded, q):
        first, size = strip(g, k, forwarded)
        at = pl.multiple_of(q * rows + c * half + first, 16)
        return buffer.at[pl.ds(at, size)]

    def share(g, k, h, buffer, source, base):
        first, size = strip(g, k, h == 0)
        return remote(
            source.at[pl.ds(pl.multiple_of(base + first, 16), size)],
            strip_rows(buffer, g, k, h == 0, q_own),
            team_send.at[g],
            team_recv.at[g, 2 * (k - 1) + h],
            chip_to(k, c),
        )

    def share_landed(g, k, h, buffer):
        place = strip_rows(buffer, g, k, h == 0, chip_q(k, -1))
        sem = team_recv.at[g, 2 * (k - 1) + h]
        remote(place, place, team_send.at[g], sem, partner).wait_recv()

    def across(g, k, buffer):
        place = strip_rows(buffer, g, k, True, chip_q(k, -1))
        return remote(
            place, place, cross_send.at[g], cross_recv.at[g, k - 1], chip_to(FAR - k, c)
        )

    def across_landed(g, k, buffer):
        place = strip_rows(buffer, g, k, True, chip_q(FAR, -1))
        remote(place, place, cross_send.at[g], cross_recv.at[g, k - 1], partner).wait_recv()

    def hand_on(g, k, buffer):
        place = buffer.at[chip_rows(chip_q(k, -1), c)]
        return remote(place, place, pass_send.at[g], pass_recv.at[g, k], partner)

    def hand_landed(g, k, buffer):
        place = buffer.at[chip_rows(chip_q(k, -1), other)]
        remote(place, place, pass_send.at[g], pass_recv.at[g, k], partner).wait_recv()

    def norm_rows(values, gain):
        factor = lax.rsqrt(jnp.mean(values * values, axis=-1, keepdims=True) + 1e-06)
        return (values * factor * gain).astype(jnp.bfloat16)

    step_rows = 64

    def norm_chip(q):
        def body(i, carry):
            at = pl.ds(pl.multiple_of(q * rows + i * step_rows, step_rows), step_rows)
            rows_in[at, :] = norm_rows(tok[at, :].astype(jnp.float32), first_gain[...])
            return carry

        lax.fori_loop(0, rows // step_rows, body, 0)

    cols, hidden_cols = w_gate.shape[1], w_ug.shape[1]
    groups = cols // GDIM
    slot = c * n_chip + q_own
    at_hidden = pl.ds(pl.multiple_of(slot * hidden_cols, hidden_cols), hidden_cols)
    locals_in = (
        pltpu.make_async_copy(
            spatial_weight.at[pl.ds(slot * groups, groups)], mixing, local_sem.at[0]
        ),
        pltpu.make_async_copy(taps_gate.at[:, at_hidden], taps.at[0], local_sem.at[1]),
        pltpu.make_async_copy(taps_value.at[:, at_hidden], taps.at[1], local_sem.at[2]),
    )

    barrier = pltpu.get_barrier_semaphore()
    for k in range(n_chip):
        for core in (c, other):
            if k or core is other:
                pl.semaphore_signal(barrier, inc=1, device_id=chip_to(k, core), device_id_type=MESH)
    for flag, step in ((has_up, 1), (has_down, -1)):

        @pl.when(flag)
        def _():
            pl.semaphore_signal(
                barrier, inc=1, device_id=(x, f_own + step * n_side, c), device_id_type=MESH
            )

    neighbours = has_up.astype(jnp.int32) + has_down.astype(jnp.int32)
    pl.semaphore_wait(barrier, n_chip * n_tp - 1 + neighbours)

    for a in (0, 1):
        start_side(a)
        start_line(a)
    for h in (0, 1):
        for k in (2, 1):
            share(0, k, h, tok, tokens, c * half).start()
    tok_copy = pltpu.make_async_copy(
        tokens, tok.at[pl.ds(pl.multiple_of(q_own * rows, rows), rows)], own_sem.at[ARRAYS]
    )
    tok_copy.start()
    start_side(2)
    for copy in locals_in:
        copy.start()
    relay(0, 0)
    relay(1, 0)
    relay(0, 1)
    tok_copy.wait()
    norm_chip(q_own)
    share_landed(0, 2, 0, tok)
    across(0, 2, tok).start()
    relay(1, 1)
    share_landed(0, 1, 0, tok)
    across(0, 1, tok).start()
    start_side(3)
    relay(0, *beyond)
    share_landed(0, 2, 1, tok)
    hand_on(0, 2, tok).start()
    hand_landed(0, 2, tok)
    norm_chip(chip_q(2, -1))
    relay(1, *beyond)
    start_line(2)
    share_landed(0, 1, 1, tok)
    hand_on(0, 1, tok).start()
    relay(2, 0)
    hand_landed(0, 1, tok)
    norm_chip(chip_q(1, -1))
    relay(2, 1)
    for k in (1, 2):
        across_landed(0, k, tok)
    hand_on(0, FAR, tok).start()
    hand_landed(0, FAR, tok)
    norm_chip(chip_q(FAR, -1))

    def project(weight, target):
        def body(i, carry):
            at = pl.ds(pl.multiple_of(i * half, half), half)
            product = jnp.dot(rows_in[at, :], weight[...], preferred_element_type=jnp.float32)
            target[at, :] = jax.nn.gelu(product)
            return carry

        lax.fori_loop(0, n_chip * n_tp, body, 0)

    blocks = n_chip * rows // BLK
    lane = lax.broadcasted_iota(jnp.int32, (BLK, BLK), 1)
    sub = lax.broadcasted_iota(jnp.int32, (BLK, BLK), 0)
    arrived_all(0)
    project(w_value, value_act)

    def stat_body(i, carry):
        at = pl.ds(pl.multiple_of(i * BLK, BLK), BLK)
        values = value_act[at, :]
        total = jnp.sum(values, axis=1, keepdims=True)
        squares = jnp.sum(values * values, axis=1, keepdims=True)
        both = jnp.where(lane == 0, total, squares).T
        stats[0, :, at] = both[0:2, :]
        return carry

    lax.fori_loop(0, blocks, stat_body, 0)
    mates = [(k, j) for k in range(n_chip) for j in range(n_tp) if k or j]

    def tell(i):
        k, j = mates[i]
        device = chip_to(k, (c + j) % n_tp)
        return remote(stats.at[0], stats.at[i + 1], stat_sem.at[0], stat_sem.at[1], device)

    for i in range(len(mates)):
        tell(i).start()
    start_side(4)
    relay(2, *beyond)
    start_line(3)
    arrived_all(1)
    project(w_gate, gate_act)
    relay(3, 0)
    told = stats.at[pl.ds(1, len(mates))]
    remote(told, told, stat_sem.at[0], stat_sem.at[1], partner).wait_recv()
    for copy in locals_in:
        copy.wait()
    at_cols = pl.ds(pl.multiple_of(slot * cols, cols), cols)

    def mix_body(i, carry):
        at = pl.ds(pl.multiple_of(i * BLK, BLK), BLK)
        total = stats[0, :, at]
        for s in range(1, len(mates) + 1):
            total = total + stats[s, :, at]
        row_mean = jnp.broadcast_to(total[0:1, :] / width, (BLK, BLK)).T[:, 0:1]
        row_square = jnp.broadcast_to(total[1:2, :] / width, (BLK, BLK)).T[:, 0:1]
        variance = row_square - row_mean * row_mean
        centred = (
            (value_act[at, :] - row_mean) * lax.rsqrt(variance + 1e-05) * value_gain[:, at_cols]
            + value_shift[:, at_cols]
        ).astype(jnp.bfloat16)
        for g in range(groups):
            group = slot * groups + g
            matrix = mixing[g]
            matrix = jnp.where(sub >= lane, matrix, jnp.zeros_like(matrix))
            bias = jnp.broadcast_to(spatial_bias[pl.ds(group, 1), :], (BLK, BLK)).T
            mixed = (
                jnp.dot(
                    matrix, centred[:, g * GDIM : (g + 1) * GDIM], preferred_element_type=jnp.float32
                )
                + bias
            )
            channels = slice(g * GDIM, (g + 1) * GDIM)
            gated[at, channels] = (gate_act[at, channels] * mixed).astype(jnp.bfloat16)
        return carry

    lax.fori_loop(0, blocks, mix_body, 0)

    cut = w_out.shape[2]

    low = z < n_line // 2
    near_z = jnp.where(low, z, n_line - 1 - z)

    def line_f(u):
        i = u // n_side
        turn = near_z - (i + 1) // 2 if i % 2 else near_z + i // 2
        p = jnp.where(i > 2 * near_z, i, turn)
        return jnp.where(low, p, n_line - 1 - p) * n_side + u % n_side

    def unit_cols(u):
        return pl.ds(pl.multiple_of(line_f(u) * cut, cut), cut)

    def pair(u, i):
        q, place = chip_q(FAR - i, 1), unit_cols(u)
        return remote(
            part.at[chip_rows(q, other), place],
            from_partner.at[pl.ds(pl.multiple_of(q * half, half), half), place],
            pair_send.at[0],
            pair_recv.at[u, jnp.minimum(i, 1)],
            partner,
        )

    def lane_cols(u, near):
        return pl.ds(pl.multiple_of(line_f(u) * cut + (2 - near) * (cut // 2), cut // 2), cut // 2)

    def to_team(u, near, t):
        place = lane_cols(u, near)
        k_rows = (near, FAR, FAR - near)[t]
        k_chip = (near, near, FAR - near)[t]
        return remote(
            part.at[chip_rows(chip_q(k_rows, 1), c), place],
            from_team.at[t, :, place],
            sum_send.at[0],
            sum_recv.at[u, t % 2],
            chip_to(k_chip, c),
        )

    def multiply(u, acts, weight):
        def body(i, carry):
            q = chip_q(FAR - i, 1)
            at = pl.ds(pl.multiple_of(q * rows, rows), rows)
            part[at, unit_cols(u)] = jnp.dot(
                acts[at, :], weight[line_f(u)], preferred_element_type=jnp.float32
            ).astype(jnp.bfloat16)
            pair(u, i).start()
            return carry

        lax.fori_loop(0, n_chip, body, 0)

    def pair_landed(u, i):
        whole = from_partner.at[pl.ds(0, (1 + i * (n_chip - 2)) * half), unit_cols(u)]
        remote(whole, whole, pair_send.at[0], pair_recv.at[u, i], partner).wait_recv()

    def reduce_pair(u):
        place = unit_cols(u)
        for k in range(FAR, -1, -1):
            if k >= FAR - 1:
                pair_landed(u, FAR - k)
            q = chip_q(k, 1)
            at = chip_rows(q, c)
            part[at, place] = (
                part[at, place].astype(jnp.float32)
                + from_partner[pl.ds(pl.multiple_of(q * half, half), half), place].astype(
                    jnp.float32
                )
            ).astype(jnp.bfloat16)
            if k == FAR:
                for near in (2, 1):
                    to_team(u, near, 1).start()
            elif k:
                to_team(u, k, 0).start()

    def pass_on(u):
        both = from_team.at[1, :, unit_cols(u)]
        remote(both, both, sum_send.at[0], sum_recv.at[u, 1], partner).wait_recv()
        for near in (2, 1):
            at, place = chip_rows(chip_q(FAR - near, 1), c), lane_cols(u, near)
            part[at, place] = (
                part[at, place].astype(jnp.float32) + from_team[1, :, place].astype(jnp.float32)
            ).astype(jnp.bfloat16)
            to_team(u, near, 2).start()

    def collected(u):
        rest = from_team.at[pl.ds(0, 2), :, unit_cols(u)]
        remote(rest, rest, sum_send.at[0], sum_recv.at[u, 0], partner).wait_recv()

    units = n_line * n_side
    lag = 2

    def out_units(acts, weight, a):
        for u in range(units):
            if u == units // 2:
                relay(3, 1)
                start_line(4)
            arrived(a, line_f(u))
            multiply(u, acts, weight)
            if u:
                reduce_pair(u - 1)
            if u >= 2 * lag:
                pass_on(u - 2 * lag)
        reduce_pair(units - 1)

    out_units(gated, w_out, 2)
    for u in range(units - 2 * lag, units):
        pass_on(u)
    relay(3, *beyond)
    relay(4, 0)
    for u in range(units):
        collected(u)

    def residual_body(i, carry):
        at = pl.ds(pl.multiple_of(i * step_rows, step_rows), step_rows)
        mine = pl.ds(pl.multiple_of(q_own * rows + c * half + i * step_rows, step_rows), step_rows)
        total = part[mine, :].astype(jnp.float32)
        for t in (0, 2):
            total = total + from_team[t, at, :].astype(jnp.float32)
        kept = (tok[mine, :].astype(jnp.float32) + total).astype(jnp.bfloat16)
        residual[at, :] = kept
        rows_in[mine, :] = norm_rows(kept.astype(jnp.float32), second_gain[...])
        return carry

    lax.fori_loop(0, half // step_rows, residual_body, 0)
    for h in (0, 1):
        for k in (1, 2):
            share(1, k, h, rows_in, rows_in, q_own * rows + c * half).start()
    hand_on(1, 0, rows_in).start()
    all_sent(from_partner, pair_send.at[0])
    all_sent(from_team, sum_send.at[0])
    for k in (1, 2):
        share_landed(1, k, 0, rows_in)
        across(1, k, rows_in).start()
    start_side(5)
    relay(4, 1)
    for k in (1, 2):
        share_landed(1, k, 1, rows_in)
        hand_on(1, k, rows_in).start()
    relay(4, *beyond)
    start_line(5)

    position = lax.broadcasted_iota(jnp.int32, (LEN, hidden_cols), 0)

    def conv(values, which):
        back1 = jnp.where(position >= 1, pltpu.roll(values, 1, 0), 0.0)
        back2 = jnp.where(position >= 2, pltpu.roll(values, 2, 0), 0.0)
        weights = taps[which]
        return weights[0:1] * back2 + weights[1:2] * back1 + weights[2:3] * values

    def raise_chip(weight, which, q):
        at = pl.ds(pl.multiple_of(q * rows, rows), rows)
        product = jnp.dot(rows_in[at, :], weight[...], preferred_element_type=jnp.float32)
        for s in range(rows // LEN):
            here = pl.ds(pl.multiple_of(q * rows + s * LEN, LEN), LEN)
            done = conv(product[s * LEN : (s + 1) * LEN], which)
            if which:
                hidden[here, :] = (gate_half[here, :] * done).astype(jnp.bfloat16)
            else:
                gate_half[here, :] = jax.nn.silu(done)

    def raise_gate(k, carry):
        hand_landed(1, k, rows_in)
        raise_chip(w_ug, 0, chip_q(k, -1))
        return carry

    def raise_value(q, carry):
        raise_chip(w_uv, 1, q)
        return carry

    arrived_all(3)
    lax.fori_loop(0, FAR, raise_gate, 0)
    for k in (1, 2):
        across_landed(1, k, rows_in)
    hand_on(1, FAR, rows_in).start()
    relay(5, 0)
    lax.fori_loop(FAR, n_chip, raise_gate, 0)
    arrived_all(4)
    lax.fori_loop(0, n_chip, raise_value, 0)

    def finish(u):
        collected(u)
        place = unit_cols(u)
        mine = chip_rows(q_own, c)
        here = pl.ds(pl.multiple_of(c * half, half), half)
        total = part[mine, place].astype(jnp.float32)
        for t in (0, 2):
            total = total + from_team[t, :, place].astype(jnp.float32)
        out[here, place] = (residual[:, place].astype(jnp.float32) + total).astype(jnp.bfloat16)
        done = out.at[here, place]
        remote(done, done, last_sem.at[0], last_sem.at[1], partner).start()

    passed = 0
    for u in range(units):
        if u == n_side:
            relay(5, 1)
        elif u % n_side == 0 and u // n_side - 1 in beyond:
            relay(5, u // n_side - 1)
        arrived(5, line_f(u))
        multiply(u, hidden, w_down)
        for v in range(passed, u if u > units // 2 else u - 1):
            pass_on(v)
            passed = v + 1
        reduce_pair(u)
    for u in range(units - 2):
        finish(u)
    pass_on(units - 1)
    for u in range(units - 2, units):
        finish(u)

    for a in range(ARRAYS):
        all_sent(block(a, 0), side_send.at[a])
        for n in range(1, n_line):
            pl.when(z == n - 1)(lambda: all_sent(blocks_of(a, 0, n * n_side), up_send.at[a]))
            pl.when(z == n)(
                lambda: all_sent(
                    blocks_of(a, n * n_side, (n_line - n) * n_side), down_send.at[a]
                )
            )
    all_sent(told, stat_sem.at[0])
    for g in range(2):
        all_sent(tok.at[pl.ds(0, rows)], team_send.at[g])
        all_sent(tok.at[pl.ds(0, half)], cross_send.at[g])
        all_sent(tok.at[pl.ds(0, (n_chip - 1 + g) * half)], pass_send.at[g])
    all_sent(from_partner, pair_send.at[0])
    all_sent(from_team, sum_send.at[0])
    theirs = out.at[pl.ds(pl.multiple_of(other * half, half), half)]
    last = remote(theirs, theirs, last_sem.at[0], last_sem.at[1], partner)
    last.wait_send()
    last.wait_recv()


def team_layer(
    dims,
    tokens,
    first_gain,
    mixer_gate,
    mixer_value,
    value_gain,
    value_shift,
    spatial_weight,
    spatial_bias,
    mixer_out,
    second_gain,
    up_gate,
    up_value,
    taps_gate,
    taps_value,
    down_proj,
):
    n_rep, n_fs, n_tp = dims
    n_chip, n_line = n_rep * PLANE, n_fs // PLANE
    rows, width = tokens.shape
    half, team_rows = rows // n_tp, rows * n_chip
    cols, hidden_cols = mixer_gate.shape[1] // n_chip, up_gate.shape[1] // n_chip
    vmem, anywhere = pl.BlockSpec(memory_space=pltpu.VMEM), pl.BlockSpec(memory_space=pl.ANY)
    bf16, f32, dma = jnp.bfloat16, jnp.float32, pltpu.SemaphoreType.DMA
    in_specs = [anywhere, vmem, anywhere, anywhere, vmem, vmem, anywhere, vmem, anywhere, vmem]
    in_specs += [anywhere] * 5
    units = n_fs
    scratch = [
        pltpu.VMEM((width, cols), bf16),
        pltpu.VMEM((width, cols), bf16),
        pltpu.VMEM((n_fs, mixer_out.shape[0] // n_chip, mixer_out.shape[1]), bf16),
        pltpu.VMEM((width, hidden_cols), bf16),
        pltpu.VMEM((width, hidden_cols), bf16),
        pltpu.VMEM((n_fs, down_proj.shape[0] // n_chip, down_proj.shape[1]), bf16),
        pltpu.VMEM((team_rows, width), bf16),
        pltpu.VMEM((team_rows, width), bf16),
        pltpu.VMEM((team_rows, cols), f32),
        pltpu.VMEM((team_rows, cols), f32),
        pltpu.VMEM((team_rows, cols), bf16),
        pltpu.VMEM((team_rows, hidden_cols), f32),
        pltpu.VMEM((team_rows, hidden_cols), bf16),
        pltpu.VMEM((team_rows, width), bf16),
        pltpu.VMEM((n_chip * half, width), bf16),
        pltpu.VMEM((n_chip - 1, half, width), bf16),
        pltpu.VMEM((half, width), bf16),
        pltpu.VMEM((n_chip * n_tp, 2, team_rows), f32),
        pltpu.VMEM((cols // GDIM,) + spatial_weight.shape[1:], bf16),
        pltpu.VMEM((2, 3, hidden_cols), f32),
        dma((ARRAYS + 1,)),
        dma((ARRAYS,)),
        dma((ARRAYS,)),
        dma((ARRAYS,)),
        dma((ARRAYS, n_fs)),
        dma((2,)),
        dma((2, 4)),
        dma((2,)),
        dma((2, n_chip)),
        dma((2,)),
        dma((1,)),
        dma((units, 2)),
        dma((1,)),
        dma((units, 2)),
        dma((2,)),
        dma((2, 2)),
        dma((2,)),
        dma((3,)),
    ]
    return pl.pallas_call(
        functools.partial(team_kernel, dims),
        out_shape=pltpu.VMEM((rows, width), bf16),
        in_specs=in_specs,
        out_specs=vmem,
        scratch_shapes=scratch,
        compiler_params=pltpu.CompilerParams(
            collective_id=0, has_side_effects=True, vmem_limit_bytes=56 * 1024 * 1024
        ),
    )(
        tokens,
        first_gain.reshape(1, -1),
        mixer_gate,
        mixer_value,
        value_gain.reshape(1, -1),
        value_shift.reshape(1, -1),
        spatial_weight,
        spatial_bias,
        mixer_out,
        second_gain.reshape(1, -1),
        up_gate,
        up_value,
        taps_gate,
        taps_value,
        down_proj,
    )


def team_fits(mesh):
    n_rep, n_fs, n_tp = (mesh.shape[name] for name in ("rep", "fs", "tp"))
    if n_tp != 2 or n_rep * PLANE != FAR + 1 or n_fs % PLANE:
        return False
    return D % (n_fs * GDIM) == 0 and D % (n_tp * n_rep * PLANE * GDIM) == 0


def solution(mesh):
    in_specs = (
        P(("rep", "fs"), None),
        P(),
        P("fs", "tp"),
        P("fs", "tp"),
        P(),
        P(),
        P(),
        P(),
        P("tp", "fs"),
        P(),
        P("fs", "tp"),
        P("fs", "tp"),
        P(),
        P(),
        P("tp", "fs"),
    )
    out_specs = P(("rep", "fs"), None)
    body = local
    if team_fits(mesh):
        dims = tuple(mesh.shape[name] for name in ("rep", "fs", "tp"))
        body = functools.partial(team_layer, dims)
    return jax.shard_map(body, mesh=mesh, in_specs=in_specs, out_specs=out_specs, check_vma=False)
```

```python
import functools

import jax
import jax.numpy as jnp
from jax import lax
from jax.experimental import pallas as pl
from jax.experimental.pallas import tpu as pltpu
from jax.sharding import PartitionSpec as P

D = 2048
GDIM = 128
BLK = 128
LEN = 128


def normalize(matrix, scale_gain):
    values = matrix.astype(jnp.float32)
    factor = lax.rsqrt(jnp.mean(values * values, axis=-1, keepdims=True) + 1e-06)
    return (values * factor * scale_gain).astype(jnp.bfloat16)


def causal_conv(values, tap_weights):
    by_sequence = values.reshape(-1, LEN, values.shape[-1])
    padded = jnp.pad(by_sequence, ((0, 0), (2, 0), (0, 0)))
    summed = (
        tap_weights[0] * padded[:, 0:LEN]
        + tap_weights[1] * padded[:, 1 : LEN + 1]
        + tap_weights[2] * padded[:, 2 : LEN + 2]
    )
    return summed.reshape(values.shape)


def local(
    tokens,
    first_gain,
    mixer_gate,
    mixer_value,
    value_gain,
    value_shift,
    spatial_weight,
    spatial_bias,
    mixer_out,
    second_gain,
    up_gate,
    up_value,
    taps_gate,
    taps_value,
    down_proj,
):
    n_rep, n_tp = lax.axis_size("rep"), lax.axis_size("tp")
    rep_index, tp_index = lax.axis_index("rep"), lax.axis_index("tp")
    team = ("rep", "tp")

    def part(array, axis):
        width = array.shape[axis] // n_rep
        return lax.dynamic_slice_in_dim(array, rep_index * width, width, axis)

    def own(array, width, axis):
        at = (tp_index * n_rep + rep_index) * width
        return lax.dynamic_slice_in_dim(array, at, width, axis)

    w_gate = lax.all_gather(part(mixer_gate, 1), "fs", axis=0, tiled=True)
    w_value = lax.all_gather(part(mixer_value, 1), "fs", axis=0, tiled=True)
    w_out = lax.all_gather(part(mixer_out, 0), "fs", axis=1, tiled=True)
    u_gate = lax.all_gather(part(up_gate, 1), "fs", axis=0, tiled=True)
    u_value = lax.all_gather(part(up_value, 1), "fs", axis=0, tiled=True)
    w_down = lax.all_gather(part(down_proj, 0), "fs", axis=1, tiled=True)

    row_share = tokens.shape[0] // n_tp
    kept_tokens = lax.dynamic_slice_in_dim(tokens, tp_index * row_share, row_share, 0)
    first = lax.all_gather(normalize(kept_tokens, first_gain), team, axis=0, tiled=True)
    row_count = first.shape[0]
    cols = w_gate.shape[1]
    gate_act = jax.nn.gelu(jnp.dot(first, w_gate, preferred_element_type=jnp.float32))
    value_act = jax.nn.gelu(jnp.dot(first, w_value, preferred_element_type=jnp.float32))
    value_sum, value_squares = lax.psum(
        (jnp.sum(value_act, axis=1), jnp.sum(value_act * value_act, axis=1)), team
    )
    row_mean = value_sum / D
    variance = value_squares / D - row_mean * row_mean
    centred = (
        (value_act - row_mean[:, None])
        * lax.rsqrt(variance[:, None] + 1e-05)
        * own(value_gain, cols, 0)
        + own(value_shift, cols, 0)
    ).astype(jnp.bfloat16)
    groups = cols // GDIM
    masked = own(spatial_weight, groups, 0) * jnp.tril(jnp.ones((BLK, BLK), jnp.bfloat16))
    blocks = centred.reshape(row_count // BLK, BLK, groups, GDIM)
    mixed_rows = (
        jnp.einsum("gts,bsgc->btgc", masked, blocks, preferred_element_type=jnp.float32)
        + own(spatial_bias, groups, 0).T[None, :, :, None]
    )
    gated_rows = (gate_act * mixed_rows.reshape(row_count, cols)).astype(jnp.bfloat16)
    summed = lax.psum_scatter(
        jnp.dot(gated_rows, w_out, preferred_element_type=jnp.float32).astype(jnp.bfloat16),
        team,
        scatter_dimension=0,
        tiled=True,
    ).astype(jnp.float32)
    residual = (kept_tokens.astype(jnp.float32) + summed).astype(jnp.bfloat16)
    second = lax.all_gather(normalize(residual, second_gain), team, axis=0, tiled=True)
    hidden_cols = u_gate.shape[1]
    gate_up = jnp.dot(second, u_gate, preferred_element_type=jnp.float32)
    value_up = jnp.dot(second, u_value, preferred_element_type=jnp.float32)
    hidden = (
        jax.nn.silu(causal_conv(gate_up, own(taps_gate, hidden_cols, 1)))
        * causal_conv(value_up, own(taps_value, hidden_cols, 1))
    ).astype(jnp.bfloat16)
    ffn_total = lax.psum_scatter(
        jnp.dot(hidden, w_down, preferred_element_type=jnp.float32).astype(jnp.bfloat16),
        team,
        scatter_dimension=0,
        tiled=True,
    ).astype(jnp.float32)
    final_rows = (residual.astype(jnp.float32) + ffn_total).astype(jnp.bfloat16)
    return lax.all_gather(final_rows, "tp", axis=0, tiled=True)


PLANE = 2
ARRAYS = 6
FAR = 3
MESH = pl.DeviceIdType.MESH


def team_kernel(
    dims,
    tokens,
    first_gain,
    mixer_gate,
    mixer_value,
    value_gain,
    value_shift,
    spatial_weight,
    spatial_bias,
    mixer_out,
    second_gain,
    up_gate,
    up_value,
    taps_gate,
    taps_value,
    down_proj,
    out,
    w_gate,
    w_value,
    w_out,
    w_ug,
    w_uv,
    w_down,
    tok,
    rows_in,
    gate_act,
    value_act,
    gated,
    gate_half,
    hidden,
    part,
    from_partner,
    from_team,
    residual,
    stats,
    mixing,
    taps,
    gains,
    scales,
    biases,
    own_sem,
    side_send,
    up_send,
    down_send,
    weight_recv,
    team_send,
    team_recv,
    pass_send,
    pass_recv,
    stat_sem,
    pair_send,
    pair_recv,
    sum_send,
    sum_recv,
    cross_send,
    cross_recv,
    last_sem,
    local_sem,
):
    n_rep, n_fs, n_tp = dims
    n_side, n_line = PLANE, n_fs // PLANE
    n_chip = n_rep * n_side
    x, c = lax.axis_index("rep"), lax.axis_index("tp")
    f_own = lax.axis_index("fs")
    z, y = f_own // n_side, f_own % n_side
    other = (c + 1) % n_tp
    q_own = x * n_side + y
    rows = tokens.shape[0]
    half = rows // n_tp
    width = tokens.shape[1]
    sources = (mixer_value, mixer_gate, mixer_out, up_gate, up_value, down_proj)
    held = (w_value, w_gate, w_out, w_ug, w_uv, w_down)
    partner = (x, f_own, other)
    has_up, has_down = z + 1 < n_line, z >= 1
    at_end = (z == 0) | (z == n_line - 1)
    low = z < n_line // 2

    def chip_to(k, core):
        dx, dy = k // n_side, k % n_side
        return ((x + dx) % n_rep, z * n_side + (y + dy) % n_side, core)

    def chip_q(k, sign):
        dx, dy = k // n_side, k % n_side
        return ((x + sign * dx + n_rep) % n_rep) * n_side + (y + sign * dy + n_side) % n_side

    def remote(src, dst, send, recv, device):
        return pltpu.make_async_remote_copy(
            src_ref=src, dst_ref=dst, send_sem=send, recv_sem=recv, device_id=device, device_id_type=MESH
        )

    def all_sent(ref, sem):
        remote(ref, ref, sem, sem, partner).wait_send()

    def blocks_of(a, f, count):
        if len(held[a].shape) == 3:
            return held[a].at[pl.ds(f, count)]
        height = sources[a].shape[0]
        return held[a].at[pl.ds(pl.multiple_of(f * height, height), count * height)]

    def block(a, f):
        return held[a].at[f] if len(held[a].shape) == 3 else blocks_of(a, f, 1)

    def piece(a, q):
        if len(held[a].shape) == 3:
            height = sources[a].shape[0] // n_chip
            return sources[a].at[pl.ds(pl.multiple_of(q * height, height), height)]
        cols = sources[a].shape[1] // n_chip
        return sources[a].at[:, pl.ds(pl.multiple_of(q * cols, cols), cols)]

    def own_copy(a):
        return pltpu.make_async_copy(piece(a, q_own), block(a, f_own), own_sem.at[a])

    def side(a):
        to_y = (y + 1) % n_side
        return remote(
            piece(a, x * n_side + to_y),
            block(a, f_own),
            side_send.at[a],
            weight_recv.at[a, f_own],
            (x, z * n_side + to_y, c),
        )

    def along(a, f, step, src):
        sem = up_send if step == 1 else down_send
        return remote(
            src, block(a, f), sem.at[a], weight_recv.at[a, f], (x, f_own + step * n_side, c)
        )

    def landed(a, f):
        remote(block(a, f), block(a, f), side_send.at[a], weight_recv.at[a, f], partner).wait_recv()

    def send_line(a, f, src, up=True, down=True):
        if up:
            pl.when(has_up)(lambda: along(a, f, 1, src).start())
        if down:
            pl.when(has_down)(lambda: along(a, f, -1, src).start())

    def start_side(a):
        own_copy(a).start()
        side(a).start()

    def start_line(a):
        send_line(a, f_own, piece(a, q_own))

    def relay(a, *distances):
        for d in distances:
            if d == 0:
                f = z * n_side + (y + 1) % n_side
                landed(a, f)
                send_line(a, f, block(a, f))
                own_copy(a).wait()
                continue
            for j in range(n_side):
                turn = j if a in (2, 5) else (y + j) % n_side
                for first in (True, False):
                    above = low if first else jnp.logical_not(low)

                    @pl.when((z + d < n_line) & has_down & above)
                    def _():
                        f = (z + d) * n_side + turn
                        landed(a, f)
                        send_line(a, f, block(a, f), up=False)

                    if first:

                        @pl.when((z - d >= 0) & has_up)
                        def _():
                            f = (z - d) * n_side + turn
                            landed(a, f)
                            send_line(a, f, block(a, f), down=False)

    beyond = tuple(range(2, n_line - 1))

    def arrived(a, f):
        pl.when(at_end & (f // n_side != z))(lambda: landed(a, f))

    def arrived_all(a):
        def body(f, carry):
            arrived(a, f)
            return carry

        lax.fori_loop(0, n_fs, body, 0)

    def chip_rows(q, core):
        return pl.ds(pl.multiple_of(q * rows + core * half, half), half)

    cuts = (half * 2 // 3 // 16 * 16, half // 2 // 16 * 16)

    def strip(g, k, forwarded):
        low = (k == 1) == forwarded
        return (0, cuts[g]) if low else (cuts[g], half - cuts[g])

    def strip_rows(buffer, g, k, forwarded, q):
        first, size = strip(g, k, forwarded)
        at = pl.multiple_of(q * rows + c * half + first, 16)
        return buffer.at[pl.ds(at, size)]

    def share(g, k, h, buffer, source, base):
        first, size = strip(g, k, h == 0)
        return remote(
            source.at[pl.ds(pl.multiple_of(base + first, 16), size)],
            strip_rows(buffer, g, k, h == 0, q_own),
            team_send.at[g],
            team_recv.at[g, 2 * (k - 1) + h],
            chip_to(k, c),
        )

    def share_landed(g, k, h, buffer):
        place = strip_rows(buffer, g, k, h == 0, chip_q(k, -1))
        sem = team_recv.at[g, 2 * (k - 1) + h]
        remote(place, place, team_send.at[g], sem, partner).wait_recv()

    def across(g, k, buffer):
        place = strip_rows(buffer, g, k, True, chip_q(k, -1))
        return remote(
            place, place, cross_send.at[g], cross_recv.at[g, k - 1], chip_to(FAR - k, c)
        )

    def across_landed(g, k, buffer):
        place = strip_rows(buffer, g, k, True, chip_q(FAR, -1))
        remote(place, place, cross_send.at[g], cross_recv.at[g, k - 1], partner).wait_recv()

    def hand_on(g, k, buffer):
        place = buffer.at[chip_rows(chip_q(k, -1), c)]
        return remote(place, place, pass_send.at[g], pass_recv.at[g, k], partner)

    def hand_landed(g, k, buffer):
        place = buffer.at[chip_rows(chip_q(k, -1), other)]
        remote(place, place, pass_send.at[g], pass_recv.at[g, k], partner).wait_recv()

    def norm_rows(values, gain):
        factor = lax.rsqrt(jnp.mean(values * values, axis=-1, keepdims=True) + 1e-06)
        return (values * factor * gain).astype(jnp.bfloat16)

    step_rows = 64

    def norm_chip(q):
        def body(i, carry):
            at = pl.ds(pl.multiple_of(q * rows + i * step_rows, step_rows), step_rows)
            rows_in[at, :] = norm_rows(tok[at, :].astype(jnp.float32), gains[0:1, :])
            return carry

        lax.fori_loop(0, rows // step_rows, body, 0)

    cols, hidden_cols = w_gate.shape[1], w_ug.shape[1]
    groups = cols // GDIM
    slot = c * n_chip + q_own
    at_hidden = pl.ds(pl.multiple_of(slot * hidden_cols, hidden_cols), hidden_cols)
    at_cols = pl.ds(pl.multiple_of(slot * cols, cols), cols)
    first_gain_in = pltpu.make_async_copy(first_gain, gains.at[0:1], local_sem.at[3])
    locals_in = (
        pltpu.make_async_copy(second_gain, gains.at[1:2], local_sem.at[4]),
        pltpu.make_async_copy(value_gain.at[:, at_cols], scales.at[0:1], local_sem.at[5]),
        pltpu.make_async_copy(value_shift.at[:, at_cols], scales.at[1:2], local_sem.at[6]),
        pltpu.make_async_copy(spatial_bias, biases, local_sem.at[7]),
        pltpu.make_async_copy(
            spatial_weight.at[pl.ds(slot * groups, groups)], mixing, local_sem.at[0]
        ),
        pltpu.make_async_copy(taps_gate.at[:, at_hidden], taps.at[0], local_sem.at[1]),
        pltpu.make_async_copy(taps_value.at[:, at_hidden], taps.at[1], local_sem.at[2]),
    )

    barrier = pltpu.get_barrier_semaphore()
    for mate in (chip_to(1, c), chip_to(2, c), partner):
        pl.semaphore_signal(barrier, inc=1, device_id=mate, device_id_type=MESH)
    for flag, step in ((has_up, 1), (has_down, -1)):

        @pl.when(flag)
        def _():
            pl.semaphore_signal(
                barrier, inc=1, device_id=(x, f_own + step * n_side, c), device_id_type=MESH
            )

    neighbours = has_up.astype(jnp.int32) + has_down.astype(jnp.int32)
    pl.semaphore_wait(barrier, FAR + neighbours)

    for a in (0, 1):
        start_side(a)
        start_line(a)
    for h in (0, 1):
        for k in (2, 1):
            share(0, k, h, tok, tokens, c * half).start()
    tok_copy = pltpu.make_async_copy(
        tokens, tok.at[pl.ds(pl.multiple_of(q_own * rows, rows), rows)], own_sem.at[ARRAYS]
    )
    tok_copy.start()
    start_side(2)
    first_gain_in.start()
    for copy in locals_in:
        copy.start()
    relay(0, 0)
    relay(1, 0)
    relay(0, 1)
    tok_copy.wait()
    first_gain_in.wait()
    norm_chip(q_own)
    share_landed(0, 2, 0, tok)
    across(0, 2, tok).start()
    relay(1, 1)
    share_landed(0, 1, 0, tok)
    across(0, 1, tok).start()
    start_side(3)
    relay(0, *beyond)
    share_landed(0, 2, 1, tok)
    hand_on(0, 2, tok).start()
    hand_landed(0, 2, tok)
    norm_chip(chip_q(2, -1))
    relay(1, *beyond)
    start_line(2)
    share_landed(0, 1, 1, tok)
    hand_on(0, 1, tok).start()
    relay(2, 0)
    hand_landed(0, 1, tok)
    norm_chip(chip_q(1, -1))
    relay(2, 1)
    for k in (1, 2):
        across_landed(0, k, tok)
    hand_on(0, FAR, tok).start()
    hand_landed(0, FAR, tok)
    norm_chip(chip_q(FAR, -1))

    def project(weight, target):
        def body(i, carry):
            at = pl.ds(pl.multiple_of(i * half, half), half)
            product = jnp.dot(rows_in[at, :], weight[...], preferred_element_type=jnp.float32)
            target[at, :] = jax.nn.gelu(product)
            return carry

        lax.fori_loop(0, n_chip * n_tp, body, 0)

    blocks = n_chip * rows // BLK
    lane = lax.broadcasted_iota(jnp.int32, (BLK, BLK), 1)
    sub = lax.broadcasted_iota(jnp.int32, (BLK, BLK), 0)
    arrived_all(0)
    project(w_value, value_act)

    def stat_body(i, carry):
        at = pl.ds(pl.multiple_of(i * BLK, BLK), BLK)
        values = value_act[at, :]
        total = jnp.sum(values, axis=1, keepdims=True)
        squares = jnp.sum(values * values, axis=1, keepdims=True)
        both = jnp.where(lane == 0, total, squares).T
        stats[0, :, at] = both[0:2, :]
        return carry

    lax.fori_loop(0, blocks, stat_body, 0)
    mates = [(k, j) for k in range(n_chip) for j in range(n_tp) if k or j]

    def tell(i):
        k, j = mates[i]
        device = chip_to(k, (c + j) % n_tp)
        return remote(stats.at[0], stats.at[i + 1], stat_sem.at[0], stat_sem.at[1], device)

    for i in range(len(mates)):
        tell(i).start()
    start_side(4)
    relay(2, *beyond)
    start_line(3)
    arrived_all(1)
    project(w_gate, gate_act)
    relay(3, 0)
    told = stats.at[pl.ds(1, len(mates))]
    remote(told, told, stat_sem.at[0], stat_sem.at[1], partner).wait_recv()
    for copy in locals_in:
        copy.wait()

    def mix_body(i, carry):
        at = pl.ds(pl.multiple_of(i * BLK, BLK), BLK)
        total = stats[0, :, at]
        for s in range(1, len(mates) + 1):
            total = total + stats[s, :, at]
        row_mean = jnp.broadcast_to(total[0:1, :] / width, (BLK, BLK)).T[:, 0:1]
        row_square = jnp.broadcast_to(total[1:2, :] / width, (BLK, BLK)).T[:, 0:1]
        variance = row_square - row_mean * row_mean
        centred = (
            (value_act[at, :] - row_mean) * lax.rsqrt(variance + 1e-05) * scales[0:1, :]
            + scales[1:2, :]
        ).astype(jnp.bfloat16)
        for g in range(groups):
            group = slot * groups + g
            matrix = mixing[g]
            matrix = jnp.where(sub >= lane, matrix, jnp.zeros_like(matrix))
            bias = jnp.broadcast_to(biases[pl.ds(group, 1), :], (BLK, BLK)).T
            mixed = (
                jnp.dot(
                    matrix, centred[:, g * GDIM : (g + 1) * GDIM], preferred_element_type=jnp.float32
                )
                + bias
            )
            channels = slice(g * GDIM, (g + 1) * GDIM)
            gated[at, channels] = (gate_act[at, channels] * mixed).astype(jnp.bfloat16)
        return carry

    lax.fori_loop(0, blocks, mix_body, 0)

    cut = w_out.shape[2]
    units = n_line * n_side

    near_z = jnp.where(low, z, n_line - 1 - z)

    def line_f(u):
        i = u // n_side
        turn = near_z - (i + 1) // 2 if i % 2 else near_z + i // 2
        p = jnp.where(i > 2 * near_z, i, turn)
        return jnp.where(low, p, n_line - 1 - p) * n_side + u % n_side

    def unit_cols(u):
        return pl.ds(pl.multiple_of(line_f(u) * cut, cut), cut)

    def pair(u, i):
        q, place = chip_q(FAR - i, 1), unit_cols(u)
        return remote(
            part.at[chip_rows(q, other), place],
            from_partner.at[pl.ds(pl.multiple_of(q * half, half), half), place],
            pair_send.at[0],
            pair_recv.at[u, jnp.minimum(i, 1)],
            partner,
        )

    def lane_cols(u, near):
        return pl.ds(pl.multiple_of(line_f(u) * cut + (2 - near) * (cut // 2), cut // 2), cut // 2)

    def to_team(u, near, t):
        place = lane_cols(u, near)
        k_rows = (near, FAR, FAR - near)[t]
        k_chip = (near, near, FAR - near)[t]
        return remote(
            part.at[chip_rows(chip_q(k_rows, 1), c), place],
            from_team.at[t, :, place],
            sum_send.at[0],
            sum_recv.at[u, t % 2],
            chip_to(k_chip, c),
        )

    def multiply(u, acts, weight):
        def body(i, carry):
            q = chip_q(FAR - i, 1)
            at = pl.ds(pl.multiple_of(q * rows, rows), rows)
            part[at, unit_cols(u)] = jnp.dot(
                acts[at, :], weight[line_f(u)], preferred_element_type=jnp.float32
            ).astype(jnp.bfloat16)
            pair(u, i).start()
            return carry

        lax.fori_loop(0, n_chip, body, 0)

    def pair_landed(u, i):
        whole = from_partner.at[pl.ds(0, (1 + i * (n_chip - 2)) * half), unit_cols(u)]
        remote(whole, whole, pair_send.at[0], pair_recv.at[u, i], partner).wait_recv()

    def reduce_pair(u):
        place = unit_cols(u)
        for k in range(FAR, -1, -1):
            if k >= FAR - 1:
                pair_landed(u, FAR - k)
            q = chip_q(k, 1)
            at = chip_rows(q, c)
            part[at, place] = (
                part[at, place].astype(jnp.float32)
                + from_partner[pl.ds(pl.multiple_of(q * half, half), half), place].astype(
                    jnp.float32
                )
            ).astype(jnp.bfloat16)
            if k == FAR:
                for near in (2, 1):
                    to_team(u, near, 1).start()
            elif k:
                to_team(u, k, 0).start()

    def pass_on(u):
        both = from_team.at[1, :, unit_cols(u)]
        remote(both, both, sum_send.at[0], sum_recv.at[u, 1], partner).wait_recv()
        for near in (2, 1):
            at, place = chip_rows(chip_q(FAR - near, 1), c), lane_cols(u, near)
            part[at, place] = (
                part[at, place].astype(jnp.float32) + from_team[1, :, place].astype(jnp.float32)
            ).astype(jnp.bfloat16)
            to_team(u, near, 2).start()

    def collected(u):
        rest = from_team.at[pl.ds(0, 2), :, unit_cols(u)]
        remote(rest, rest, sum_send.at[0], sum_recv.at[u, 0], partner).wait_recv()

    lag = 2

    def out_units(acts, weight, a):
        for u in range(units):
            if u == units // 2:
                relay(3, 1)
                start_line(4)
            arrived(a, line_f(u))
            multiply(u, acts, weight)
            if u:
                reduce_pair(u - 1)
            if u >= 2 * lag:
                pass_on(u - 2 * lag)
        reduce_pair(units - 1)

    out_units(gated, w_out, 2)
    for u in range(units - 2 * lag, units):
        pass_on(u)
    relay(3, *beyond)
    relay(4, 0)
    for u in range(units):
        collected(u)

    def residual_body(i, carry):
        at = pl.ds(pl.multiple_of(i * step_rows, step_rows), step_rows)
        mine = pl.ds(pl.multiple_of(q_own * rows + c * half + i * step_rows, step_rows), step_rows)
        total = part[mine, :].astype(jnp.float32)
        for t in (0, 2):
            total = total + from_team[t, at, :].astype(jnp.float32)
        kept = (tok[mine, :].astype(jnp.float32) + total).astype(jnp.bfloat16)
        residual[at, :] = kept
        rows_in[mine, :] = norm_rows(kept.astype(jnp.float32), gains[1:2, :])
        return carry

    lax.fori_loop(0, half // step_rows, residual_body, 0)
    for h in (0, 1):
        for k in (1, 2):
            share(1, k, h, rows_in, rows_in, q_own * rows + c * half).start()
    hand_on(1, 0, rows_in).start()
    all_sent(from_partner, pair_send.at[0])
    all_sent(from_team, sum_send.at[0])
    for k in (1, 2):
        share_landed(1, k, 0, rows_in)
        across(1, k, rows_in).start()
    start_side(5)
    relay(4, 1)
    for k in (1, 2):
        share_landed(1, k, 1, rows_in)
        hand_on(1, k, rows_in).start()
    relay(4, *beyond)
    start_line(5)

    position = lax.broadcasted_iota(jnp.int32, (LEN, hidden_cols), 0)

    def conv(values, which):
        back1 = jnp.where(position >= 1, pltpu.roll(values, 1, 0), 0.0)
        back2 = jnp.where(position >= 2, pltpu.roll(values, 2, 0), 0.0)
        weights = taps[which]
        return weights[0:1] * back2 + weights[1:2] * back1 + weights[2:3] * values

    def raise_chip(weight, which, q):
        at = pl.ds(pl.multiple_of(q * rows, rows), rows)
        product = jnp.dot(rows_in[at, :], weight[...], preferred_element_type=jnp.float32)
        for s in range(rows // LEN):
            here = pl.ds(pl.multiple_of(q * rows + s * LEN, LEN), LEN)
            done = conv(product[s * LEN : (s + 1) * LEN], which)
            if which:
                hidden[here, :] = (gate_half[here, :] * done).astype(jnp.bfloat16)
            else:
                gate_half[here, :] = jax.nn.silu(done)

    def raise_gate(k, carry):
        hand_landed(1, k, rows_in)
        raise_chip(w_ug, 0, chip_q(k, -1))
        return carry

    def raise_value(q, carry):
        raise_chip(w_uv, 1, q)
        return carry

    arrived_all(3)
    lax.fori_loop(0, FAR, raise_gate, 0)
    for k in (1, 2):
        across_landed(1, k, rows_in)
    hand_on(1, FAR, rows_in).start()
    relay(5, 0)
    lax.fori_loop(FAR, n_chip, raise_gate, 0)
    arrived_all(4)
    lax.fori_loop(0, n_chip, raise_value, 0)

    def finish(u):
        collected(u)
        place = unit_cols(u)
        mine = chip_rows(q_own, c)
        here = pl.ds(pl.multiple_of(c * half, half), half)
        total = part[mine, place].astype(jnp.float32)
        for t in (0, 2):
            total = total + from_team[t, :, place].astype(jnp.float32)
        out[here, place] = (residual[:, place].astype(jnp.float32) + total).astype(jnp.bfloat16)
        done = out.at[here, place]
        remote(done, done, last_sem.at[0], last_sem.at[1], partner).start()

    passed = 0
    for u in range(units):
        if u == n_side:
            relay(5, 1)
        elif u % n_side == 0 and u // n_side - 1 in beyond:
            relay(5, u // n_side - 1)
        early = u > units // 2
        for v in range(passed, u if early else u - 1):
            pass_on(v)
            passed = v + 1
        if early:
            finish(u - units // 2 - 1)
        arrived(5, line_f(u))
        multiply(u, hidden, w_down)
        reduce_pair(u)
    for u in range(units - units // 2 - 1, units - 1):
        finish(u)
    pass_on(units - 1)
    finish(units - 1)

    for a in range(ARRAYS):
        all_sent(block(a, 0), side_send.at[a])
        for n in range(1, n_line):
            pl.when(z == n - 1)(lambda: all_sent(blocks_of(a, 0, n * n_side), up_send.at[a]))
            pl.when(z == n)(
                lambda: all_sent(
                    blocks_of(a, n * n_side, (n_line - n) * n_side), down_send.at[a]
                )
            )
    all_sent(told, stat_sem.at[0])
    for g in range(2):
        all_sent(tok.at[pl.ds(0, rows)], team_send.at[g])
        all_sent(tok.at[pl.ds(0, half)], cross_send.at[g])
        all_sent(tok.at[pl.ds(0, (n_chip - 1 + g) * half)], pass_send.at[g])
    all_sent(from_partner, pair_send.at[0])
    all_sent(from_team, sum_send.at[0])
    theirs = out.at[pl.ds(pl.multiple_of(other * half, half), half)]
    last = remote(theirs, theirs, last_sem.at[0], last_sem.at[1], partner)
    last.wait_send()
    last.wait_recv()


def team_layer(
    dims,
    tokens,
    first_gain,
    mixer_gate,
    mixer_value,
    value_gain,
    value_shift,
    spatial_weight,
    spatial_bias,
    mixer_out,
    second_gain,
    up_gate,
    up_value,
    taps_gate,
    taps_value,
    down_proj,
):
    n_rep, n_fs, n_tp = dims
    n_chip, n_line = n_rep * PLANE, n_fs // PLANE
    rows, width = tokens.shape
    half, team_rows = rows // n_tp, rows * n_chip
    cols, hidden_cols = mixer_gate.shape[1] // n_chip, up_gate.shape[1] // n_chip
    vmem, anywhere = pl.BlockSpec(memory_space=pltpu.VMEM), pl.BlockSpec(memory_space=pl.ANY)
    bf16, f32, dma = jnp.bfloat16, jnp.float32, pltpu.SemaphoreType.DMA
    in_specs = [anywhere] * 15
    units = n_fs
    scratch = [
        pltpu.VMEM((width, cols), bf16),
        pltpu.VMEM((width, cols), bf16),
        pltpu.VMEM((n_fs, mixer_out.shape[0] // n_chip, mixer_out.shape[1]), bf16),
        pltpu.VMEM((width, hidden_cols), bf16),
        pltpu.VMEM((width, hidden_cols), bf16),
        pltpu.VMEM((n_fs, down_proj.shape[0] // n_chip, down_proj.shape[1]), bf16),
        pltpu.VMEM((team_rows, width), bf16),
        pltpu.VMEM((team_rows, width), bf16),
        pltpu.VMEM((team_rows, cols), f32),
        pltpu.VMEM((team_rows, cols), f32),
        pltpu.VMEM((team_rows, cols), bf16),
        pltpu.VMEM((team_rows, hidden_cols), f32),
        pltpu.VMEM((team_rows, hidden_cols), bf16),
        pltpu.VMEM((team_rows, width), bf16),
        pltpu.VMEM((n_chip * half, width), bf16),
        pltpu.VMEM((n_chip - 1, half, width), bf16),
        pltpu.VMEM((half, width), bf16),
        pltpu.VMEM((n_chip * n_tp, 2, team_rows), f32),
        pltpu.VMEM((cols // GDIM,) + spatial_weight.shape[1:], bf16),
        pltpu.VMEM((2, 3, hidden_cols), f32),
        pltpu.VMEM((2, width), f32),
        pltpu.VMEM((2, cols), f32),
        pltpu.VMEM(spatial_bias.shape, f32),
        dma((ARRAYS + 1,)),
        dma((ARRAYS,)),
        dma((ARRAYS,)),
        dma((ARRAYS,)),
        dma((ARRAYS, n_fs)),
        dma((2,)),
        dma((2, 4)),
        dma((2,)),
        dma((2, n_chip)),
        dma((2,)),
        dma((1,)),
        dma((units, 2)),
        dma((1,)),
        dma((units, 2)),
        dma((2,)),
        dma((2, 2)),
        dma((2,)),
        dma((8,)),
    ]
    return pl.pallas_call(
        functools.partial(team_kernel, dims),
        out_shape=pltpu.VMEM((rows, width), bf16),
        in_specs=in_specs,
        out_specs=vmem,
        scratch_shapes=scratch,
        compiler_params=pltpu.CompilerParams(
            collective_id=0, has_side_effects=True, vmem_limit_bytes=56 * 1024 * 1024
        ),
    )(
        tokens,
        first_gain.reshape(1, -1),
        mixer_gate,
        mixer_value,
        value_gain.reshape(1, -1),
        value_shift.reshape(1, -1),
        spatial_weight,
        spatial_bias,
        mixer_out,
        second_gain.reshape(1, -1),
        up_gate,
        up_value,
        taps_gate,
        taps_value,
        down_proj,
    )


def team_fits(mesh):
    n_rep, n_fs, n_tp = (mesh.shape[name] for name in ("rep", "fs", "tp"))
    if n_tp != 2 or n_rep * PLANE != FAR + 1 or n_fs % PLANE:
        return False
    return D % (n_fs * GDIM) == 0 and D % (n_tp * n_rep * PLANE * GDIM) == 0


def solution(mesh):
    in_specs = (
        P(("rep", "fs"), None),
        P(),
        P("fs", "tp"),
        P("fs", "tp"),
        P(),
        P(),
        P(),
        P(),
        P("tp", "fs"),
        P(),
        P("fs", "tp"),
        P("fs", "tp"),
        P(),
        P(),
        P("tp", "fs"),
    )
    out_specs = P(("rep", "fs"), None)
    body = local
    if team_fits(mesh):
        dims = tuple(mesh.shape[name] for name in ("rep", "fs", "tp"))
        body = functools.partial(team_layer, dims)
    return jax.shard_map(body, mesh=mesh, in_specs=in_specs, out_specs=out_specs, check_vma=False)
```

```python
import functools

import jax
import jax.numpy as jnp
from jax import lax
from jax.experimental import pallas as pl
from jax.experimental.pallas import tpu as pltpu
from jax.sharding import PartitionSpec as P

D = 2048
GDIM = 128
BLK = 128
LEN = 128


def normalize(matrix, scale_gain):
    values = matrix.astype(jnp.float32)
    factor = lax.rsqrt(jnp.mean(values * values, axis=-1, keepdims=True) + 1e-06)
    return (values * factor * scale_gain).astype(jnp.bfloat16)


def causal_conv(values, tap_weights):
    by_sequence = values.reshape(-1, LEN, values.shape[-1])
    padded = jnp.pad(by_sequence, ((0, 0), (2, 0), (0, 0)))
    summed = (
        tap_weights[0] * padded[:, 0:LEN]
        + tap_weights[1] * padded[:, 1 : LEN + 1]
        + tap_weights[2] * padded[:, 2 : LEN + 2]
    )
    return summed.reshape(values.shape)


def local(
    tokens,
    first_gain,
    mixer_gate,
    mixer_value,
    value_gain,
    value_shift,
    spatial_weight,
    spatial_bias,
    mixer_out,
    second_gain,
    up_gate,
    up_value,
    taps_gate,
    taps_value,
    down_proj,
):
    n_rep, n_tp = lax.axis_size("rep"), lax.axis_size("tp")
    rep_index, tp_index = lax.axis_index("rep"), lax.axis_index("tp")
    team = ("rep", "tp")

    def part(array, axis):
        width = array.shape[axis] // n_rep
        return lax.dynamic_slice_in_dim(array, rep_index * width, width, axis)

    def own(array, width, axis):
        at = (tp_index * n_rep + rep_index) * width
        return lax.dynamic_slice_in_dim(array, at, width, axis)

    w_gate = lax.all_gather(part(mixer_gate, 1), "fs", axis=0, tiled=True)
    w_value = lax.all_gather(part(mixer_value, 1), "fs", axis=0, tiled=True)
    w_out = lax.all_gather(part(mixer_out, 0), "fs", axis=1, tiled=True)
    u_gate = lax.all_gather(part(up_gate, 1), "fs", axis=0, tiled=True)
    u_value = lax.all_gather(part(up_value, 1), "fs", axis=0, tiled=True)
    w_down = lax.all_gather(part(down_proj, 0), "fs", axis=1, tiled=True)

    row_share = tokens.shape[0] // n_tp
    kept_tokens = lax.dynamic_slice_in_dim(tokens, tp_index * row_share, row_share, 0)
    first = lax.all_gather(normalize(kept_tokens, first_gain), team, axis=0, tiled=True)
    row_count = first.shape[0]
    cols = w_gate.shape[1]
    gate_act = jax.nn.gelu(jnp.dot(first, w_gate, preferred_element_type=jnp.float32))
    value_act = jax.nn.gelu(jnp.dot(first, w_value, preferred_element_type=jnp.float32))
    value_sum, value_squares = lax.psum(
        (jnp.sum(value_act, axis=1), jnp.sum(value_act * value_act, axis=1)), team
    )
    row_mean = value_sum / D
    variance = value_squares / D - row_mean * row_mean
    centred = (
        (value_act - row_mean[:, None])
        * lax.rsqrt(variance[:, None] + 1e-05)
        * own(value_gain, cols, 0)
        + own(value_shift, cols, 0)
    ).astype(jnp.bfloat16)
    groups = cols // GDIM
    masked = own(spatial_weight, groups, 0) * jnp.tril(jnp.ones((BLK, BLK), jnp.bfloat16))
    blocks = centred.reshape(row_count // BLK, BLK, groups, GDIM)
    mixed_rows = (
        jnp.einsum("gts,bsgc->btgc", masked, blocks, preferred_element_type=jnp.float32)
        + own(spatial_bias, groups, 0).T[None, :, :, None]
    )
    gated_rows = (gate_act * mixed_rows.reshape(row_count, cols)).astype(jnp.bfloat16)
    summed = lax.psum_scatter(
        jnp.dot(gated_rows, w_out, preferred_element_type=jnp.float32).astype(jnp.bfloat16),
        team,
        scatter_dimension=0,
        tiled=True,
    ).astype(jnp.float32)
    residual = (kept_tokens.astype(jnp.float32) + summed).astype(jnp.bfloat16)
    second = lax.all_gather(normalize(residual, second_gain), team, axis=0, tiled=True)
    hidden_cols = u_gate.shape[1]
    gate_up = jnp.dot(second, u_gate, preferred_element_type=jnp.float32)
    value_up = jnp.dot(second, u_value, preferred_element_type=jnp.float32)
    hidden = (
        jax.nn.silu(causal_conv(gate_up, own(taps_gate, hidden_cols, 1)))
        * causal_conv(value_up, own(taps_value, hidden_cols, 1))
    ).astype(jnp.bfloat16)
    ffn_total = lax.psum_scatter(
        jnp.dot(hidden, w_down, preferred_element_type=jnp.float32).astype(jnp.bfloat16),
        team,
        scatter_dimension=0,
        tiled=True,
    ).astype(jnp.float32)
    final_rows = (residual.astype(jnp.float32) + ffn_total).astype(jnp.bfloat16)
    return lax.all_gather(final_rows, "tp", axis=0, tiled=True)


PLANE = 2
ARRAYS = 6
FAR = 3
MESH = pl.DeviceIdType.MESH


def team_kernel(
    dims,
    tokens,
    first_gain,
    mixer_gate,
    mixer_value,
    value_gain,
    value_shift,
    spatial_weight,
    spatial_bias,
    mixer_out,
    second_gain,
    up_gate,
    up_value,
    taps_gate,
    taps_value,
    down_proj,
    out,
    w_gate,
    w_value,
    w_out,
    w_ug,
    w_uv,
    w_down,
    tok,
    rows_in,
    gate_act,
    value_act,
    gated,
    gate_half,
    hidden,
    part,
    from_partner,
    from_team,
    residual,
    stats,
    mixing,
    taps,
    gains,
    scales,
    biases,
    ahead,
    own_sem,
    side_send,
    up_send,
    down_send,
    weight_recv,
    team_send,
    team_recv,
    pass_send,
    pass_recv,
    stat_sem,
    pair_send,
    pair_recv,
    sum_send,
    sum_recv,
    cross_send,
    cross_recv,
    last_sem,
    local_sem,
):
    n_rep, n_fs, n_tp = dims
    n_side, n_line = PLANE, n_fs // PLANE
    n_chip = n_rep * n_side
    x, c = lax.axis_index("rep"), lax.axis_index("tp")
    f_own = lax.axis_index("fs")
    z, y = f_own // n_side, f_own % n_side
    other = (c + 1) % n_tp
    q_own = x * n_side + y
    rows = tokens.shape[0]
    half = rows // n_tp
    width = tokens.shape[1]
    sources = (mixer_value, mixer_gate, mixer_out, up_gate, up_value, down_proj)
    held = (w_value, w_gate, w_out, w_ug, w_uv, w_down)
    partner = (x, f_own, other)
    has_up, has_down = z + 1 < n_line, z >= 1
    at_end = (z == 0) | (z == n_line - 1)
    low = z < n_line // 2

    def chip_to(k, core):
        dx, dy = k // n_side, k % n_side
        return ((x + dx) % n_rep, z * n_side + (y + dy) % n_side, core)

    def chip_q(k, sign):
        dx, dy = k // n_side, k % n_side
        return ((x + sign * dx + n_rep) % n_rep) * n_side + (y + sign * dy + n_side) % n_side

    def remote(src, dst, send, recv, device):
        return pltpu.make_async_remote_copy(
            src_ref=src, dst_ref=dst, send_sem=send, recv_sem=recv, device_id=device, device_id_type=MESH
        )

    def all_sent(ref, sem):
        remote(ref, ref, sem, sem, partner).wait_send()

    def blocks_of(a, f, count):
        if len(held[a].shape) == 3:
            return held[a].at[pl.ds(f, count)]
        height = sources[a].shape[0]
        return held[a].at[pl.ds(pl.multiple_of(f * height, height), count * height)]

    def block(a, f):
        return held[a].at[f] if len(held[a].shape) == 3 else blocks_of(a, f, 1)

    def piece(a, q):
        if len(held[a].shape) == 3:
            height = sources[a].shape[0] // n_chip
            return sources[a].at[pl.ds(pl.multiple_of(q * height, height), height)]
        cols = sources[a].shape[1] // n_chip
        return sources[a].at[:, pl.ds(pl.multiple_of(q * cols, cols), cols)]

    def own_copy(a):
        return pltpu.make_async_copy(piece(a, q_own), block(a, f_own), own_sem.at[a])

    q_side = x * n_side + (y + 1) % n_side

    def staged(a):
        return pltpu.make_async_copy(piece(a, q_side), ahead.at[a], local_sem.at[8 + a])

    def side(a):
        to_y = (y + 1) % n_side
        return remote(
            piece(a, q_side) if a > 1 else ahead.at[a],
            block(a, f_own),
            side_send.at[a],
            weight_recv.at[a, f_own],
            (x, z * n_side + to_y, c),
        )

    def along(a, f, step, src):
        sem = up_send if step == 1 else down_send
        return remote(
            src, block(a, f), sem.at[a], weight_recv.at[a, f], (x, f_own + step * n_side, c)
        )

    def landed(a, f):
        remote(block(a, f), block(a, f), side_send.at[a], weight_recv.at[a, f], partner).wait_recv()

    def send_line(a, f, src, up=True, down=True):
        if up:
            pl.when(has_up)(lambda: along(a, f, 1, src).start())
        if down:
            pl.when(has_down)(lambda: along(a, f, -1, src).start())

    def start_side(a):
        own_copy(a).start()
        side(a).start()

    def start_line(a):
        send_line(a, f_own, piece(a, q_own))

    def relay(a, *distances):
        for d in distances:
            if d == 0:
                f = z * n_side + (y + 1) % n_side
                landed(a, f)
                send_line(a, f, block(a, f))
                if a > 1:
                    own_copy(a).wait()
                continue
            for j in range(n_side):
                turn = j if a in (2, 5) else (y + j) % n_side
                for first in (True, False):
                    above = low if first else jnp.logical_not(low)

                    @pl.when((z + d < n_line) & has_down & above)
                    def _():
                        f = (z + d) * n_side + turn
                        landed(a, f)
                        send_line(a, f, block(a, f), up=False)

                    if first:

                        @pl.when((z - d >= 0) & has_up)
                        def _():
                            f = (z - d) * n_side + turn
                            landed(a, f)
                            send_line(a, f, block(a, f), down=False)

    beyond = tuple(range(2, n_line - 1))

    def arrived(a, f):
        pl.when(at_end & (f // n_side != z))(lambda: landed(a, f))

    def arrived_all(a):
        def body(f, carry):
            arrived(a, f)
            return carry

        lax.fori_loop(0, n_fs, body, 0)

    def chip_rows(q, core):
        return pl.ds(pl.multiple_of(q * rows + core * half, half), half)

    cuts = (half * 2 // 3 // 16 * 16, half // 2 // 16 * 16)

    def strip(g, k, forwarded):
        low = (k == 1) == forwarded
        return (0, cuts[g]) if low else (cuts[g], half - cuts[g])

    def strip_rows(buffer, g, k, forwarded, q):
        first, size = strip(g, k, forwarded)
        at = pl.multiple_of(q * rows + c * half + first, 16)
        return buffer.at[pl.ds(at, size)]

    def share(g, k, h, buffer, source, base):
        first, size = strip(g, k, h == 0)
        return remote(
            source.at[pl.ds(pl.multiple_of(base + first, 16), size)],
            strip_rows(buffer, g, k, h == 0, q_own),
            team_send.at[g],
            team_recv.at[g, 2 * (k - 1) + h],
            chip_to(k, c),
        )

    def share_landed(g, k, h, buffer):
        place = strip_rows(buffer, g, k, h == 0, chip_q(k, -1))
        sem = team_recv.at[g, 2 * (k - 1) + h]
        remote(place, place, team_send.at[g], sem, partner).wait_recv()

    def across(g, k, buffer):
        place = strip_rows(buffer, g, k, True, chip_q(k, -1))
        return remote(
            place, place, cross_send.at[g], cross_recv.at[g, k - 1], chip_to(FAR - k, c)
        )

    def across_landed(g, k, buffer):
        place = strip_rows(buffer, g, k, True, chip_q(FAR, -1))
        remote(place, place, cross_send.at[g], cross_recv.at[g, k - 1], partner).wait_recv()

    def hand_on(g, k, buffer):
        place = buffer.at[chip_rows(chip_q(k, -1), c)]
        return remote(place, place, pass_send.at[g], pass_recv.at[g, k], partner)

    def hand_landed(g, k, buffer):
        place = buffer.at[chip_rows(chip_q(k, -1), other)]
        remote(place, place, pass_send.at[g], pass_recv.at[g, k], partner).wait_recv()

    def norm_rows(values, gain):
        factor = lax.rsqrt(jnp.mean(values * values, axis=-1, keepdims=True) + 1e-06)
        return (values * factor * gain).astype(jnp.bfloat16)

    step_rows = 64

    def norm_chip(q):
        def body(i, carry):
            at = pl.ds(pl.multiple_of(q * rows + i * step_rows, step_rows), step_rows)
            rows_in[at, :] = norm_rows(tok[at, :].astype(jnp.float32), gains[0:1, :])
            return carry

        lax.fori_loop(0, rows // step_rows, body, 0)

    cols, hidden_cols = w_gate.shape[1], w_ug.shape[1]
    groups = cols // GDIM
    slot = c * n_chip + q_own
    at_hidden = pl.ds(pl.multiple_of(slot * hidden_cols, hidden_cols), hidden_cols)
    at_cols = pl.ds(pl.multiple_of(slot * cols, cols), cols)
    first_gain_in = pltpu.make_async_copy(first_gain, gains.at[0:1], local_sem.at[3])
    locals_in = (
        pltpu.make_async_copy(second_gain, gains.at[1:2], local_sem.at[4]),
        pltpu.make_async_copy(value_gain.at[:, at_cols], scales.at[0:1], local_sem.at[5]),
        pltpu.make_async_copy(value_shift.at[:, at_cols], scales.at[1:2], local_sem.at[6]),
        pltpu.make_async_copy(spatial_bias, biases, local_sem.at[7]),
        pltpu.make_async_copy(
            spatial_weight.at[pl.ds(slot * groups, groups)], mixing, local_sem.at[0]
        ),
        pltpu.make_async_copy(taps_gate.at[:, at_hidden], taps.at[0], local_sem.at[1]),
        pltpu.make_async_copy(taps_value.at[:, at_hidden], taps.at[1], local_sem.at[2]),
    )

    for a in (0, 1):
        own_copy(a).start()
        staged(a).start()

    barrier = pltpu.get_barrier_semaphore()
    for mate in (chip_to(1, c), chip_to(2, c), partner):
        pl.semaphore_signal(barrier, inc=1, device_id=mate, device_id_type=MESH)
    for flag, step in ((has_up, 1), (has_down, -1)):

        @pl.when(flag)
        def _():
            pl.semaphore_signal(
                barrier, inc=1, device_id=(x, f_own + step * n_side, c), device_id_type=MESH
            )

    neighbours = has_up.astype(jnp.int32) + has_down.astype(jnp.int32)
    pl.semaphore_wait(barrier, FAR + neighbours)

    for a in (0, 1):
        own_copy(a).wait()
        send_line(a, f_own, block(a, f_own))
        staged(a).wait()
        side(a).start()
    for h in (0, 1):
        for k in (2, 1):
            share(0, k, h, tok, tokens, c * half).start()
    tok_copy = pltpu.make_async_copy(
        tokens, tok.at[pl.ds(pl.multiple_of(q_own * rows, rows), rows)], own_sem.at[ARRAYS]
    )
    tok_copy.start()
    start_side(2)
    first_gain_in.start()
    for copy in locals_in:
        copy.start()
    relay(0, 0)
    relay(1, 0)
    relay(0, 1)
    tok_copy.wait()
    first_gain_in.wait()
    norm_chip(q_own)
    share_landed(0, 2, 0, tok)
    across(0, 2, tok).start()
    relay(1, 1)
    share_landed(0, 1, 0, tok)
    across(0, 1, tok).start()
    start_side(3)
    relay(0, *beyond)
    share_landed(0, 2, 1, tok)
    hand_on(0, 2, tok).start()
    hand_landed(0, 2, tok)
    norm_chip(chip_q(2, -1))
    relay(1, *beyond)
    start_line(2)
    share_landed(0, 1, 1, tok)
    hand_on(0, 1, tok).start()
    relay(2, 0)
    hand_landed(0, 1, tok)
    norm_chip(chip_q(1, -1))
    relay(2, 1)
    for k in (1, 2):
        across_landed(0, k, tok)
    hand_on(0, FAR, tok).start()
    hand_landed(0, FAR, tok)
    norm_chip(chip_q(FAR, -1))

    def project(weight, target):
        def body(i, carry):
            at = pl.ds(pl.multiple_of(i * half, half), half)
            product = jnp.dot(rows_in[at, :], weight[...], preferred_element_type=jnp.float32)
            target[at, :] = jax.nn.gelu(product)
            return carry

        lax.fori_loop(0, n_chip * n_tp, body, 0)

    blocks = n_chip * rows // BLK
    lane = lax.broadcasted_iota(jnp.int32, (BLK, BLK), 1)
    sub = lax.broadcasted_iota(jnp.int32, (BLK, BLK), 0)
    arrived_all(0)
    project(w_value, value_act)

    def stat_body(i, carry):
        at = pl.ds(pl.multiple_of(i * BLK, BLK), BLK)
        values = value_act[at, :]
        total = jnp.sum(values, axis=1, keepdims=True)
        squares = jnp.sum(values * values, axis=1, keepdims=True)
        both = jnp.where(lane == 0, total, squares).T
        stats[0, :, at] = both[0:2, :]
        return carry

    lax.fori_loop(0, blocks, stat_body, 0)
    mates = [(k, j) for k in range(n_chip) for j in range(n_tp) if k or j]

    def tell(i):
        k, j = mates[i]
        device = chip_to(k, (c + j) % n_tp)
        return remote(stats.at[0], stats.at[i + 1], stat_sem.at[0], stat_sem.at[1], device)

    for i in range(len(mates)):
        tell(i).start()
    start_side(4)
    relay(2, *beyond)
    start_line(3)
    arrived_all(1)
    project(w_gate, gate_act)
    relay(3, 0)
    told = stats.at[pl.ds(1, len(mates))]
    remote(told, told, stat_sem.at[0], stat_sem.at[1], partner).wait_recv()
    for copy in locals_in:
        copy.wait()

    def mix_body(i, carry):
        at = pl.ds(pl.multiple_of(i * BLK, BLK), BLK)
        total = stats[0, :, at]
        for s in range(1, len(mates) + 1):
            total = total + stats[s, :, at]
        row_mean = jnp.broadcast_to(total[0:1, :] / width, (BLK, BLK)).T[:, 0:1]
        row_square = jnp.broadcast_to(total[1:2, :] / width, (BLK, BLK)).T[:, 0:1]
        variance = row_square - row_mean * row_mean
        centred = (
            (value_act[at, :] - row_mean) * lax.rsqrt(variance + 1e-05) * scales[0:1, :]
            + scales[1:2, :]
        ).astype(jnp.bfloat16)
        for g in range(groups):
            group = slot * groups + g
            matrix = mixing[g]
            matrix = jnp.where(sub >= lane, matrix, jnp.zeros_like(matrix))
            bias = jnp.broadcast_to(biases[pl.ds(group, 1), :], (BLK, BLK)).T
            mixed = (
                jnp.dot(
                    matrix, centred[:, g * GDIM : (g + 1) * GDIM], preferred_element_type=jnp.float32
                )
                + bias
            )
            channels = slice(g * GDIM, (g + 1) * GDIM)
            gated[at, channels] = (gate_act[at, channels] * mixed).astype(jnp.bfloat16)
        return carry

    lax.fori_loop(0, blocks, mix_body, 0)

    cut = w_out.shape[2]
    units = n_line * n_side

    near_z = jnp.where(low, z, n_line - 1 - z)

    def line_f(u):
        i = u // n_side
        turn = near_z - (i + 1) // 2 if i % 2 else near_z + i // 2
        p = jnp.where(i > 2 * near_z, i, turn)
        return jnp.where(low, p, n_line - 1 - p) * n_side + u % n_side

    def unit_cols(u):
        return pl.ds(pl.multiple_of(line_f(u) * cut, cut), cut)

    def pair(u, i):
        q, place = chip_q(FAR - i, 1), unit_cols(u)
        return remote(
            part.at[chip_rows(q, other), place],
            from_partner.at[pl.ds(pl.multiple_of(q * half, half), half), place],
            pair_send.at[0],
            pair_recv.at[u, jnp.minimum(i, 1)],
            partner,
        )

    def lane_cols(u, near):
        return pl.ds(pl.multiple_of(line_f(u) * cut + (2 - near) * (cut // 2), cut // 2), cut // 2)

    def to_team(u, near, t):
        place = lane_cols(u, near)
        k_rows = (near, FAR, FAR - near)[t]
        k_chip = (near, near, FAR - near)[t]
        return remote(
            part.at[chip_rows(chip_q(k_rows, 1), c), place],
            from_team.at[t, :, place],
            sum_send.at[0],
            sum_recv.at[u, t % 2],
            chip_to(k_chip, c),
        )

    def multiply(u, acts, weight):
        band = n_side * rows

        def body(i, carry):
            at_x = (x + 1 + i) % n_rep
            at = pl.ds(pl.multiple_of(at_x * band, band), band)
            part[at, unit_cols(u)] = jnp.dot(
                acts[at, :], weight[line_f(u)], preferred_element_type=jnp.float32
            ).astype(jnp.bfloat16)
            for j in range(n_side):
                pair(u, i * n_side + j).start()
            return carry

        lax.fori_loop(0, n_rep, body, 0)

    def pair_landed(u, i):
        whole = from_partner.at[pl.ds(0, (1 + i * (n_chip - 2)) * half), unit_cols(u)]
        remote(whole, whole, pair_send.at[0], pair_recv.at[u, i], partner).wait_recv()

    def reduce_pair(u, chips=tuple(range(FAR, -1, -1))):
        place = unit_cols(u)
        for k in chips:
            if k >= FAR - 1:
                pair_landed(u, FAR - k)
            q = chip_q(k, 1)
            at = chip_rows(q, c)
            part[at, place] = (
                part[at, place].astype(jnp.float32)
                + from_partner[pl.ds(pl.multiple_of(q * half, half), half), place].astype(
                    jnp.float32
                )
            ).astype(jnp.bfloat16)
            if k == FAR:
                for near in (2, 1):
                    to_team(u, near, 1).start()
            elif k:
                to_team(u, k, 0).start()

    def pass_on(u):
        both = from_team.at[1, :, unit_cols(u)]
        remote(both, both, sum_send.at[0], sum_recv.at[u, 1], partner).wait_recv()
        for near in (2, 1):
            at, place = chip_rows(chip_q(FAR - near, 1), c), lane_cols(u, near)
            part[at, place] = (
                part[at, place].astype(jnp.float32) + from_team[1, :, place].astype(jnp.float32)
            ).astype(jnp.bfloat16)
            to_team(u, near, 2).start()

    def collected(u):
        rest = from_team.at[pl.ds(0, 2), :, unit_cols(u)]
        remote(rest, rest, sum_send.at[0], sum_recv.at[u, 0], partner).wait_recv()

    lag = 2

    def out_units(acts, weight, a):
        for u in range(units):
            if u == units // 2:
                relay(3, 1)
                start_line(4)
            arrived(a, line_f(u))
            multiply(u, acts, weight)
            if u:
                reduce_pair(u - 1)
            if u >= 2 * lag:
                pass_on(u - 2 * lag)
        reduce_pair(units - 1)

    out_units(gated, w_out, 2)
    for u in range(units - 2 * lag, units):
        pass_on(u)
    relay(3, *beyond)
    relay(4, 0)
    for u in range(units):
        collected(u)

    def residual_body(i, carry):
        at = pl.ds(pl.multiple_of(i * step_rows, step_rows), step_rows)
        mine = pl.ds(pl.multiple_of(q_own * rows + c * half + i * step_rows, step_rows), step_rows)
        total = part[mine, :].astype(jnp.float32)
        for t in (0, 2):
            total = total + from_team[t, at, :].astype(jnp.float32)
        kept = (tok[mine, :].astype(jnp.float32) + total).astype(jnp.bfloat16)
        residual[at, :] = kept
        rows_in[mine, :] = norm_rows(kept.astype(jnp.float32), gains[1:2, :])
        return carry

    lax.fori_loop(0, half // step_rows, residual_body, 0)
    for h in (0, 1):
        for k in (1, 2):
            share(1, k, h, rows_in, rows_in, q_own * rows + c * half).start()
    hand_on(1, 0, rows_in).start()
    all_sent(from_partner, pair_send.at[0])
    all_sent(from_team, sum_send.at[0])
    for k in (1, 2):
        share_landed(1, k, 0, rows_in)
        across(1, k, rows_in).start()
    start_side(5)
    relay(4, 1)
    for k in (1, 2):
        share_landed(1, k, 1, rows_in)
        hand_on(1, k, rows_in).start()
    relay(4, *beyond)
    start_line(5)

    position = lax.broadcasted_iota(jnp.int32, (LEN, hidden_cols), 0)

    def conv(values, which):
        back1 = jnp.where(position >= 1, pltpu.roll(values, 1, 0), 0.0)
        back2 = jnp.where(position >= 2, pltpu.roll(values, 2, 0), 0.0)
        weights = taps[which]
        return weights[0:1] * back2 + weights[1:2] * back1 + weights[2:3] * values

    def raise_chip(weight, which, q):
        at = pl.ds(pl.multiple_of(q * rows, rows), rows)
        product = jnp.dot(rows_in[at, :], weight[...], preferred_element_type=jnp.float32)
        for s in range(rows // LEN):
            here = pl.ds(pl.multiple_of(q * rows + s * LEN, LEN), LEN)
            done = conv(product[s * LEN : (s + 1) * LEN], which)
            if which:
                hidden[here, :] = (gate_half[here, :] * done).astype(jnp.bfloat16)
            else:
                gate_half[here, :] = jax.nn.silu(done)

    def raise_gate(k, carry):
        hand_landed(1, k, rows_in)
        raise_chip(w_ug, 0, chip_q(k, -1))
        return carry

    def raise_value(q, carry):
        raise_chip(w_uv, 1, q)
        return carry

    arrived_all(3)
    lax.fori_loop(0, FAR, raise_gate, 0)
    for k in (1, 2):
        across_landed(1, k, rows_in)
    hand_on(1, FAR, rows_in).start()
    relay(5, 0)
    lax.fori_loop(FAR, n_chip, raise_gate, 0)
    arrived_all(4)
    lax.fori_loop(0, n_chip, raise_value, 0)

    def finish(u):
        collected(u)
        place = unit_cols(u)
        mine = chip_rows(q_own, c)
        here = pl.ds(pl.multiple_of(c * half, half), half)
        total = part[mine, place].astype(jnp.float32)
        for t in (0, 2):
            total = total + from_team[t, :, place].astype(jnp.float32)
        out[here, place] = (residual[:, place].astype(jnp.float32) + total).astype(jnp.bfloat16)
        done = out.at[here, place]
        remote(done, done, last_sem.at[0], last_sem.at[1], partner).start()

    passed = 0
    for u in range(units):
        if u == n_side:
            relay(5, 1)
        elif u % n_side == 0 and u // n_side - 1 in beyond:
            relay(5, u // n_side - 1)
        arrived(5, line_f(u))
        multiply(u, hidden, w_down)
        reduce_pair(u, (FAR,))
        for v in range(passed, u if u > units // 2 else u - 1):
            pass_on(v)
            passed = v + 1
        reduce_pair(u, tuple(range(FAR - 1, -1, -1)))
        if u > units // 2:
            finish(u - units // 2 - 1)
    for u in range(units - units // 2 - 1, units - 2):
        finish(u)
    pass_on(units - 1)
    finish(units - 2)
    finish(units - 1)

    for a in range(ARRAYS):
        all_sent(block(a, 0), side_send.at[a])
        for n in range(1, n_line):
            pl.when(z == n - 1)(lambda: all_sent(blocks_of(a, 0, n * n_side), up_send.at[a]))
            pl.when(z == n)(
                lambda: all_sent(
                    blocks_of(a, n * n_side, (n_line - n) * n_side), down_send.at[a]
                )
            )
    all_sent(told, stat_sem.at[0])
    for g in range(2):
        all_sent(tok.at[pl.ds(0, rows)], team_send.at[g])
        all_sent(tok.at[pl.ds(0, half)], cross_send.at[g])
        all_sent(tok.at[pl.ds(0, (n_chip - 1 + g) * half)], pass_send.at[g])
    all_sent(from_partner, pair_send.at[0])
    all_sent(from_team, sum_send.at[0])
    theirs = out.at[pl.ds(pl.multiple_of(other * half, half), half)]
    last = remote(theirs, theirs, last_sem.at[0], last_sem.at[1], partner)
    last.wait_send()
    last.wait_recv()


def team_layer(
    dims,
    tokens,
    first_gain,
    mixer_gate,
    mixer_value,
    value_gain,
    value_shift,
    spatial_weight,
    spatial_bias,
    mixer_out,
    second_gain,
    up_gate,
    up_value,
    taps_gate,
    taps_value,
    down_proj,
):
    n_rep, n_fs, n_tp = dims
    n_chip, n_line = n_rep * PLANE, n_fs // PLANE
    rows, width = tokens.shape
    half, team_rows = rows // n_tp, rows * n_chip
    cols, hidden_cols = mixer_gate.shape[1] // n_chip, up_gate.shape[1] // n_chip
    vmem, anywhere = pl.BlockSpec(memory_space=pltpu.VMEM), pl.BlockSpec(memory_space=pl.ANY)
    bf16, f32, dma = jnp.bfloat16, jnp.float32, pltpu.SemaphoreType.DMA
    in_specs = [anywhere] * 15
    units = n_fs
    scratch = [
        pltpu.VMEM((width, cols), bf16),
        pltpu.VMEM((width, cols), bf16),
        pltpu.VMEM((n_fs, mixer_out.shape[0] // n_chip, mixer_out.shape[1]), bf16),
        pltpu.VMEM((width, hidden_cols), bf16),
        pltpu.VMEM((width, hidden_cols), bf16),
        pltpu.VMEM((n_fs, down_proj.shape[0] // n_chip, down_proj.shape[1]), bf16),
        pltpu.VMEM((team_rows, width), bf16),
        pltpu.VMEM((team_rows, width), bf16),
        pltpu.VMEM((team_rows, cols), f32),
        pltpu.VMEM((team_rows, cols), f32),
        pltpu.VMEM((team_rows, cols), bf16),
        pltpu.VMEM((team_rows, hidden_cols), f32),
        pltpu.VMEM((team_rows, hidden_cols), bf16),
        pltpu.VMEM((team_rows, width), bf16),
        pltpu.VMEM((n_chip * half, width), bf16),
        pltpu.VMEM((n_chip - 1, half, width), bf16),
        pltpu.VMEM((half, width), bf16),
        pltpu.VMEM((n_chip * n_tp, 2, team_rows), f32),
        pltpu.VMEM((cols // GDIM,) + spatial_weight.shape[1:], bf16),
        pltpu.VMEM((2, 3, hidden_cols), f32),
        pltpu.VMEM((2, width), f32),
        pltpu.VMEM((2, cols), f32),
        pltpu.VMEM(spatial_bias.shape, f32),
        pltpu.VMEM((2, mixer_value.shape[0], cols), bf16),
        dma((ARRAYS + 1,)),
        dma((ARRAYS,)),
        dma((ARRAYS,)),
        dma((ARRAYS,)),
        dma((ARRAYS, n_fs)),
        dma((2,)),
        dma((2, 4)),
        dma((2,)),
        dma((2, n_chip)),
        dma((2,)),
        dma((1,)),
        dma((units, 2)),
        dma((1,)),
        dma((units, 2)),
        dma((2,)),
        dma((2, 2)),
        dma((2,)),
        dma((10,)),
    ]
    return pl.pallas_call(
        functools.partial(team_kernel, dims),
        out_shape=pltpu.VMEM((rows, width), bf16),
        in_specs=in_specs,
        out_specs=vmem,
        scratch_shapes=scratch,
        compiler_params=pltpu.CompilerParams(
            collective_id=0, has_side_effects=True, vmem_limit_bytes=56 * 1024 * 1024
        ),
    )(
        tokens,
        first_gain.reshape(1, -1),
        mixer_gate,
        mixer_value,
        value_gain.reshape(1, -1),
        value_shift.reshape(1, -1),
        spatial_weight,
        spatial_bias,
        mixer_out,
        second_gain.reshape(1, -1),
        up_gate,
        up_value,
        taps_gate,
        taps_value,
        down_proj,
    )


def team_fits(mesh):
    n_rep, n_fs, n_tp = (mesh.shape[name] for name in ("rep", "fs", "tp"))
    if n_tp != 2 or n_rep * PLANE != FAR + 1 or n_fs % PLANE:
        return False
    return D % (n_fs * GDIM) == 0 and D % (n_tp * n_rep * PLANE * GDIM) == 0


def solution(mesh):
    in_specs = (
        P(("rep", "fs"), None),
        P(),
        P("fs", "tp"),
        P("fs", "tp"),
        P(),
        P(),
        P(),
        P(),
        P("tp", "fs"),
        P(),
        P("fs", "tp"),
        P("fs", "tp"),
        P(),
        P(),
        P("tp", "fs"),
    )
    out_specs = P(("rep", "fs"), None)
    body = local
    if team_fits(mesh):
        dims = tuple(mesh.shape[name] for name in ("rep", "fs", "tp"))
        body = functools.partial(team_layer, dims)
    return jax.shard_map(body, mesh=mesh, in_specs=in_specs, out_specs=out_specs, check_vma=False)
```

```python
import functools

import jax
import jax.numpy as jnp
from jax import lax
from jax.experimental import pallas as pl
from jax.experimental.pallas import tpu as pltpu
from jax.sharding import PartitionSpec as P

D = 2048
GDIM = 128
BLK = 128
LEN = 128


def normalize(matrix, scale_gain):
    values = matrix.astype(jnp.float32)
    factor = lax.rsqrt(jnp.mean(values * values, axis=-1, keepdims=True) + 1e-06)
    return (values * factor * scale_gain).astype(jnp.bfloat16)


def causal_conv(values, tap_weights):
    by_sequence = values.reshape(-1, LEN, values.shape[-1])
    padded = jnp.pad(by_sequence, ((0, 0), (2, 0), (0, 0)))
    summed = (
        tap_weights[0] * padded[:, 0:LEN]
        + tap_weights[1] * padded[:, 1 : LEN + 1]
        + tap_weights[2] * padded[:, 2 : LEN + 2]
    )
    return summed.reshape(values.shape)


def local(
    tokens,
    first_gain,
    mixer_gate,
    mixer_value,
    value_gain,
    value_shift,
    spatial_weight,
    spatial_bias,
    mixer_out,
    second_gain,
    up_gate,
    up_value,
    taps_gate,
    taps_value,
    down_proj,
):
    n_rep, n_tp = lax.axis_size("rep"), lax.axis_size("tp")
    rep_index, tp_index = lax.axis_index("rep"), lax.axis_index("tp")
    team = ("rep", "tp")

    def part(array, axis):
        width = array.shape[axis] // n_rep
        return lax.dynamic_slice_in_dim(array, rep_index * width, width, axis)

    def own(array, width, axis):
        at = (tp_index * n_rep + rep_index) * width
        return lax.dynamic_slice_in_dim(array, at, width, axis)

    w_gate = lax.all_gather(part(mixer_gate, 1), "fs", axis=0, tiled=True)
    w_value = lax.all_gather(part(mixer_value, 1), "fs", axis=0, tiled=True)
    w_out = lax.all_gather(part(mixer_out, 0), "fs", axis=1, tiled=True)
    u_gate = lax.all_gather(part(up_gate, 1), "fs", axis=0, tiled=True)
    u_value = lax.all_gather(part(up_value, 1), "fs", axis=0, tiled=True)
    w_down = lax.all_gather(part(down_proj, 0), "fs", axis=1, tiled=True)

    row_share = tokens.shape[0] // n_tp
    kept_tokens = lax.dynamic_slice_in_dim(tokens, tp_index * row_share, row_share, 0)
    first = lax.all_gather(normalize(kept_tokens, first_gain), team, axis=0, tiled=True)
    row_count = first.shape[0]
    cols = w_gate.shape[1]
    gate_act = jax.nn.gelu(jnp.dot(first, w_gate, preferred_element_type=jnp.float32))
    value_act = jax.nn.gelu(jnp.dot(first, w_value, preferred_element_type=jnp.float32))
    value_sum, value_squares = lax.psum(
        (jnp.sum(value_act, axis=1), jnp.sum(value_act * value_act, axis=1)), team
    )
    row_mean = value_sum / D
    variance = value_squares / D - row_mean * row_mean
    centred = (
        (value_act - row_mean[:, None])
        * lax.rsqrt(variance[:, None] + 1e-05)
        * own(value_gain, cols, 0)
        + own(value_shift, cols, 0)
    ).astype(jnp.bfloat16)
    groups = cols // GDIM
    masked = own(spatial_weight, groups, 0) * jnp.tril(jnp.ones((BLK, BLK), jnp.bfloat16))
    blocks = centred.reshape(row_count // BLK, BLK, groups, GDIM)
    mixed_rows = (
        jnp.einsum("gts,bsgc->btgc", masked, blocks, preferred_element_type=jnp.float32)
        + own(spatial_bias, groups, 0).T[None, :, :, None]
    )
    gated_rows = (gate_act * mixed_rows.reshape(row_count, cols)).astype(jnp.bfloat16)
    summed = lax.psum_scatter(
        jnp.dot(gated_rows, w_out, preferred_element_type=jnp.float32).astype(jnp.bfloat16),
        team,
        scatter_dimension=0,
        tiled=True,
    ).astype(jnp.float32)
    residual = (kept_tokens.astype(jnp.float32) + summed).astype(jnp.bfloat16)
    second = lax.all_gather(normalize(residual, second_gain), team, axis=0, tiled=True)
    hidden_cols = u_gate.shape[1]
    gate_up = jnp.dot(second, u_gate, preferred_element_type=jnp.float32)
    value_up = jnp.dot(second, u_value, preferred_element_type=jnp.float32)
    hidden = (
        jax.nn.silu(causal_conv(gate_up, own(taps_gate, hidden_cols, 1)))
        * causal_conv(value_up, own(taps_value, hidden_cols, 1))
    ).astype(jnp.bfloat16)
    ffn_total = lax.psum_scatter(
        jnp.dot(hidden, w_down, preferred_element_type=jnp.float32).astype(jnp.bfloat16),
        team,
        scatter_dimension=0,
        tiled=True,
    ).astype(jnp.float32)
    final_rows = (residual.astype(jnp.float32) + ffn_total).astype(jnp.bfloat16)
    return lax.all_gather(final_rows, "tp", axis=0, tiled=True)


PLANE = 2
ARRAYS = 6
FAR = 3
MESH = pl.DeviceIdType.MESH


def team_kernel(
    dims,
    tokens,
    first_gain,
    mixer_gate,
    mixer_value,
    value_gain,
    value_shift,
    spatial_weight,
    spatial_bias,
    mixer_out,
    second_gain,
    up_gate,
    up_value,
    taps_gate,
    taps_value,
    down_proj,
    out,
    w_gate,
    w_value,
    w_out,
    w_ug,
    w_uv,
    w_down,
    tok,
    rows_in,
    gate_act,
    value_act,
    gated,
    gate_half,
    hidden,
    part,
    from_partner,
    from_team,
    residual,
    stats,
    mixing,
    taps,
    gains,
    scales,
    biases,
    ahead,
    own_sem,
    side_send,
    up_send,
    down_send,
    weight_recv,
    team_send,
    team_recv,
    pass_send,
    pass_recv,
    stat_sem,
    pair_send,
    pair_recv,
    sum_send,
    sum_recv,
    cross_send,
    cross_recv,
    last_sem,
    local_sem,
    late_recv,
):
    n_rep, n_fs, n_tp = dims
    n_side, n_line = PLANE, n_fs // PLANE
    n_chip = n_rep * n_side
    x, c = lax.axis_index("rep"), lax.axis_index("tp")
    f_own = lax.axis_index("fs")
    z, y = f_own // n_side, f_own % n_side
    other = (c + 1) % n_tp
    q_own = x * n_side + y
    rows = tokens.shape[0]
    half = rows // n_tp
    width = tokens.shape[1]
    sources = (mixer_value, mixer_gate, mixer_out, up_gate, up_value, down_proj)
    held = (w_value, w_gate, w_out, w_ug, w_uv, w_down)
    partner = (x, f_own, other)
    has_up, has_down = z + 1 < n_line, z >= 1
    at_end = (z == 0) | (z == n_line - 1)
    low = z < n_line // 2

    def chip_to(k, core):
        dx, dy = k // n_side, k % n_side
        return ((x + dx) % n_rep, z * n_side + (y + dy) % n_side, core)

    def chip_q(k, sign):
        dx, dy = k // n_side, k % n_side
        return ((x + sign * dx + n_rep) % n_rep) * n_side + (y + sign * dy + n_side) % n_side

    def remote(src, dst, send, recv, device):
        return pltpu.make_async_remote_copy(
            src_ref=src, dst_ref=dst, send_sem=send, recv_sem=recv, device_id=device, device_id_type=MESH
        )

    def all_sent(ref, sem):
        remote(ref, ref, sem, sem, partner).wait_send()

    def blocks_of(a, f, count):
        if len(held[a].shape) == 3:
            return held[a].at[pl.ds(f, count)]
        height = sources[a].shape[0]
        return held[a].at[pl.ds(pl.multiple_of(f * height, height), count * height)]

    def block(a, f):
        return held[a].at[f] if len(held[a].shape) == 3 else blocks_of(a, f, 1)

    def piece(a, q):
        if len(held[a].shape) == 3:
            height = sources[a].shape[0] // n_chip
            return sources[a].at[pl.ds(pl.multiple_of(q * height, height), height)]
        cols = sources[a].shape[1] // n_chip
        return sources[a].at[:, pl.ds(pl.multiple_of(q * cols, cols), cols)]

    def own_copy(a):
        return pltpu.make_async_copy(piece(a, q_own), block(a, f_own), own_sem.at[a])

    q_side = x * n_side + (y + 1) % n_side

    def staged(a):
        return pltpu.make_async_copy(piece(a, q_side), ahead.at[a], local_sem.at[8 + a])

    def side(a):
        to_y = (y + 1) % n_side
        return remote(
            piece(a, q_side) if a > 1 else ahead.at[a],
            block(a, f_own),
            side_send.at[a],
            weight_recv.at[a, f_own],
            (x, z * n_side + to_y, c),
        )

    def along(a, f, step, src):
        sem = up_send if step == 1 else down_send
        return remote(
            src, block(a, f), sem.at[a], weight_recv.at[a, f], (x, f_own + step * n_side, c)
        )

    def halves(a, f):
        cut = sources[a].shape[1] // 2
        return [held[a].at[f, :, pl.ds(h * cut, cut)] for h in (0, 1)]

    def send_halves(a, f, step):
        for h, ref in enumerate(halves(a, f)):
            sem = up_send if step == 1 else down_send
            recv = late_recv.at[0] if h else weight_recv.at[a, f]
            remote(ref, ref, sem.at[a], recv, (x, f_own + step * n_side, c)).start()

    def half_landed(a, f, h):
        ref = halves(a, f)[h]
        recv = late_recv.at[0] if h else weight_recv.at[a, f]
        pl.when(at_end)(lambda: remote(ref, ref, side_send.at[a], recv, partner).wait_recv())

    def landed(a, f):
        remote(block(a, f), block(a, f), side_send.at[a], weight_recv.at[a, f], partner).wait_recv()

    def send_line(a, f, src, up=True, down=True):
        if up:
            pl.when(has_up)(lambda: along(a, f, 1, src).start())
        if down:
            pl.when(has_down)(lambda: along(a, f, -1, src).start())

    def start_side(a):
        own_copy(a).start()
        side(a).start()

    def start_line(a):
        send_line(a, f_own, piece(a, q_own))

    def relay(a, *distances):
        for d in distances:
            if d == 0:
                f = z * n_side + (y + 1) % n_side
                landed(a, f)
                send_line(a, f, block(a, f))
                if a > 1:
                    own_copy(a).wait()
                continue
            for j in range(n_side):
                turn = j if a in (2, 5) else (y + j) % n_side
                final = a == ARRAYS - 1 and d == n_line - 2 and j == n_side - 1
                for first in (True, False):
                    above = low if first else jnp.logical_not(low)

                    @pl.when((z + d < n_line) & has_down & above)
                    def _():
                        f = (z + d) * n_side + turn
                        landed(a, f)
                        if final:
                            send_halves(a, f, -1)
                        else:
                            send_line(a, f, block(a, f), up=False)

                    if first:

                        @pl.when((z - d >= 0) & has_up)
                        def _():
                            f = (z - d) * n_side + turn
                            landed(a, f)
                            if final:
                                send_halves(a, f, 1)
                            else:
                                send_line(a, f, block(a, f), down=False)

    beyond = tuple(range(2, n_line - 1))

    def arrived(a, f):
        pl.when(at_end & (f // n_side != z))(lambda: landed(a, f))

    def arrived_all(a):
        def body(f, carry):
            arrived(a, f)
            return carry

        lax.fori_loop(0, n_fs, body, 0)

    def chip_rows(q, core):
        return pl.ds(pl.multiple_of(q * rows + core * half, half), half)

    cuts = (half * 2 // 3 // 16 * 16, half // 2 // 16 * 16)

    def strip(g, k, forwarded):
        low = (k == 1) == forwarded
        return (0, cuts[g]) if low else (cuts[g], half - cuts[g])

    def strip_rows(buffer, g, k, forwarded, q):
        first, size = strip(g, k, forwarded)
        at = pl.multiple_of(q * rows + c * half + first, 16)
        return buffer.at[pl.ds(at, size)]

    def share(g, k, h, buffer, source, base):
        first, size = strip(g, k, h == 0)
        return remote(
            source.at[pl.ds(pl.multiple_of(base + first, 16), size)],
            strip_rows(buffer, g, k, h == 0, q_own),
            team_send.at[g],
            team_recv.at[g, 2 * (k - 1) + h],
            chip_to(k, c),
        )

    def share_landed(g, k, h, buffer):
        place = strip_rows(buffer, g, k, h == 0, chip_q(k, -1))
        sem = team_recv.at[g, 2 * (k - 1) + h]
        remote(place, place, team_send.at[g], sem, partner).wait_recv()

    def across(g, k, buffer):
        place = strip_rows(buffer, g, k, True, chip_q(k, -1))
        return remote(
            place, place, cross_send.at[g], cross_recv.at[g, k - 1], chip_to(FAR - k, c)
        )

    def across_landed(g, k, buffer):
        place = strip_rows(buffer, g, k, True, chip_q(FAR, -1))
        remote(place, place, cross_send.at[g], cross_recv.at[g, k - 1], partner).wait_recv()

    def hand_on(g, k, buffer):
        place = buffer.at[chip_rows(chip_q(k, -1), c)]
        return remote(place, place, pass_send.at[g], pass_recv.at[g, k], partner)

    def hand_landed(g, k, buffer):
        place = buffer.at[chip_rows(chip_q(k, -1), other)]
        remote(place, place, pass_send.at[g], pass_recv.at[g, k], partner).wait_recv()

    def norm_rows(values, gain):
        factor = lax.rsqrt(jnp.mean(values * values, axis=-1, keepdims=True) + 1e-06)
        return (values * factor * gain).astype(jnp.bfloat16)

    step_rows = 64

    def norm_chip(q):
        def body(i, carry):
            at = pl.ds(pl.multiple_of(q * rows + i * step_rows, step_rows), step_rows)
            rows_in[at, :] = norm_rows(tok[at, :].astype(jnp.float32), gains[0:1, :])
            return carry

        lax.fori_loop(0, rows // step_rows, body, 0)

    cols, hidden_cols = w_gate.shape[1], w_ug.shape[1]
    groups = cols // GDIM
    slot = c * n_chip + q_own
    at_hidden = pl.ds(pl.multiple_of(slot * hidden_cols, hidden_cols), hidden_cols)
    at_cols = pl.ds(pl.multiple_of(slot * cols, cols), cols)
    first_gain_in = pltpu.make_async_copy(first_gain, gains.at[0:1], local_sem.at[3])
    locals_in = (
        pltpu.make_async_copy(second_gain, gains.at[1:2], local_sem.at[4]),
        pltpu.make_async_copy(value_gain.at[:, at_cols], scales.at[0:1], local_sem.at[5]),
        pltpu.make_async_copy(value_shift.at[:, at_cols], scales.at[1:2], local_sem.at[6]),
        pltpu.make_async_copy(spatial_bias, biases, local_sem.at[7]),
        pltpu.make_async_copy(
            spatial_weight.at[pl.ds(slot * groups, groups)], mixing, local_sem.at[0]
        ),
        pltpu.make_async_copy(taps_gate.at[:, at_hidden], taps.at[0], local_sem.at[1]),
        pltpu.make_async_copy(taps_value.at[:, at_hidden], taps.at[1], local_sem.at[2]),
    )

    for a in (0, 1):
        own_copy(a).start()
        staged(a).start()

    barrier = pltpu.get_barrier_semaphore()
    for mate in (chip_to(1, c), chip_to(2, c), partner):
        pl.semaphore_signal(barrier, inc=1, device_id=mate, device_id_type=MESH)
    for flag, step in ((has_up, 1), (has_down, -1)):

        @pl.when(flag)
        def _():
            pl.semaphore_signal(
                barrier, inc=1, device_id=(x, f_own + step * n_side, c), device_id_type=MESH
            )

    neighbours = has_up.astype(jnp.int32) + has_down.astype(jnp.int32)
    pl.semaphore_wait(barrier, FAR + neighbours)

    for a in (0, 1):
        own_copy(a).wait()
        send_line(a, f_own, block(a, f_own))
        staged(a).wait()
        side(a).start()
    for h in (0, 1):
        for k in (2, 1):
            share(0, k, h, tok, tokens, c * half).start()
    tok_copy = pltpu.make_async_copy(
        tokens, tok.at[pl.ds(pl.multiple_of(q_own * rows, rows), rows)], own_sem.at[ARRAYS]
    )
    tok_copy.start()
    start_side(2)
    first_gain_in.start()
    for copy in locals_in:
        copy.start()
    relay(0, 0)
    relay(1, 0)
    relay(0, 1)
    tok_copy.wait()
    first_gain_in.wait()
    norm_chip(q_own)
    share_landed(0, 2, 0, tok)
    across(0, 2, tok).start()
    relay(1, 1)
    share_landed(0, 1, 0, tok)
    across(0, 1, tok).start()
    start_side(3)
    relay(0, *beyond)
    share_landed(0, 2, 1, tok)
    hand_on(0, 2, tok).start()
    hand_landed(0, 2, tok)
    norm_chip(chip_q(2, -1))
    relay(1, *beyond)
    start_line(2)
    share_landed(0, 1, 1, tok)
    hand_on(0, 1, tok).start()
    relay(2, 0)
    hand_landed(0, 1, tok)
    norm_chip(chip_q(1, -1))
    relay(2, 1)
    for k in (1, 2):
        across_landed(0, k, tok)
    hand_on(0, FAR, tok).start()
    hand_landed(0, FAR, tok)
    norm_chip(chip_q(FAR, -1))

    def project(weight, target):
        def body(i, carry):
            at = pl.ds(pl.multiple_of(i * half, half), half)
            product = jnp.dot(rows_in[at, :], weight[...], preferred_element_type=jnp.float32)
            target[at, :] = jax.nn.gelu(product)
            return carry

        lax.fori_loop(0, n_chip * n_tp, body, 0)

    blocks = n_chip * rows // BLK
    lane = lax.broadcasted_iota(jnp.int32, (BLK, BLK), 1)
    sub = lax.broadcasted_iota(jnp.int32, (BLK, BLK), 0)
    arrived_all(0)
    project(w_value, value_act)

    def stat_body(i, carry):
        at = pl.ds(pl.multiple_of(i * BLK, BLK), BLK)
        values = value_act[at, :]
        total = jnp.sum(values, axis=1, keepdims=True)
        squares = jnp.sum(values * values, axis=1, keepdims=True)
        both = jnp.where(lane == 0, total, squares).T
        stats[0, :, at] = both[0:2, :]
        return carry

    lax.fori_loop(0, blocks, stat_body, 0)
    mates = [(k, j) for k in range(n_chip) for j in range(n_tp) if k or j]

    def tell(i):
        k, j = mates[i]
        device = chip_to(k, (c + j) % n_tp)
        return remote(stats.at[0], stats.at[i + 1], stat_sem.at[0], stat_sem.at[1], device)

    for i in range(len(mates)):
        tell(i).start()
    start_side(4)
    relay(2, *beyond)
    start_line(3)
    arrived_all(1)
    project(w_gate, gate_act)
    relay(3, 0)
    told = stats.at[pl.ds(1, len(mates))]
    remote(told, told, stat_sem.at[0], stat_sem.at[1], partner).wait_recv()
    for copy in locals_in:
        copy.wait()

    def mix_body(i, carry):
        at = pl.ds(pl.multiple_of(i * BLK, BLK), BLK)
        total = stats[0, :, at]
        for s in range(1, len(mates) + 1):
            total = total + stats[s, :, at]
        row_mean = jnp.broadcast_to(total[0:1, :] / width, (BLK, BLK)).T[:, 0:1]
        row_square = jnp.broadcast_to(total[1:2, :] / width, (BLK, BLK)).T[:, 0:1]
        variance = row_square - row_mean * row_mean
        centred = (
            (value_act[at, :] - row_mean) * lax.rsqrt(variance + 1e-05) * scales[0:1, :]
            + scales[1:2, :]
        ).astype(jnp.bfloat16)
        for g in range(groups):
            group = slot * groups + g
            matrix = mixing[g]
            matrix = jnp.where(sub >= lane, matrix, jnp.zeros_like(matrix))
            bias = jnp.broadcast_to(biases[pl.ds(group, 1), :], (BLK, BLK)).T
            mixed = (
                jnp.dot(
                    matrix, centred[:, g * GDIM : (g + 1) * GDIM], preferred_element_type=jnp.float32
                )
                + bias
            )
            channels = slice(g * GDIM, (g + 1) * GDIM)
            gated[at, channels] = (gate_act[at, channels] * mixed).astype(jnp.bfloat16)
        return carry

    lax.fori_loop(0, blocks, mix_body, 0)

    cut = w_out.shape[2]
    units = n_line * n_side

    near_z = jnp.where(low, z, n_line - 1 - z)

    def line_f(u):
        i = u // n_side
        turn = near_z - (i + 1) // 2 if i % 2 else near_z + i // 2
        p = jnp.where(i > 2 * near_z, i, turn)
        return jnp.where(low, p, n_line - 1 - p) * n_side + u % n_side

    def shape_of(u):
        line, low_col, size = min(u, units - 1), 0, cut
        if isinstance(u, float):
            line, low_col, size = units - 1, int(u * 2) % 2 * (cut // 2), cut // 2
        return line, low_col, size

    def sem_of(u):
        return units - 1 + int(u * 2) % 2 if isinstance(u, float) else u

    def unit_cols(u):
        line, low_col, size = shape_of(u)
        return pl.ds(pl.multiple_of(line_f(line) * cut + low_col, size), size)

    def pair(u, i):
        q, place = chip_q(FAR - i, 1), unit_cols(u)
        return remote(
            part.at[chip_rows(q, other), place],
            from_partner.at[pl.ds(pl.multiple_of(q * half, half), half), place],
            pair_send.at[0],
            pair_recv.at[sem_of(u), jnp.minimum(i, 1)],
            partner,
        )

    def lane(u, near):
        line, low_col, size = shape_of(u)
        if size < cut:
            return (2 - near) * (half // 2), half // 2, unit_cols(u)
        size = cut // 2
        at = line_f(line) * cut + (2 - near) * size
        return 0, half, pl.ds(pl.multiple_of(at, size), size)

    def lane_part(u, near, q):
        first, count, place = lane(u, near)
        return pl.ds(pl.multiple_of(q * rows + c * half + first, 16), count), place

    def to_team(u, near, t):
        first, count, place = lane(u, near)
        k_rows = (near, FAR, FAR - near)[t]
        k_chip = (near, near, FAR - near)[t]
        return remote(
            part.at[lane_part(u, near, chip_q(k_rows, 1))],
            from_team.at[t, pl.ds(first, count), place],
            sum_send.at[0],
            sum_recv.at[sem_of(u), t % 2],
            chip_to(k_chip, c),
        )

    def multiply(u, acts, weight):
        line, low_col, size = shape_of(u)
        band = n_side * rows

        def body(i, carry):
            at_x = (x + 1 + i) % n_rep
            at = pl.ds(pl.multiple_of(at_x * band, band), band)
            part[at, unit_cols(u)] = jnp.dot(
                acts[at, :],
                weight[line_f(line), :, low_col : low_col + size],
                preferred_element_type=jnp.float32,
            ).astype(jnp.bfloat16)
            for j in range(n_side):
                pair(u, i * n_side + j).start()
            return carry

        lax.fori_loop(0, n_rep, body, 0)

    def pair_landed(u, i):
        whole = from_partner.at[pl.ds(0, (1 + i * (n_chip - 2)) * half), unit_cols(u)]
        remote(whole, whole, pair_send.at[0], pair_recv.at[sem_of(u), i], partner).wait_recv()

    def reduce_pair(u, chips=tuple(range(FAR, -1, -1))):
        place = unit_cols(u)
        for k in chips:
            if k >= FAR - 1:
                pair_landed(u, FAR - k)
            q = chip_q(k, 1)
            at = chip_rows(q, c)
            part[at, place] = (
                part[at, place].astype(jnp.float32)
                + from_partner[pl.ds(pl.multiple_of(q * half, half), half), place].astype(
                    jnp.float32
                )
            ).astype(jnp.bfloat16)
            if k == FAR:
                for near in (2, 1):
                    to_team(u, near, 1).start()
            elif k:
                to_team(u, k, 0).start()

    def pass_on(u):
        both = from_team.at[1, :, unit_cols(u)]
        remote(both, both, sum_send.at[0], sum_recv.at[sem_of(u), 1], partner).wait_recv()
        for near in (2, 1):
            first, count, place = lane(u, near)
            at, _ = lane_part(u, near, chip_q(FAR - near, 1))
            come = from_team[1, first : first + count, place]
            part[at, place] = (
                part[at, place].astype(jnp.float32) + come.astype(jnp.float32)
            ).astype(jnp.bfloat16)
            to_team(u, near, 2).start()

    def collected(u):
        rest = from_team.at[pl.ds(0, 2), :, unit_cols(u)]
        remote(rest, rest, sum_send.at[0], sum_recv.at[sem_of(u), 0], partner).wait_recv()

    lag = 2

    def out_units(acts, weight, a):
        for u in range(units):
            if u == units // 2:
                relay(3, 1)
                start_line(4)
            arrived(a, line_f(u))
            multiply(u, acts, weight)
            if u:
                reduce_pair(u - 1)
            if u >= 2 * lag:
                pass_on(u - 2 * lag)
        reduce_pair(units - 1)

    out_units(gated, w_out, 2)
    for u in range(units - 2 * lag, units):
        pass_on(u)
    relay(3, *beyond)
    relay(4, 0)
    for u in range(units):
        collected(u)

    def residual_body(i, carry):
        at = pl.ds(pl.multiple_of(i * step_rows, step_rows), step_rows)
        mine = pl.ds(pl.multiple_of(q_own * rows + c * half + i * step_rows, step_rows), step_rows)
        total = part[mine, :].astype(jnp.float32)
        for t in (0, 2):
            total = total + from_team[t, at, :].astype(jnp.float32)
        kept = (tok[mine, :].astype(jnp.float32) + total).astype(jnp.bfloat16)
        residual[at, :] = kept
        rows_in[mine, :] = norm_rows(kept.astype(jnp.float32), gains[1:2, :])
        return carry

    lax.fori_loop(0, half // step_rows, residual_body, 0)
    for h in (0, 1):
        for k in (1, 2):
            share(1, k, h, rows_in, rows_in, q_own * rows + c * half).start()
    hand_on(1, 0, rows_in).start()
    all_sent(from_partner, pair_send.at[0])
    all_sent(from_team, sum_send.at[0])
    for k in (1, 2):
        share_landed(1, k, 0, rows_in)
        across(1, k, rows_in).start()
    start_side(5)
    relay(4, 1)
    for k in (1, 2):
        share_landed(1, k, 1, rows_in)
        hand_on(1, k, rows_in).start()
    relay(4, *beyond)
    start_line(5)

    position = lax.broadcasted_iota(jnp.int32, (LEN, hidden_cols), 0)

    def conv(values, which):
        back1 = jnp.where(position >= 1, pltpu.roll(values, 1, 0), 0.0)
        back2 = jnp.where(position >= 2, pltpu.roll(values, 2, 0), 0.0)
        weights = taps[which]
        return weights[0:1] * back2 + weights[1:2] * back1 + weights[2:3] * values

    def raise_chip(weight, which, q):
        at = pl.ds(pl.multiple_of(q * rows, rows), rows)
        product = jnp.dot(rows_in[at, :], weight[...], preferred_element_type=jnp.float32)
        for s in range(rows // LEN):
            here = pl.ds(pl.multiple_of(q * rows + s * LEN, LEN), LEN)
            done = conv(product[s * LEN : (s + 1) * LEN], which)
            if which:
                hidden[here, :] = (gate_half[here, :] * done).astype(jnp.bfloat16)
            else:
                gate_half[here, :] = jax.nn.silu(done)

    def raise_gate(k, carry):
        hand_landed(1, k, rows_in)
        raise_chip(w_ug, 0, chip_q(k, -1))
        return carry

    def raise_value(q, carry):
        raise_chip(w_uv, 1, q)
        return carry

    arrived_all(3)
    lax.fori_loop(0, FAR, raise_gate, 0)
    for k in (1, 2):
        across_landed(1, k, rows_in)
    hand_on(1, FAR, rows_in).start()
    relay(5, 0)
    lax.fori_loop(FAR, n_chip, raise_gate, 0)
    arrived_all(4)
    lax.fori_loop(0, n_chip, raise_value, 0)

    def finish(u):
        collected(u)
        place = unit_cols(u)
        mine = chip_rows(q_own, c)
        here = pl.ds(pl.multiple_of(c * half, half), half)
        total = part[mine, place].astype(jnp.float32)
        for t in (0, 2):
            total = total + from_team[t, :, place].astype(jnp.float32)
        out[here, place] = (residual[:, place].astype(jnp.float32) + total).astype(jnp.bfloat16)
        done = out.at[here, place]
        remote(done, done, last_sem.at[0], last_sem.at[1], partner).start()

    order = tuple(range(units - 1)) + (units - 1.0, units - 0.5)
    passed = 0
    for i, u in enumerate(order):
        if u == n_side:
            relay(5, 1)
        elif u % n_side == 0 and u // n_side - 1 in beyond:
            relay(5, u // n_side - 1)
        if isinstance(u, float):
            half_landed(5, line_f(units - 1), i - units + 1)
        else:
            arrived(5, line_f(u))
        multiply(u, hidden, w_down)
        reduce_pair(u, (FAR,))
        while passed < (i - (i < 5)) and i != units - 1:
            pass_on(order[passed])
            passed += 1
        reduce_pair(u, tuple(range(FAR - 1, -1, -1)))
        if units // 2 < i < units - 1:
            finish(order[i - units // 2 - 1])
    for u in order[2:5]:
        finish(u)
    pass_on(order[-1])
    for u in order[5:]:
        finish(u)

    for a in range(ARRAYS):
        all_sent(block(a, 0), side_send.at[a])
        for n in range(1, n_line):
            pl.when(z == n - 1)(lambda: all_sent(blocks_of(a, 0, n * n_side), up_send.at[a]))
            pl.when(z == n)(
                lambda: all_sent(
                    blocks_of(a, n * n_side, (n_line - n) * n_side), down_send.at[a]
                )
            )
    all_sent(told, stat_sem.at[0])
    for g in range(2):
        all_sent(tok.at[pl.ds(0, rows)], team_send.at[g])
        all_sent(tok.at[pl.ds(0, half)], cross_send.at[g])
        all_sent(tok.at[pl.ds(0, (n_chip - 1 + g) * half)], pass_send.at[g])
    all_sent(from_partner, pair_send.at[0])
    all_sent(from_team, sum_send.at[0])
    theirs = out.at[pl.ds(pl.multiple_of(other * half, half), half)]
    last = remote(theirs, theirs, last_sem.at[0], last_sem.at[1], partner)
    last.wait_send()
    last.wait_recv()


def team_layer(
    dims,
    tokens,
    first_gain,
    mixer_gate,
    mixer_value,
    value_gain,
    value_shift,
    spatial_weight,
    spatial_bias,
    mixer_out,
    second_gain,
    up_gate,
    up_value,
    taps_gate,
    taps_value,
    down_proj,
):
    n_rep, n_fs, n_tp = dims
    n_chip, n_line = n_rep * PLANE, n_fs // PLANE
    rows, width = tokens.shape
    half, team_rows = rows // n_tp, rows * n_chip
    cols, hidden_cols = mixer_gate.shape[1] // n_chip, up_gate.shape[1] // n_chip
    vmem, anywhere = pl.BlockSpec(memory_space=pltpu.VMEM), pl.BlockSpec(memory_space=pl.ANY)
    bf16, f32, dma = jnp.bfloat16, jnp.float32, pltpu.SemaphoreType.DMA
    in_specs = [anywhere] * 15
    units = n_fs
    scratch = [
        pltpu.VMEM((width, cols), bf16),
        pltpu.VMEM((width, cols), bf16),
        pltpu.VMEM((n_fs, mixer_out.shape[0] // n_chip, mixer_out.shape[1]), bf16),
        pltpu.VMEM((width, hidden_cols), bf16),
        pltpu.VMEM((width, hidden_cols), bf16),
        pltpu.VMEM((n_fs, down_proj.shape[0] // n_chip, down_proj.shape[1]), bf16),
        pltpu.VMEM((team_rows, width), bf16),
        pltpu.VMEM((team_rows, width), bf16),
        pltpu.VMEM((team_rows, cols), f32),
        pltpu.VMEM((team_rows, cols), f32),
        pltpu.VMEM((team_rows, cols), bf16),
        pltpu.VMEM((team_rows, hidden_cols), f32),
        pltpu.VMEM((team_rows, hidden_cols), bf16),
        pltpu.VMEM((team_rows, width), bf16),
        pltpu.VMEM((n_chip * half, width), bf16),
        pltpu.VMEM((n_chip - 1, half, width), bf16),
        pltpu.VMEM((half, width), bf16),
        pltpu.VMEM((n_chip * n_tp, 2, team_rows), f32),
        pltpu.VMEM((cols // GDIM,) + spatial_weight.shape[1:], bf16),
        pltpu.VMEM((2, 3, hidden_cols), f32),
        pltpu.VMEM((2, width), f32),
        pltpu.VMEM((2, cols), f32),
        pltpu.VMEM(spatial_bias.shape, f32),
        pltpu.VMEM((2, mixer_value.shape[0], cols), bf16),
        dma((ARRAYS + 1,)),
        dma((ARRAYS,)),
        dma((ARRAYS,)),
        dma((ARRAYS,)),
        dma((ARRAYS, n_fs)),
        dma((2,)),
        dma((2, 4)),
        dma((2,)),
        dma((2, n_chip)),
        dma((2,)),
        dma((1,)),
        dma((units + 1, 2)),
        dma((1,)),
        dma((units + 1, 2)),
        dma((2,)),
        dma((2, 2)),
        dma((2,)),
        dma((10,)),
        dma((1,)),
    ]
    return pl.pallas_call(
        functools.partial(team_kernel, dims),
        out_shape=pltpu.VMEM((rows, width), bf16),
        in_specs=in_specs,
        out_specs=vmem,
        scratch_shapes=scratch,
        compiler_params=pltpu.CompilerParams(
            collective_id=0, has_side_effects=True, vmem_limit_bytes=56 * 1024 * 1024
        ),
    )(
        tokens,
        first_gain.reshape(1, -1),
        mixer_gate,
        mixer_value,
        value_gain.reshape(1, -1),
        value_shift.reshape(1, -1),
        spatial_weight,
        spatial_bias,
        mixer_out,
        second_gain.reshape(1, -1),
        up_gate,
        up_value,
        taps_gate,
        taps_value,
        down_proj,
    )


def team_fits(mesh):
    n_rep, n_fs, n_tp = (mesh.shape[name] for name in ("rep", "fs", "tp"))
    if n_tp != 2 or n_rep * PLANE != FAR + 1 or n_fs % PLANE or n_fs < 3 * PLANE:
        return False
    return D % (n_fs * GDIM) == 0 and D % (n_tp * n_rep * PLANE * GDIM) == 0


def solution(mesh):
    in_specs = (
        P(("rep", "fs"), None),
        P(),
        P("fs", "tp"),
        P("fs", "tp"),
        P(),
        P(),
        P(),
        P(),
        P("tp", "fs"),
        P(),
        P("fs", "tp"),
        P("fs", "tp"),
        P(),
        P(),
        P("tp", "fs"),
    )
    out_specs = P(("rep", "fs"), None)
    body = local
    if team_fits(mesh):
        dims = tuple(mesh.shape[name] for name in ("rep", "fs", "tp"))
        body = functools.partial(team_layer, dims)
    return jax.shard_map(body, mesh=mesh, in_specs=in_specs, out_specs=out_specs, check_vma=False)
```

```python
import functools

import jax
import jax.numpy as jnp
from jax import lax
from jax.experimental import pallas as pl
from jax.experimental.pallas import tpu as pltpu
from jax.sharding import PartitionSpec as P

D = 2048
GDIM = 128
BLK = 128
LEN = 128


def normalize(matrix, scale_gain):
    values = matrix.astype(jnp.float32)
    factor = lax.rsqrt(jnp.mean(values * values, axis=-1, keepdims=True) + 1e-06)
    return (values * factor * scale_gain).astype(jnp.bfloat16)


def causal_conv(values, tap_weights):
    by_sequence = values.reshape(-1, LEN, values.shape[-1])
    padded = jnp.pad(by_sequence, ((0, 0), (2, 0), (0, 0)))
    summed = (
        tap_weights[0] * padded[:, 0:LEN]
        + tap_weights[1] * padded[:, 1 : LEN + 1]
        + tap_weights[2] * padded[:, 2 : LEN + 2]
    )
    return summed.reshape(values.shape)


def local(
    tokens,
    first_gain,
    mixer_gate,
    mixer_value,
    value_gain,
    value_shift,
    spatial_weight,
    spatial_bias,
    mixer_out,
    second_gain,
    up_gate,
    up_value,
    taps_gate,
    taps_value,
    down_proj,
):
    n_rep, n_tp = lax.axis_size("rep"), lax.axis_size("tp")
    rep_index, tp_index = lax.axis_index("rep"), lax.axis_index("tp")
    team = ("rep", "tp")

    def part(array, axis):
        width = array.shape[axis] // n_rep
        return lax.dynamic_slice_in_dim(array, rep_index * width, width, axis)

    def own(array, width, axis):
        at = (tp_index * n_rep + rep_index) * width
        return lax.dynamic_slice_in_dim(array, at, width, axis)

    w_gate = lax.all_gather(part(mixer_gate, 1), "fs", axis=0, tiled=True)
    w_value = lax.all_gather(part(mixer_value, 1), "fs", axis=0, tiled=True)
    w_out = lax.all_gather(part(mixer_out, 0), "fs", axis=1, tiled=True)
    u_gate = lax.all_gather(part(up_gate, 1), "fs", axis=0, tiled=True)
    u_value = lax.all_gather(part(up_value, 1), "fs", axis=0, tiled=True)
    w_down = lax.all_gather(part(down_proj, 0), "fs", axis=1, tiled=True)

    row_share = tokens.shape[0] // n_tp
    kept_tokens = lax.dynamic_slice_in_dim(tokens, tp_index * row_share, row_share, 0)
    first = lax.all_gather(normalize(kept_tokens, first_gain), team, axis=0, tiled=True)
    row_count = first.shape[0]
    cols = w_gate.shape[1]
    gate_act = jax.nn.gelu(jnp.dot(first, w_gate, preferred_element_type=jnp.float32))
    value_act = jax.nn.gelu(jnp.dot(first, w_value, preferred_element_type=jnp.float32))
    value_sum, value_squares = lax.psum(
        (jnp.sum(value_act, axis=1), jnp.sum(value_act * value_act, axis=1)), team
    )
    row_mean = value_sum / D
    variance = value_squares / D - row_mean * row_mean
    centred = (
        (value_act - row_mean[:, None])
        * lax.rsqrt(variance[:, None] + 1e-05)
        * own(value_gain, cols, 0)
        + own(value_shift, cols, 0)
    ).astype(jnp.bfloat16)
    groups = cols // GDIM
    masked = own(spatial_weight, groups, 0) * jnp.tril(jnp.ones((BLK, BLK), jnp.bfloat16))
    blocks = centred.reshape(row_count // BLK, BLK, groups, GDIM)
    mixed_rows = (
        jnp.einsum("gts,bsgc->btgc", masked, blocks, preferred_element_type=jnp.float32)
        + own(spatial_bias, groups, 0).T[None, :, :, None]
    )
    gated_rows = (gate_act * mixed_rows.reshape(row_count, cols)).astype(jnp.bfloat16)
    summed = lax.psum_scatter(
        jnp.dot(gated_rows, w_out, preferred_element_type=jnp.float32).astype(jnp.bfloat16),
        team,
        scatter_dimension=0,
        tiled=True,
    ).astype(jnp.float32)
    residual = (kept_tokens.astype(jnp.float32) + summed).astype(jnp.bfloat16)
    second = lax.all_gather(normalize(residual, second_gain), team, axis=0, tiled=True)
    hidden_cols = u_gate.shape[1]
    gate_up = jnp.dot(second, u_gate, preferred_element_type=jnp.float32)
    value_up = jnp.dot(second, u_value, preferred_element_type=jnp.float32)
    hidden = (
        jax.nn.silu(causal_conv(gate_up, own(taps_gate, hidden_cols, 1)))
        * causal_conv(value_up, own(taps_value, hidden_cols, 1))
    ).astype(jnp.bfloat16)
    ffn_total = lax.psum_scatter(
        jnp.dot(hidden, w_down, preferred_element_type=jnp.float32).astype(jnp.bfloat16),
        team,
        scatter_dimension=0,
        tiled=True,
    ).astype(jnp.float32)
    final_rows = (residual.astype(jnp.float32) + ffn_total).astype(jnp.bfloat16)
    return lax.all_gather(final_rows, "tp", axis=0, tiled=True)


PLANE = 2
ARRAYS = 6
FAR = 3
MESH = pl.DeviceIdType.MESH


def team_kernel(
    dims,
    tokens,
    first_gain,
    mixer_gate,
    mixer_value,
    value_gain,
    value_shift,
    spatial_weight,
    spatial_bias,
    mixer_out,
    second_gain,
    up_gate,
    up_value,
    taps_gate,
    taps_value,
    down_proj,
    out,
    w_gate,
    w_value,
    w_out,
    w_ug,
    w_uv,
    w_down,
    tok,
    rows_in,
    gate_act,
    value_act,
    gated,
    gate_half,
    hidden,
    part,
    from_partner,
    from_team,
    residual,
    stats,
    mixing,
    taps,
    gains,
    scales,
    biases,
    ahead,
    own_sem,
    side_send,
    up_send,
    down_send,
    weight_recv,
    team_send,
    team_recv,
    pass_send,
    pass_recv,
    stat_sem,
    pair_send,
    pair_recv,
    sum_send,
    sum_recv,
    cross_send,
    cross_recv,
    last_sem,
    local_sem,
    late_recv,
):
    n_rep, n_fs, n_tp = dims
    n_side, n_line = PLANE, n_fs // PLANE
    n_chip = n_rep * n_side
    x, c = lax.axis_index("rep"), lax.axis_index("tp")
    f_own = lax.axis_index("fs")
    z, y = f_own // n_side, f_own % n_side
    other = (c + 1) % n_tp
    q_own = x * n_side + y
    rows = tokens.shape[0]
    half = rows // n_tp
    width = tokens.shape[1]
    sources = (mixer_value, mixer_gate, mixer_out, up_gate, up_value, down_proj)
    held = (w_value, w_gate, w_out, w_ug, w_uv, w_down)
    partner = (x, f_own, other)
    has_up, has_down = z + 1 < n_line, z >= 1
    at_end = (z == 0) | (z == n_line - 1)
    low = z < n_line // 2

    def chip_to(k, core):
        dx, dy = k // n_side, k % n_side
        return ((x + dx) % n_rep, z * n_side + (y + dy) % n_side, core)

    def chip_q(k, sign):
        dx, dy = k // n_side, k % n_side
        return ((x + sign * dx + n_rep) % n_rep) * n_side + (y + sign * dy + n_side) % n_side

    def remote(src, dst, send, recv, device):
        return pltpu.make_async_remote_copy(
            src_ref=src, dst_ref=dst, send_sem=send, recv_sem=recv, device_id=device, device_id_type=MESH
        )

    def all_sent(ref, sem):
        remote(ref, ref, sem, sem, partner).wait_send()

    def blocks_of(a, f, count):
        if len(held[a].shape) == 3:
            return held[a].at[pl.ds(f, count)]
        height = sources[a].shape[0]
        return held[a].at[pl.ds(pl.multiple_of(f * height, height), count * height)]

    def block(a, f):
        return held[a].at[f] if len(held[a].shape) == 3 else blocks_of(a, f, 1)

    def piece(a, q):
        if len(held[a].shape) == 3:
            height = sources[a].shape[0] // n_chip
            return sources[a].at[pl.ds(pl.multiple_of(q * height, height), height)]
        cols = sources[a].shape[1] // n_chip
        return sources[a].at[:, pl.ds(pl.multiple_of(q * cols, cols), cols)]

    def own_copy(a):
        return pltpu.make_async_copy(piece(a, q_own), block(a, f_own), weight_recv.at[a, f_own])

    q_side = x * n_side + (y + 1) % n_side

    def staged(a):
        return pltpu.make_async_copy(piece(a, q_side), ahead.at[a], local_sem.at[8 + a])

    def side(a):
        to_y = (y + 1) % n_side
        return remote(
            piece(a, q_side) if a > 1 else ahead.at[a],
            block(a, f_own),
            side_send.at[0],
            weight_recv.at[a, f_own],
            (x, z * n_side + to_y, c),
        )

    def along(a, f, step, src):
        sem = up_send if step == 1 else down_send
        return remote(
            src, block(a, f), sem.at[a // 4], weight_recv.at[a, f], (x, f_own + step * n_side, c)
        )

    def halves(a, f):
        cut = sources[a].shape[1] // 2
        return [held[a].at[f, :, pl.ds(h * cut, cut)] for h in (0, 1)]

    def send_halves(a, f, step):
        for h, ref in enumerate(halves(a, f)):
            sem = up_send if step == 1 else down_send
            recv = late_recv.at[0] if h else weight_recv.at[a, f]
            remote(ref, ref, sem.at[a // 4], recv, (x, f_own + step * n_side, c)).start()

    def half_landed(a, f, h):
        ref = halves(a, f)[h]
        recv = late_recv.at[0] if h else weight_recv.at[a, f]
        pl.when(at_end)(lambda: remote(ref, ref, side_send.at[0], recv, partner).wait_recv())

    def landed(a, f):
        remote(block(a, f), block(a, f), side_send.at[0], weight_recv.at[a, f], partner).wait_recv()

    def send_line(a, f, src, up=True, down=True):
        if up:
            pl.when(has_up)(lambda: along(a, f, 1, src).start())
        if down:
            pl.when(has_down)(lambda: along(a, f, -1, src).start())

    def start_side(a):
        own_copy(a).start()
        side(a).start()

    def start_line(a):
        send_line(a, f_own, piece(a, q_own))

    def relay(a, *distances):
        for d in distances:
            if d == 0:
                f = z * n_side + (y + 1) % n_side
                landed(a, f)
                send_line(a, f, block(a, f))
                if a > 1:
                    own_copy(a).wait()
                continue
            for j in range(n_side):
                turn = j if a in (2, 5) else (y + j) % n_side
                final = a == ARRAYS - 1 and d == n_line - 2 and j == n_side - 1
                for first in (True, False):
                    above = low if first else jnp.logical_not(low)

                    @pl.when((z + d < n_line) & has_down & above)
                    def _():
                        f = (z + d) * n_side + turn
                        landed(a, f)
                        if final:
                            send_halves(a, f, -1)
                        else:
                            send_line(a, f, block(a, f), up=False)

                    if first:

                        @pl.when((z - d >= 0) & has_up)
                        def _():
                            f = (z - d) * n_side + turn
                            landed(a, f)
                            if final:
                                send_halves(a, f, 1)
                            else:
                                send_line(a, f, block(a, f), down=False)

    beyond = tuple(range(2, n_line - 1))

    def arrived(a, f):
        pl.when(at_end & (f // n_side != z))(lambda: landed(a, f))

    def arrived_all(a):
        def body(f, carry):
            arrived(a, f)
            return carry

        lax.fori_loop(0, n_fs, body, 0)

    def chip_rows(q, core):
        return pl.ds(pl.multiple_of(q * rows + core * half, half), half)

    cuts = (half * 2 // 3 // 16 * 16, half // 2 // 16 * 16)

    def strip(g, k, forwarded):
        low = (k == 1) == forwarded
        return (0, cuts[g]) if low else (cuts[g], half - cuts[g])

    def strip_rows(buffer, g, k, forwarded, q):
        first, size = strip(g, k, forwarded)
        at = pl.multiple_of(q * rows + c * half + first, 16)
        return buffer.at[pl.ds(at, size)]

    def share(g, k, h, buffer, source, base):
        first, size = strip(g, k, h == 0)
        return remote(
            source.at[pl.ds(pl.multiple_of(base + first, 16), size)],
            strip_rows(buffer, g, k, h == 0, q_own),
            team_send.at[g],
            team_recv.at[g, 2 * (k - 1) + h],
            chip_to(k, c),
        )

    def share_landed(g, k, h, buffer):
        place = strip_rows(buffer, g, k, h == 0, chip_q(k, -1))
        sem = team_recv.at[g, 2 * (k - 1) + h]
        remote(place, place, team_send.at[g], sem, partner).wait_recv()

    def across(g, k, buffer):
        place = strip_rows(buffer, g, k, True, chip_q(k, -1))
        return remote(
            place, place, cross_send.at[g], cross_recv.at[g, k - 1], chip_to(FAR - k, c)
        )

    def across_landed(g, k, buffer):
        place = strip_rows(buffer, g, k, True, chip_q(FAR, -1))
        remote(place, place, cross_send.at[g], cross_recv.at[g, k - 1], partner).wait_recv()

    def hand_on(g, k, buffer):
        place = buffer.at[chip_rows(chip_q(k, -1), c)]
        return remote(place, place, pass_send.at[g], pass_recv.at[g, k], partner)

    def hand_landed(g, k, buffer):
        place = buffer.at[chip_rows(chip_q(k, -1), other)]
        remote(place, place, pass_send.at[g], pass_recv.at[g, k], partner).wait_recv()

    def norm_rows(values, gain):
        factor = lax.rsqrt(jnp.mean(values * values, axis=-1, keepdims=True) + 1e-06)
        return (values * factor * gain).astype(jnp.bfloat16)

    step_rows = 64

    def norm_chip(q):
        def body(i, carry):
            at = pl.ds(pl.multiple_of(q * rows + i * step_rows, step_rows), step_rows)
            rows_in[at, :] = norm_rows(tok[at, :].astype(jnp.float32), gains[0:1, :])
            return carry

        lax.fori_loop(0, rows // step_rows, body, 0)

    cols, hidden_cols = w_gate.shape[1], w_ug.shape[1]
    groups = cols // GDIM
    slot = c * n_chip + q_own
    at_hidden = pl.ds(pl.multiple_of(slot * hidden_cols, hidden_cols), hidden_cols)
    at_cols = pl.ds(pl.multiple_of(slot * cols, cols), cols)
    first_gain_in = pltpu.make_async_copy(first_gain, gains.at[0:1], local_sem.at[3])
    locals_in = (
        pltpu.make_async_copy(second_gain, gains.at[1:2], local_sem.at[4]),
        pltpu.make_async_copy(value_gain.at[:, at_cols], scales.at[0:1], local_sem.at[5]),
        pltpu.make_async_copy(value_shift.at[:, at_cols], scales.at[1:2], local_sem.at[6]),
        pltpu.make_async_copy(spatial_bias, biases, local_sem.at[7]),
        pltpu.make_async_copy(
            spatial_weight.at[pl.ds(slot * groups, groups)], mixing, local_sem.at[0]
        ),
        pltpu.make_async_copy(taps_gate.at[:, at_hidden], taps.at[0], local_sem.at[1]),
        pltpu.make_async_copy(taps_value.at[:, at_hidden], taps.at[1], local_sem.at[2]),
    )

    for a in (0, 1):
        own_copy(a).start()
        staged(a).start()

    barrier = pltpu.get_barrier_semaphore()
    for mate in (chip_to(1, c), chip_to(2, c), partner):
        pl.semaphore_signal(barrier, inc=1, device_id=mate, device_id_type=MESH)
    for flag, step in ((has_up, 1), (has_down, -1)):

        @pl.when(flag)
        def _():
            pl.semaphore_signal(
                barrier, inc=1, device_id=(x, f_own + step * n_side, c), device_id_type=MESH
            )

    neighbours = has_up.astype(jnp.int32) + has_down.astype(jnp.int32)
    pl.semaphore_wait(barrier, FAR + neighbours)

    for a in (0, 1):
        own_copy(a).wait()
        send_line(a, f_own, block(a, f_own))
        staged(a).wait()
        side(a).start()
    for h in (0, 1):
        for k in (2, 1):
            share(0, k, h, tok, tokens, c * half).start()
    tok_copy = pltpu.make_async_copy(
        tokens, tok.at[pl.ds(pl.multiple_of(q_own * rows, rows), rows)], own_sem.at[0]
    )
    tok_copy.start()
    start_side(2)
    first_gain_in.start()
    for copy in locals_in:
        copy.start()
    relay(0, 0)
    relay(1, 0)
    relay(0, 1)
    tok_copy.wait()
    first_gain_in.wait()
    norm_chip(q_own)
    share_landed(0, 2, 0, tok)
    across(0, 2, tok).start()
    relay(1, 1)
    share_landed(0, 1, 0, tok)
    across(0, 1, tok).start()
    start_side(3)
    relay(0, *beyond)
    share_landed(0, 2, 1, tok)
    hand_on(0, 2, tok).start()
    hand_landed(0, 2, tok)
    norm_chip(chip_q(2, -1))
    relay(1, *beyond)
    start_line(2)
    share_landed(0, 1, 1, tok)
    hand_on(0, 1, tok).start()
    relay(2, 0)
    hand_landed(0, 1, tok)
    norm_chip(chip_q(1, -1))
    relay(2, 1)
    for k in (1, 2):
        across_landed(0, k, tok)
    hand_on(0, FAR, tok).start()
    hand_landed(0, FAR, tok)
    norm_chip(chip_q(FAR, -1))

    def project(weight, target):
        def body(i, carry):
            at = pl.ds(pl.multiple_of(i * half, half), half)
            product = jnp.dot(rows_in[at, :], weight[...], preferred_element_type=jnp.float32)
            target[at, :] = jax.nn.gelu(product)
            return carry

        lax.fori_loop(0, n_chip * n_tp, body, 0)

    blocks = n_chip * rows // BLK
    lane = lax.broadcasted_iota(jnp.int32, (BLK, BLK), 1)
    sub = lax.broadcasted_iota(jnp.int32, (BLK, BLK), 0)
    arrived_all(0)
    project(w_value, value_act)

    def stat_body(i, carry):
        at = pl.ds(pl.multiple_of(i * BLK, BLK), BLK)
        values = value_act[at, :]
        total = jnp.sum(values, axis=1, keepdims=True)
        squares = jnp.sum(values * values, axis=1, keepdims=True)
        both = jnp.where(lane == 0, total, squares).T
        stats[0, :, at] = both[0:2, :]
        return carry

    lax.fori_loop(0, blocks, stat_body, 0)
    mates = [(k, j) for k in range(n_chip) for j in range(n_tp) if k or j]

    def tell(i):
        k, j = mates[i]
        device = chip_to(k, (c + j) % n_tp)
        return remote(stats.at[0], stats.at[i + 1], stat_sem.at[0], stat_sem.at[1], device)

    for i in range(len(mates)):
        tell(i).start()
    start_side(4)
    relay(2, *beyond)
    start_line(3)
    arrived_all(1)
    project(w_gate, gate_act)
    relay(3, 0)
    told = stats.at[pl.ds(1, len(mates))]
    remote(told, told, stat_sem.at[0], stat_sem.at[1], partner).wait_recv()
    for copy in locals_in:
        copy.wait()

    def mix_body(i, carry):
        at = pl.ds(pl.multiple_of(i * BLK, BLK), BLK)
        total = stats[0, :, at]
        for s in range(1, len(mates) + 1):
            total = total + stats[s, :, at]
        row_mean = jnp.broadcast_to(total[0:1, :] / width, (BLK, BLK)).T[:, 0:1]
        row_square = jnp.broadcast_to(total[1:2, :] / width, (BLK, BLK)).T[:, 0:1]
        variance = row_square - row_mean * row_mean
        centred = (
            (value_act[at, :] - row_mean) * lax.rsqrt(variance + 1e-05) * scales[0:1, :]
            + scales[1:2, :]
        ).astype(jnp.bfloat16)
        for g in range(groups):
            group = slot * groups + g
            matrix = mixing[g]
            matrix = jnp.where(sub >= lane, matrix, jnp.zeros_like(matrix))
            bias = jnp.broadcast_to(biases[pl.ds(group, 1), :], (BLK, BLK)).T
            mixed = (
                jnp.dot(
                    matrix, centred[:, g * GDIM : (g + 1) * GDIM], preferred_element_type=jnp.float32
                )
                + bias
            )
            channels = slice(g * GDIM, (g + 1) * GDIM)
            gated[at, channels] = (gate_act[at, channels] * mixed).astype(jnp.bfloat16)
        return carry

    lax.fori_loop(0, blocks, mix_body, 0)

    cut = w_out.shape[2]
    units = n_line * n_side

    near_z = jnp.where(low, z, n_line - 1 - z)

    def line_f(u):
        i = u // n_side
        turn = near_z - (i + 1) // 2 if i % 2 else near_z + i // 2
        p = jnp.where(i > 2 * near_z, i, turn)
        return jnp.where(low, p, n_line - 1 - p) * n_side + u % n_side

    def shape_of(u):
        line, low_col, size = min(u, units - 1), 0, cut
        if isinstance(u, float):
            line, low_col, size = units - 1, int(u * 2) % 2 * (cut // 2), cut // 2
        return line, low_col, size

    def sem_of(u):
        return units - 1 + int(u * 2) % 2 if isinstance(u, float) else u

    def unit_cols(u):
        line, low_col, size = shape_of(u)
        return pl.ds(pl.multiple_of(line_f(line) * cut + low_col, size), size)

    def pair(u, i):
        q, place = chip_q(FAR - i, 1), unit_cols(u)
        return remote(
            part.at[chip_rows(q, other), place],
            from_partner.at[pl.ds(pl.multiple_of(q * half, half), half), place],
            pair_send.at[0],
            pair_recv.at[sem_of(u), jnp.minimum(i, 1)],
            partner,
        )

    def lane(u, near):
        line, low_col, size = shape_of(u)
        if size < cut:
            return (2 - near) * (half // 2), half // 2, unit_cols(u)
        size = cut // 2
        at = line_f(line) * cut + (2 - near) * size
        return 0, half, pl.ds(pl.multiple_of(at, size), size)

    def lane_part(u, near, q):
        first, count, place = lane(u, near)
        return pl.ds(pl.multiple_of(q * rows + c * half + first, 16), count), place

    def to_team(u, near, t):
        first, count, place = lane(u, near)
        k_rows = (near, FAR, FAR - near)[t]
        k_chip = (near, near, FAR - near)[t]
        return remote(
            part.at[lane_part(u, near, chip_q(k_rows, 1))],
            from_team.at[t, pl.ds(first, count), place],
            sum_send.at[0],
            sum_recv.at[sem_of(u), t % 2],
            chip_to(k_chip, c),
        )

    def multiply(u, acts, weight):
        line, low_col, size = shape_of(u)
        band = n_side * rows

        def body(i, carry):
            at_x = (x + 1 + i) % n_rep
            at = pl.ds(pl.multiple_of(at_x * band, band), band)
            part[at, unit_cols(u)] = jnp.dot(
                acts[at, :],
                weight[line_f(line), :, low_col : low_col + size],
                preferred_element_type=jnp.float32,
            ).astype(jnp.bfloat16)
            for j in range(n_side):
                pair(u, i * n_side + j).start()
            return carry

        lax.fori_loop(0, n_rep, body, 0)

    def pair_landed(u, i):
        whole = from_partner.at[pl.ds(0, (1 + i * (n_chip - 2)) * half), unit_cols(u)]
        remote(whole, whole, pair_send.at[0], pair_recv.at[sem_of(u), i], partner).wait_recv()

    def reduce_pair(u, chips=tuple(range(FAR, -1, -1))):
        place = unit_cols(u)
        for k in chips:
            if k >= FAR - 1:
                pair_landed(u, FAR - k)
            q = chip_q(k, 1)
            at = chip_rows(q, c)
            part[at, place] = (
                part[at, place].astype(jnp.float32)
                + from_partner[pl.ds(pl.multiple_of(q * half, half), half), place].astype(
                    jnp.float32
                )
            ).astype(jnp.bfloat16)
            if k == FAR:
                for near in (2, 1):
                    to_team(u, near, 1).start()
            elif k:
                to_team(u, k, 0).start()

    def pass_on(u):
        both = from_team.at[1, :, unit_cols(u)]
        remote(both, both, sum_send.at[0], sum_recv.at[sem_of(u), 1], partner).wait_recv()
        for near in (2, 1):
            first, count, place = lane(u, near)
            at, _ = lane_part(u, near, chip_q(FAR - near, 1))
            come = from_team[1, first : first + count, place]
            part[at, place] = (
                part[at, place].astype(jnp.float32) + come.astype(jnp.float32)
            ).astype(jnp.bfloat16)
            to_team(u, near, 2).start()

    def collected(u):
        rest = from_team.at[pl.ds(0, 2), :, unit_cols(u)]
        remote(rest, rest, sum_send.at[0], sum_recv.at[sem_of(u), 0], partner).wait_recv()

    lag = 2

    def out_units(acts, weight, a):
        for u in range(units):
            if u == units // 2:
                relay(3, 1)
                start_line(4)
            arrived(a, line_f(u))
            multiply(u, acts, weight)
            if u:
                reduce_pair(u - 1)
            if u >= 2 * lag:
                pass_on(u - 2 * lag)
        reduce_pair(units - 1)

    out_units(gated, w_out, 2)
    for u in range(units - 2 * lag, units):
        pass_on(u)
    relay(3, *beyond)
    relay(4, 0)
    for u in range(units):
        collected(u)

    def residual_body(i, carry):
        at = pl.ds(pl.multiple_of(i * step_rows, step_rows), step_rows)
        mine = pl.ds(pl.multiple_of(q_own * rows + c * half + i * step_rows, step_rows), step_rows)
        total = part[mine, :].astype(jnp.float32)
        for t in (0, 2):
            total = total + from_team[t, at, :].astype(jnp.float32)
        kept = (tok[mine, :].astype(jnp.float32) + total).astype(jnp.bfloat16)
        residual[at, :] = kept
        rows_in[mine, :] = norm_rows(kept.astype(jnp.float32), gains[1:2, :])
        return carry

    lax.fori_loop(0, half // step_rows, residual_body, 0)
    for h in (0, 1):
        for k in (1, 2):
            share(1, k, h, rows_in, rows_in, q_own * rows + c * half).start()
    hand_on(1, 0, rows_in).start()
    all_sent(from_partner, pair_send.at[0])
    all_sent(from_team, sum_send.at[0])
    for k in (1, 2):
        share_landed(1, k, 0, rows_in)
        across(1, k, rows_in).start()
    start_side(5)
    relay(4, 1)
    for k in (1, 2):
        share_landed(1, k, 1, rows_in)
        hand_on(1, k, rows_in).start()
    relay(4, *beyond)
    start_line(5)

    position = lax.broadcasted_iota(jnp.int32, (LEN, hidden_cols), 0)

    def conv(values, which):
        back1 = jnp.where(position >= 1, pltpu.roll(values, 1, 0), 0.0)
        back2 = jnp.where(position >= 2, pltpu.roll(values, 2, 0), 0.0)
        weights = taps[which]
        return weights[0:1] * back2 + weights[1:2] * back1 + weights[2:3] * values

    def raise_chip(weight, which, q):
        at = pl.ds(pl.multiple_of(q * rows, rows), rows)
        product = jnp.dot(rows_in[at, :], weight[...], preferred_element_type=jnp.float32)
        for s in range(rows // LEN):
            here = pl.ds(pl.multiple_of(q * rows + s * LEN, LEN), LEN)
            done = conv(product[s * LEN : (s + 1) * LEN], which)
            if which:
                hidden[here, :] = (gate_half[here, :] * done).astype(jnp.bfloat16)
            else:
                gate_half[here, :] = jax.nn.silu(done)

    def raise_gate(k, carry):
        hand_landed(1, k, rows_in)
        raise_chip(w_ug, 0, chip_q(k, -1))
        return carry

    def raise_value(q, carry):
        raise_chip(w_uv, 1, q)
        return carry

    arrived_all(3)
    lax.fori_loop(0, FAR, raise_gate, 0)
    for k in (1, 2):
        across_landed(1, k, rows_in)
    hand_on(1, FAR, rows_in).start()
    relay(5, 0)
    lax.fori_loop(FAR, n_chip, raise_gate, 0)
    arrived_all(4)
    lax.fori_loop(0, n_chip, raise_value, 0)

    def finish(u):
        collected(u)
        place = unit_cols(u)
        mine = chip_rows(q_own, c)
        here = pl.ds(pl.multiple_of(c * half, half), half)
        total = part[mine, place].astype(jnp.float32)
        for t in (0, 2):
            total = total + from_team[t, :, place].astype(jnp.float32)
        out[here, place] = (residual[:, place].astype(jnp.float32) + total).astype(jnp.bfloat16)
        done = out.at[here, place]
        remote(done, done, last_sem.at[0], last_sem.at[1], partner).start()

    order = tuple(range(units - 1)) + (units - 1.0, units - 0.5)
    passed = 0
    for i, u in enumerate(order):
        if u == n_side:
            relay(5, 1)
        elif u % n_side == 0 and u // n_side - 1 in beyond:
            relay(5, u // n_side - 1)
        if isinstance(u, float):
            half_landed(5, line_f(units - 1), i - units + 1)
        else:
            arrived(5, line_f(u))
        multiply(u, hidden, w_down)
        reduce_pair(u, (FAR,))
        while passed < (i - (i < 5)) and i != units - 1:
            pass_on(order[passed])
            passed += 1
        reduce_pair(u, tuple(range(FAR - 1, -1, -1)))
        if units // 2 < i < units - 1:
            finish(order[i - units // 2 - 1])
    for u in order[2:5]:
        finish(u)
    pass_on(order[-1])
    for u in order[5:]:
        finish(u)

    def flat(arrays, count):
        size = sum(block(a, 0).shape[0] * block(a, 0).shape[1] for a in arrays)
        return tok.at[pl.ds(0, count * size // width)]

    all_sent(flat(range(ARRAYS), 1), side_send.at[0])
    for i, arrays in enumerate((range(4), range(4, ARRAYS))):
        for n in range(1, n_line):
            pl.when(z == n - 1)(lambda: all_sent(flat(arrays, n * n_side), up_send.at[i]))
            pl.when(z == n)(
                lambda: all_sent(flat(arrays, (n_line - n) * n_side), down_send.at[i])
            )
    all_sent(told, stat_sem.at[0])
    for g in range(2):
        all_sent(tok.at[pl.ds(0, rows)], team_send.at[g])
        all_sent(tok.at[pl.ds(0, half)], cross_send.at[g])
        all_sent(tok.at[pl.ds(0, (n_chip - 1 + g) * half)], pass_send.at[g])
    all_sent(from_partner, pair_send.at[0])
    all_sent(from_team, sum_send.at[0])
    theirs = out.at[pl.ds(pl.multiple_of(other * half, half), half)]
    last = remote(theirs, theirs, last_sem.at[0], last_sem.at[1], partner)
    last.wait_send()
    last.wait_recv()


def team_layer(
    dims,
    tokens,
    first_gain,
    mixer_gate,
    mixer_value,
    value_gain,
    value_shift,
    spatial_weight,
    spatial_bias,
    mixer_out,
    second_gain,
    up_gate,
    up_value,
    taps_gate,
    taps_value,
    down_proj,
):
    n_rep, n_fs, n_tp = dims
    n_chip, n_line = n_rep * PLANE, n_fs // PLANE
    rows, width = tokens.shape
    half, team_rows = rows // n_tp, rows * n_chip
    cols, hidden_cols = mixer_gate.shape[1] // n_chip, up_gate.shape[1] // n_chip
    vmem, anywhere = pl.BlockSpec(memory_space=pltpu.VMEM), pl.BlockSpec(memory_space=pl.ANY)
    bf16, f32, dma = jnp.bfloat16, jnp.float32, pltpu.SemaphoreType.DMA
    in_specs = [anywhere] * 15
    units = n_fs
    scratch = [
        pltpu.VMEM((width, cols), bf16),
        pltpu.VMEM((width, cols), bf16),
        pltpu.VMEM((n_fs, mixer_out.shape[0] // n_chip, mixer_out.shape[1]), bf16),
        pltpu.VMEM((width, hidden_cols), bf16),
        pltpu.VMEM((width, hidden_cols), bf16),
        pltpu.VMEM((n_fs, down_proj.shape[0] // n_chip, down_proj.shape[1]), bf16),
        pltpu.VMEM((team_rows, width), bf16),
        pltpu.VMEM((team_rows, width), bf16),
        pltpu.VMEM((team_rows, cols), f32),
        pltpu.VMEM((team_rows, cols), f32),
        pltpu.VMEM((team_rows, cols), bf16),
        pltpu.VMEM((team_rows, hidden_cols), f32),
        pltpu.VMEM((team_rows, hidden_cols), bf16),
        pltpu.VMEM((team_rows, width), bf16),
        pltpu.VMEM((n_chip * half, width), bf16),
        pltpu.VMEM((n_chip - 1, half, width), bf16),
        pltpu.VMEM((half, width), bf16),
        pltpu.VMEM((n_chip * n_tp, 2, team_rows), f32),
        pltpu.VMEM((cols // GDIM,) + spatial_weight.shape[1:], bf16),
        pltpu.VMEM((2, 3, hidden_cols), f32),
        pltpu.VMEM((2, width), f32),
        pltpu.VMEM((2, cols), f32),
        pltpu.VMEM(spatial_bias.shape, f32),
        pltpu.VMEM((2, mixer_value.shape[0], cols), bf16),
        dma((1,)),
        dma((1,)),
        dma((2,)),
        dma((2,)),
        dma((ARRAYS, n_fs)),
        dma((2,)),
        dma((2, 4)),
        dma((2,)),
        dma((2, n_chip)),
        dma((2,)),
        dma((1,)),
        dma((units + 1, 2)),
        dma((1,)),
        dma((units + 1, 2)),
        dma((2,)),
        dma((2, 2)),
        dma((2,)),
        dma((10,)),
        dma((1,)),
    ]
    return pl.pallas_call(
        functools.partial(team_kernel, dims),
        out_shape=pltpu.VMEM((rows, width), bf16),
        in_specs=in_specs,
        out_specs=vmem,
        scratch_shapes=scratch,
        compiler_params=pltpu.CompilerParams(
            collective_id=0, has_side_effects=True, vmem_limit_bytes=56 * 1024 * 1024
        ),
    )(
        tokens,
        first_gain.reshape(1, -1),
        mixer_gate,
        mixer_value,
        value_gain.reshape(1, -1),
        value_shift.reshape(1, -1),
        spatial_weight,
        spatial_bias,
        mixer_out,
        second_gain.reshape(1, -1),
        up_gate,
        up_value,
        taps_gate,
        taps_value,
        down_proj,
    )


def team_fits(mesh):
    n_rep, n_fs, n_tp = (mesh.shape[name] for name in ("rep", "fs", "tp"))
    if n_tp != 2 or n_rep * PLANE != FAR + 1 or n_fs % PLANE or n_fs < 3 * PLANE:
        return False
    return D % (n_fs * GDIM) == 0 and D % (n_tp * n_rep * PLANE * GDIM) == 0


def solution(mesh):
    in_specs = (
        P(("rep", "fs"), None),
        P(),
        P("fs", "tp"),
        P("fs", "tp"),
        P(),
        P(),
        P(),
        P(),
        P("tp", "fs"),
        P(),
        P("fs", "tp"),
        P("fs", "tp"),
        P(),
        P(),
        P("tp", "fs"),
    )
    out_specs = P(("rep", "fs"), None)
    body = local
    if team_fits(mesh):
        dims = tuple(mesh.shape[name] for name in ("rep", "fs", "tp"))
        body = functools.partial(team_layer, dims)
    return jax.shard_map(body, mesh=mesh, in_specs=in_specs, out_specs=out_specs, check_vma=False)
```
